256 devices in a mesh: sp: 64 (over z, x, core), tp: 4 (over y).
Axes of the slice: x: 4, y: 4, z: 8, core: 2. Of those that a mesh axis runs over, the one named last changes fastest.
Arguments:
- incoming_residual_stream: bfloat16 [32768, 2048], P(('sp', 'tp')), may hold values from -6 to 6
- result_valve: bfloat16 [32768, 2048], P('sp', 'tp'), may hold values from -6 to 6
- channel_feed_matrix: bfloat16 [32768, 2048], P('sp', 'tp'), may hold values from -6 to 6
- memory_feed_matrix: bfloat16 [32768, 512], P('sp', 'tp'), may hold values from -6 to 6
- memory_query_matrix: bfloat16 [32768, 512], P('sp', 'tp'), may hold values from -6 to 6
- unsoftened_deltas: float32 [32768, 32], P('sp', 'tp'), may hold values from -2.7 to 2.7
- delta_offset: float32 [32], P('tp'), may hold values from -4.5 to -3.5
- channel_fading_speed: float32 [32], P('tp'), as said below
- extra_log_fading: float32 [32768, 32], P('sp', 'tp'), may hold values from -0.7 to 0
- bypass_factor: float32 [32], P('tp'), may hold values from 0.1 to 1.9
- channel_feed_kernel: bfloat16 [4, 2048], P(None, 'tp'), may hold values from -3 to 3
- memory_feed_kernel: bfloat16 [4, 512], P(None, 'tp'), may hold values from -3 to 3
- memory_query_kernel: bfloat16 [4, 512], P(None, 'tp'), may hold values from -3 to 3
- cluster_scaling_vector: float32 [2048], P('tp'), may hold values from 0.1 to 1.9
- mixer_result_matrix: bfloat16 [2048, 2048], P('tp'), may hold values from -0.125 to 0.125
- initial_scaling_vector: float32 [2048], replicated, may hold values from 0.1 to 1.9
- valve_matrix: bfloat16 [2048, 5632], P('sp', 'tp'), may hold values from -0.125 to 0.125
- widen_matrix: bfloat16 [2048, 5632], P('sp', 'tp'), may hold values from -0.125 to 0.125
- shrink_matrix: bfloat16 [5632, 2048], P('tp', 'sp'), may hold values from -0.078125 to 0.078125
- valve_filter_kernel: bfloat16 [3, 5632], P(None, 'tp'), may hold values from -3.5 to 3.5
- widen_filter_kernel: bfloat16 [3, 5632], P(None, 'tp'), may hold values from -3.5 to 3.5
- latter_scaling_vector: float32 [2048], replicated, may hold values from 0.1 to 1.9
Outputs:
- layer_out: bfloat16 [32768, 2048], P(('sp', 'tp'))
The draws below stay inside these ranges and needn't reach their ends.
Inputs may be any that keep to these rules, and one draw needn't show every extreme that they name: `channel_fading_speed`: positive.
All inputs are finite; a program needn't handle non-finite values.
Results may differ from the reference program's by a relative error of at most 0.02.
Values may be sent and summed in bfloat16 or wider, within the bound.
No kernel may reach another device: no remote copies, remote signals or barrier semaphores. Data moves between devices by JAX's collectives and lax.ppermute only.
A program may use at most 128 MiB of HBM per device.

```python
import math
import jax
import jax.numpy as jnp
from jax import lax

D = 2048
HEADS = 32
HEAD_DIM = 64
GROUPS = 4
STATE = 128
FF = 5632
CONV = 4
FCONV = 3
BLOCK = 128
TOK_DEV = 512
INNER = 2048
TOKENS = 32768
N_TP = 4


def draw_unsoftened_deltas(key, part):
    noise_key = jax.random.fold_in(key, 11)
    block_key = jax.random.fold_in(key, 12)
    centred_part = jnp.clip(0.5 * jax.random.normal(noise_key, (TOKENS, HEADS), jnp.float32), -2.0, 2.0)
    shifts = jax.random.uniform(block_key, (TOKENS // TOK_DEV, 1), jnp.float32, -0.7, 0.7)
    return centred_part + jnp.repeat(shifts, TOK_DEV, axis=0)


def draw_channel_fading_speed(key, part):
    slow_share = 0.5
    slow_mask = jax.random.uniform(jax.random.fold_in(key, 21), (HEADS,), jnp.float32) < slow_share
    fast_rate = jnp.exp(jax.random.uniform(jax.random.fold_in(key, 22), (HEADS,), jnp.float32, 0.0, math.log(4.0)))
    slow_rate = jax.random.uniform(jax.random.fold_in(key, 23), (HEADS,), jnp.float32, 10.0, 30.0) / TOKENS
    return jnp.where(slow_mask, slow_rate, fast_rate)


def draw_extra_log_fading(key, part):
    hits = jax.random.uniform(jax.random.fold_in(key, 31), (TOKENS, HEADS), jnp.float32) < 4.0 / TOKENS
    drops = jnp.log(jax.random.uniform(jax.random.fold_in(key, 32), (TOKENS, HEADS), jnp.float32, 0.5, 0.8))
    return jnp.where(hits, drops, 0.0)


def block_levels(key, dims, cuts, least, largest):
    level = 1.0
    for axis_at, shards_of in cuts:
        heights = jax.random.uniform(jax.random.fold_in(jax.random.fold_in(key, 6), axis_at), (shards_of,), jnp.float32, least / len(cuts), largest / len(cuts))
        level = level * jnp.repeat(jnp.exp(heights), dims[axis_at] // shards_of).reshape((-1,) + (1,) * (len(dims) - 1 - axis_at))
    return level


def noise(rng, dims, scale, limit, cuts=(), held_as=jnp.bfloat16):
    result = jax.random.normal(rng, dims, jnp.float32) * scale
    if len(cuts) > 0:
        result = block_levels(rng, dims, cuts, -0.22, 0.18) * result
    return jnp.clip(result, min=-limit, max=limit).astype(held_as)


def setup_inputs(seed: int = 0) -> dict:
    keys = jax.random.split(jax.random.key(seed), 23)
    incoming_residual_stream = noise(keys[0], (TOKENS, D), 1.0, 6.0, ((0, 256),))
    result_valve = noise(keys[1], (TOKENS, INNER), 1.0, 6.0, ((0, 64), (1, 4)))
    channel_feed_matrix = noise(keys[2], (TOKENS, INNER), 1.0, 6.0, ((0, 64), (1, 4)))
    memory_feed_matrix = noise(keys[3], (TOKENS, GROUPS * STATE), 1.0, 6.0, ((0, 64), (1, 4)))
    memory_query_matrix = noise(keys[4], (TOKENS, GROUPS * STATE), 1.0, 6.0, ((0, 64), (1, 4)))
    unsoftened_deltas = draw_unsoftened_deltas(jax.random.fold_in(keys[22], 71), 0)
    delta_offset = jnp.clip(-4.5 + 1.0 * jax.random.uniform(keys[6], (HEADS,), jnp.float32) ** block_levels(keys[6], (HEADS,), ((0, 4),), -0.2, 0.2), -4.5, -3.5)
    channel_fading_speed = draw_channel_fading_speed(jax.random.fold_in(keys[22], 71), 0)
    extra_log_fading = draw_extra_log_fading(jax.random.fold_in(keys[22], 71), 0)
    bypass_factor = jnp.clip(1.0 + 0.18 * jax.random.normal(keys[9], (HEADS,), jnp.float32), 0.1, 1.9)
    channel_feed_kernel = noise(keys[10], (CONV, INNER), CONV ** -0.5, 3.0, ((1, 4),))
    memory_feed_kernel = noise(keys[11], (CONV, GROUPS * STATE), CONV ** -0.5, 3.0, ((1, 4),))
    memory_query_kernel = noise(keys[12], (CONV, GROUPS * STATE), CONV ** -0.5, 3.0, ((1, 4),))
    cluster_scaling_vector = jnp.clip(1.0 + 0.18 * jax.random.normal(keys[13], (INNER,), jnp.float32), 0.1, 1.9)
    mixer_result_matrix = noise(keys[14], (INNER, D), INNER ** -0.5, 0.125, ((0, 4),))
    initial_scaling_vector = jnp.clip(1.0 + 0.18 * jax.random.normal(keys[15], (D,), jnp.float32), 0.1, 1.9)
    valve_matrix = noise(keys[16], (D, FF), D ** -0.5, 0.125, ((0, 64), (1, 4)))
    widen_matrix = noise(keys[17], (D, FF), D ** -0.5, 0.125, ((0, 64), (1, 4)))
    shrink_matrix = noise(keys[18], (FF, D), FF ** -0.5, 0.078125, ((0, 4), (1, 64)))
    valve_filter_kernel = noise(keys[19], (FCONV, FF), FCONV ** -0.5, 3.5, ((1, 4),))
    widen_filter_kernel = noise(keys[20], (FCONV, FF), FCONV ** -0.5, 3.5, ((1, 4),))
    latter_scaling_vector = jnp.clip(1.0 + 0.18 * jax.random.normal(keys[21], (D,), jnp.float32), 0.1, 1.9)
    return {"incoming_residual_stream": incoming_residual_stream, "result_valve": result_valve, "channel_feed_matrix": channel_feed_matrix, "memory_feed_matrix": memory_feed_matrix, "memory_query_matrix": memory_query_matrix, "unsoftened_deltas": unsoftened_deltas, "delta_offset": delta_offset, "channel_fading_speed": channel_fading_speed, "extra_log_fading": extra_log_fading, "bypass_factor": bypass_factor, "channel_feed_kernel": channel_feed_kernel, "memory_feed_kernel": memory_feed_kernel, "memory_query_kernel": memory_query_kernel, "cluster_scaling_vector": cluster_scaling_vector, "mixer_result_matrix": mixer_result_matrix, "initial_scaling_vector": initial_scaling_vector, "valve_matrix": valve_matrix, "widen_matrix": widen_matrix, "shrink_matrix": shrink_matrix, "valve_filter_kernel": valve_filter_kernel, "widen_filter_kernel": widen_filter_kernel, "latter_scaling_vector": latter_scaling_vector}


EPSILON = 1e-05
ALPHA = 2.0 ** 0.25
HIGHEST = lax.Precision.HIGHEST

def causal_conv(signal, before, tap_weights):
    tap_count = tap_weights.shape[0]
    row_count = signal.shape[0]
    padded = jnp.concatenate([before, signal], axis=0).astype(jnp.float32)
    running = jnp.zeros(signal.shape, jnp.float32)
    for tap_index in range(tap_count):
        running = running + tap_weights[tap_index].astype(jnp.float32) * padded[tap_index:tap_index + row_count]
    return running

def zero_rim(signal, tap_count):
    return jnp.zeros((tap_count - 1, signal.shape[1]), signal.dtype)

def layer_norm(values, scales):
    row_mean = lax.optimization_barrier(jnp.mean(values, axis=-1, keepdims=True))
    centred = values - row_mean
    spread = lax.optimization_barrier(jnp.mean(centred * centred, axis=-1, keepdims=True))
    return centred * lax.rsqrt(spread + EPSILON) * scales

def block_sum(activations, weights, pieces):
    slice_width = activations.shape[1] // pieces
    running = jnp.zeros((activations.shape[0], weights.shape[1]), jnp.float32)
    for piece_index in range(pieces):
        lower = piece_index * slice_width
        partial_value = jnp.dot(activations[:, lower:lower + slice_width], weights[lower:lower + slice_width], preferred_element_type=jnp.float32)
        rounded = lax.optimization_barrier(partial_value.astype(jnp.bfloat16))
        running = running + rounded.astype(jnp.float32)
    return running

def ssd_block(state_now, inputs):
    x_blk, b_blk, c_blk, decay_blk = inputs
    cum_decay = jnp.cumsum(decay_blk, axis=0)
    block_len = decay_blk.shape[0]
    causal = jnp.tril(jnp.ones((block_len, block_len), dtype=bool))
    between = cum_decay[:, None] - cum_decay[None, :]
    lag = jnp.exp(jnp.where(causal[:, :, None, None], between, -jnp.inf))
    affinity = jnp.einsum('lgn,sgn->lsg', c_blk, b_blk, precision=HIGHEST)
    mixing = affinity[..., None] * lag
    within = jnp.einsum('lsgh,sghp->lghp', mixing, x_blk, precision=HIGHEST)
    carried = jnp.einsum('lgn,ghpn->lghp', c_blk, state_now, precision=HIGHEST) * jnp.exp(cum_decay)[..., None]
    to_end = jnp.exp(cum_decay[-1] - cum_decay)
    fresh = jnp.einsum('lgn,lghp->ghpn', b_blk, x_blk * to_end[..., None], precision=HIGHEST)
    state_next = state_now * jnp.exp(cum_decay[-1])[..., None, None] + fresh
    return (state_next, within + carried)

def reference(incoming_residual_stream, result_valve, channel_feed_matrix, memory_feed_matrix, memory_query_matrix, unsoftened_deltas, delta_offset, channel_fading_speed, extra_log_fading, bypass_factor, channel_feed_kernel, memory_feed_kernel, memory_query_kernel, cluster_scaling_vector, mixer_result_matrix, initial_scaling_vector, valve_matrix, widen_matrix, shrink_matrix, valve_filter_kernel, widen_filter_kernel, latter_scaling_vector):
    group_heads = HEADS // GROUPS
    x_act = jax.nn.silu(causal_conv(channel_feed_matrix, zero_rim(channel_feed_matrix, CONV), channel_feed_kernel)).astype(jnp.bfloat16)
    b_act = jax.nn.silu(causal_conv(memory_feed_matrix, zero_rim(memory_feed_matrix, CONV), memory_feed_kernel)).astype(jnp.bfloat16)
    c_act = jax.nn.silu(causal_conv(memory_query_matrix, zero_rim(memory_query_matrix, CONV), memory_query_kernel)).astype(jnp.bfloat16)
    channel_delta_amount = jax.nn.softplus(unsoftened_deltas + delta_offset[None, :])
    log_fading_amount = extra_log_fading - channel_fading_speed[None, :] * channel_delta_amount
    block_count = TOKENS // BLOCK
    x_heads = x_act.astype(jnp.float32).reshape(TOKENS, GROUPS, group_heads, HEAD_DIM)
    x_scaled = x_heads * channel_delta_amount.reshape(TOKENS, GROUPS, group_heads)[..., None]
    x_blocks = x_scaled.reshape(block_count, BLOCK, GROUPS, group_heads, HEAD_DIM)
    b_blocks = b_act.astype(jnp.float32).reshape(block_count, BLOCK, GROUPS, STATE)
    c_blocks = c_act.astype(jnp.float32).reshape(block_count, BLOCK, GROUPS, STATE)
    decay_blocks = log_fading_amount.reshape(block_count, BLOCK, GROUPS, group_heads)
    initial = jnp.zeros((GROUPS, group_heads, HEAD_DIM, STATE), jnp.float32)
    _, mixed = lax.scan(ssd_block, initial, (x_blocks, b_blocks, c_blocks, decay_blocks))
    y_heads = mixed.reshape(TOKENS, GROUPS, group_heads, HEAD_DIM)
    y_heads = y_heads + bypass_factor.reshape(GROUPS, group_heads)[None, :, :, None] * x_heads
    gated = y_heads.reshape(TOKENS, GROUPS, INNER // GROUPS)
    gated = gated * jax.nn.silu(result_valve.astype(jnp.float32)).reshape(TOKENS, GROUPS, INNER // GROUPS)
    gated = gated * lax.rsqrt(lax.optimization_barrier(jnp.mean(gated * gated, axis=-1, keepdims=True)) + EPSILON)
    y_norm = (gated.reshape(TOKENS, INNER) * cluster_scaling_vector[None, :]).astype(jnp.bfloat16)
    mixer = block_sum(y_norm, mixer_result_matrix, N_TP)
    normed = layer_norm(ALPHA * incoming_residual_stream.astype(jnp.float32) + mixer, initial_scaling_vector).astype(jnp.bfloat16)
    gate_proj = jnp.dot(normed, valve_matrix, preferred_element_type=jnp.float32).astype(jnp.bfloat16)
    up_proj = jnp.dot(normed, widen_matrix, preferred_element_type=jnp.float32).astype(jnp.bfloat16)
    gate_conv = causal_conv(gate_proj, zero_rim(gate_proj, FCONV), valve_filter_kernel)
    up_conv = causal_conv(up_proj, zero_rim(up_proj, FCONV), widen_filter_kernel)
    hidden = (jax.nn.silu(gate_conv) * up_conv).astype(jnp.bfloat16)
    channel = block_sum(hidden, shrink_matrix, N_TP)
    return layer_norm(ALPHA * normed.astype(jnp.float32) + channel, latter_scaling_vector).astype(jnp.bfloat16)
```

```python
import jax
import jax.numpy as jnp
from jax import lax
from jax.experimental import pallas as pl
from jax.experimental.pallas import tpu as pltpu
from jax.sharding import Mesh
from jax.sharding import PartitionSpec as P

HEADS = 32
HEAD_DIM = 64
GROUPS = 4
STATE = 128
CONV = 4
FCONV = 3
BLOCK = 128
SP = ("sp_0", "sp_1", "sp_2")
SP_TP = ("sp_0", "sp_1", "sp_2", "tp")

EPSILON = 1e-05
ALPHA = 2.0**0.25
F32 = jnp.float32
BF16 = jnp.bfloat16
NEG = -1e30

ROWS = 512
CH = 512
NH = 8
QUARTER = 128
D = 2048
HALF = 1024
FFL = 1408

VMEM = pl.BlockSpec(memory_space=pltpu.VMEM)
SMEM = pl.BlockSpec(memory_space=pltpu.SMEM)


def dot(a, b):
    return jnp.dot(a, b, preferred_element_type=F32)


def dot_nt(a, b, precision=None):
    return lax.dot_general(
        a, b, (((1,), (1,)), ((), ())), precision=precision, preferred_element_type=F32
    )


def silu(v):
    return v / (1.0 + jnp.exp(-v))


def lane_pairs(column_of, rows):
    low = lax.broadcasted_iota(jnp.int32, (rows, 128), 1) < HEAD_DIM
    slabs = []
    for q in range(NH // 2):
        first = jnp.broadcast_to(column_of[:, 2 * q : 2 * q + 1], (rows, 128))
        second = jnp.broadcast_to(column_of[:, 2 * q + 1 : 2 * q + 2], (rows, 128))
        slabs.append(jnp.where(low, first, second))
    return slabs


def local_kernel(
    x_ref, b_ref, c_ref, rim_ref, xt_ref, bt_ref, ct_ref, delta_ref, extra_ref, head_ref,
    y_ref, cact_ref, grow_ref, msg_ref,
    xpad, bpad, cpad,
):
    xpad[0:8, :] = rim_ref[:, 0:CH].astype(F32)
    bpad[0:8, :] = rim_ref[:, CH : CH + STATE].astype(F32)
    cpad[0:8, :] = rim_ref[:, CH + STATE : CH + 2 * STATE].astype(F32)
    xpad[8 : 8 + ROWS, :] = x_ref[...].astype(F32)
    bpad[8 : 8 + ROWS, :] = b_ref[...].astype(F32)
    cpad[8 : 8 + ROWS, :] = c_ref[...].astype(F32)

    def conv(pad, taps, start):
        total = None
        for k in range(CONV):
            term = taps[k : k + 1, :].astype(F32) * pad[pl.ds(start + 8 - CONV + 1 + k, BLOCK), :]
            total = term if total is None else total + term
        return silu(total)

    offset = head_ref[0:1, :]
    speed = head_ref[1:2, :]
    bypass = lane_pairs(head_ref[2:3, :], 1)
    row = lax.broadcasted_iota(jnp.int32, (BLOCK, BLOCK), 0)
    col = lax.broadcasted_iota(jnp.int32, (BLOCK, BLOCK), 1)
    causal = row >= col
    lower = jnp.where(causal, 1.0, 0.0).astype(F32)
    eye = jnp.where(
        lax.broadcasted_iota(jnp.int32, (NH, NH), 0) == lax.broadcasted_iota(jnp.int32, (NH, NH), 1),
        1.0,
        0.0,
    ).astype(F32)
    low = col < HEAD_DIM
    state = [jnp.zeros((STATE, 128), F32) for _ in range(NH // 2)]
    base = jnp.zeros((1, NH), F32)
    for i in range(ROWS // BLOCK):
        start = i * BLOCK
        rows = pl.ds(start, BLOCK)
        step_in = delta_ref[rows, :] + offset
        step = jnp.maximum(step_in, 0.0) + jnp.log1p(jnp.exp(-jnp.abs(step_in)))
        fading = extra_ref[rows, :] - speed * step
        cum = jnp.dot(lower, fading, precision=lax.Precision.HIGHEST, preferred_element_type=F32)
        cum_t = dot_nt(eye, cum, precision=lax.Precision.HIGHEST)
        last = cum[BLOCK - 1 : BLOCK, :]
        x_act = conv(xpad, xt_ref, start).astype(BF16).astype(F32)
        b_act = conv(bpad, bt_ref, start).astype(BF16)
        c_act = conv(cpad, ct_ref, start).astype(BF16)
        cact_ref[rows, :] = c_act
        grow_ref[rows, :] = jnp.exp(base + cum)
        affinity = dot_nt(c_act, b_act)
        b_turned = b_act.astype(F32).T.astype(BF16)
        steps = lane_pairs(step, BLOCK)
        to_end = lane_pairs(jnp.exp(last - cum), BLOCK)
        grown = lane_pairs(jnp.exp(cum), BLOCK)
        kept = lane_pairs(jnp.exp(last), 1)
        for q in range(NH // 2):
            cols = slice(q * 128, (q + 1) * 128)
            x_here = x_act[:, cols]
            scaled = x_here * steps[q]
            narrow = scaled.astype(BF16)
            within = []
            for h in (2 * q, 2 * q + 1):
                between = cum[:, h : h + 1] - cum_t[h : h + 1, :]
                lag = jnp.exp(jnp.where(causal, between, NEG))
                within.append(dot((affinity * lag).astype(BF16), narrow))
            total = jnp.where(low, within[0], within[1]) + bypass[q] * x_here
            if i > 0:
                total = total + dot(c_act, state[q].astype(BF16)) * grown[q]
            y_ref[rows, cols] = total
            fresh = dot(b_turned, (scaled * to_end[q]).astype(BF16))
            state[q] = fresh if i == 0 else state[q] * kept[q] + fresh
        base = base + last
    totals = lane_pairs(base, 1)
    for q in range(NH // 2):
        block = slice(q * 16, (q + 1) * 16)
        msg_ref[block, 0:8, :] = state[q].reshape(16, 8, 128).astype(BF16)
        left = totals[q]
        parts = []
        for _ in range(3):
            part = left.astype(BF16)
            parts.append(part.astype(F32))
            left = left - part.astype(F32)
        line = lax.broadcasted_iota(jnp.int32, (8, 128), 0)
        packed = jnp.where(line == 0, parts[0], jnp.where(line == 1, parts[1], parts[2]))
        packed = jnp.where(line < 3, packed, 0.0).astype(BF16)
        msg_ref[block, 8:16, :] = jnp.broadcast_to(packed[None], (16, 8, 128))


def run_local(x, b, c, rim, xt, bt, ct, delta, extra, heads):
    return pl.pallas_call(
        local_kernel,
        out_shape=(
            jax.ShapeDtypeStruct((ROWS, CH), F32),
            jax.ShapeDtypeStruct((ROWS, STATE), BF16),
            jax.ShapeDtypeStruct((ROWS, NH), F32),
            jax.ShapeDtypeStruct((64, 16, 128), BF16),
        ),
        in_specs=[VMEM] * 10,
        out_specs=(VMEM,) * 4,
        scratch_shapes=[
            pltpu.VMEM((ROWS + 8, CH), F32),
            pltpu.VMEM((ROWS + 8, STATE), F32),
            pltpu.VMEM((ROWS + 8, STATE), F32),
        ],
        name="local_mixer",
    )(x, b, c, rim, xt, bt, ct, delta, extra, heads)


def prefix_kernel(in_ref, out_ref):
    entering = jnp.zeros((8, 128), F32)
    for j in range(64):
        out_ref[j] = entering.astype(BF16)
        piece = in_ref[j].astype(F32)
        total = piece[8:9, :] + piece[9:10, :] + piece[10:11, :]
        entering = entering * jnp.exp(total) + piece[0:8, :]


def run_prefix(received):
    return pl.pallas_call(
        prefix_kernel,
        out_shape=jax.ShapeDtypeStruct((64, 8, 128), BF16),
        in_specs=[VMEM],
        out_specs=VMEM,
        name="state_prefix",
    )(received)


def project_kernel(
    place_ref, y_ref, cact_ref, grow_ref, in_ref, valve_ref, scale_ref, w_ref,
    send_l, send_r, keep_l, keep_r, norm,
):
    for i in range(ROWS // BLOCK):
        rows = pl.ds(i * BLOCK, BLOCK)
        grown = lane_pairs(grow_ref[rows, :], BLOCK)
        c_act = cact_ref[rows, :]
        gated = []
        square = jnp.zeros((BLOCK, 1), F32)
        for q in range(NH // 2):
            cols = slice(q * 128, (q + 1) * 128)
            entering = in_ref[q * 16 : (q + 1) * 16].astype(F32).reshape(STATE, 128).astype(BF16)
            y = y_ref[rows, cols] + dot(c_act, entering) * grown[q]
            y = y * silu(valve_ref[rows, cols].astype(F32))
            gated.append(y)
            square = square + jnp.sum(y * y, axis=-1, keepdims=True)
        factor = lax.rsqrt(square * (1.0 / CH) + EPSILON)
        for q in range(NH // 2):
            cols = slice(q * 128, (q + 1) * 128)
            norm[rows, cols] = (gated[q] * factor * scale_ref[0:1, cols]).astype(BF16)

    def rows_of(k):
        return norm[pl.ds(pl.multiple_of(place_ref[k] * QUARTER, QUARTER), QUARTER), :]

    own, near, far, across = (rows_of(k) for k in range(4))
    left = w_ref[:, 0:HALF]
    right = w_ref[:, HALF:D]
    send_l[...] = dot(jnp.concatenate([near, across], axis=0), left).astype(BF16)
    send_r[...] = dot(jnp.concatenate([far, across], axis=0), right).astype(BF16)
    keep_l[...] = dot(jnp.concatenate([own, far], axis=0), left)
    keep_r[...] = dot(jnp.concatenate([own, near], axis=0), right)


def run_project(place, y, cact, grow, entering, valve, scale, w):
    return pl.pallas_call(
        project_kernel,
        out_shape=(
            jax.ShapeDtypeStruct((2 * QUARTER, HALF), BF16),
            jax.ShapeDtypeStruct((2 * QUARTER, HALF), BF16),
            jax.ShapeDtypeStruct((2 * QUARTER, HALF), F32),
            jax.ShapeDtypeStruct((2 * QUARTER, HALF), F32),
        ),
        in_specs=[SMEM] + [VMEM] * 7,
        out_specs=(VMEM,) * 4,
        scratch_shapes=[pltpu.VMEM((ROWS, CH), BF16)],
        name="gate_project",
    )(place, y, cact, grow, entering, valve, scale, w)


def normed_halves(values_l, values_r, scale_ref):
    mean = (
        jnp.sum(values_l, axis=-1, keepdims=True) + jnp.sum(values_r, axis=-1, keepdims=True)
    ) * (1.0 / D)
    left = values_l - mean
    right = values_r - mean
    spread = (
        jnp.sum(left * left, axis=-1, keepdims=True)
        + jnp.sum(right * right, axis=-1, keepdims=True)
    ) * (1.0 / D)
    factor = lax.rsqrt(spread + EPSILON)
    return left * factor * scale_ref[0:1, 0:HALF], right * factor * scale_ref[0:1, HALF:D]


def first_norm_kernel(
    keep_l, keep_r, once_l, once_r, twice_l, twice_r, res_ref, scale_ref, out_l, out_r
):
    left = keep_l[...] + once_l[...].astype(F32) + twice_l[...].astype(F32)
    right = keep_r[...] + once_r[...].astype(F32) + twice_r[...].astype(F32)
    left = left + ALPHA * res_ref[:, 0:HALF].astype(F32)
    right = right + ALPHA * res_ref[:, HALF:D].astype(F32)
    left, right = normed_halves(left, right, scale_ref)
    out_l[...] = left.astype(BF16)
    out_r[...] = right.astype(BF16)


def last_norm_kernel(
    keep_l, keep_r, once_l, once_r, twice_l, twice_r, res_l, res_r, scale_ref, out_ref
):
    left = keep_l[...] + once_l[...].astype(F32) + twice_l[...].astype(F32)
    right = keep_r[...] + once_r[...].astype(F32) + twice_r[...].astype(F32)
    left = left + ALPHA * res_l[...].astype(F32)
    right = right + ALPHA * res_r[...].astype(F32)
    left, right = normed_halves(left, right, scale_ref)
    out_ref[:, 0:HALF] = left.astype(BF16)
    out_ref[:, HALF:D] = right.astype(BF16)


TOP = pl.BlockSpec((QUARTER, HALF), lambda i: (0, 0))


def run_first_norm(keeps, onces, twices, residual, scale):
    return pl.pallas_call(
        first_norm_kernel,
        grid=(1,),
        out_shape=(jax.ShapeDtypeStruct((QUARTER, HALF), BF16),) * 2,
        in_specs=[TOP] * 6
        + [
            pl.BlockSpec((QUARTER, D), lambda i: (0, 0)),
            pl.BlockSpec((1, D), lambda i: (0, 0)),
        ],
        out_specs=(TOP, TOP),
        name="first_norm",
    )(*keeps, *onces, *twices, residual, scale)


def run_last_norm(keeps, onces, twices, own, scale):
    return pl.pallas_call(
        last_norm_kernel,
        grid=(1,),
        out_shape=jax.ShapeDtypeStruct((QUARTER, D), BF16),
        in_specs=[TOP] * 8 + [pl.BlockSpec((1, D), lambda i: (0, 0))],
        out_specs=pl.BlockSpec((QUARTER, D), lambda i: (0, 0)),
        name="last_norm",
    )(*keeps, *onces, *twices, *own, scale)


RIM = 16


def widen_kernel(
    place_ref, own_l, own_r, far_l, near_r, nf_l, nf_r, rim_ref, gate_w, up_w, gate_t, up_t,
    hid_ref, rows, gate_pad, up_pad,
):
    @pl.when(pl.program_id(0) == 0)
    def _():
        def at(k):
            return pl.ds(pl.multiple_of(RIM + place_ref[k] * QUARTER, RIM), QUARTER)

        left = slice(0, HALF)
        right = slice(HALF, D)
        rows[0:RIM, :] = rim_ref[...]
        rows[at(0), left] = own_l[...]
        rows[at(0), right] = own_r[...]
        rows[at(2), left] = far_l[...]
        rows[at(1), right] = near_r[...]
        rows[at(1), left] = nf_l[0:QUARTER, :]
        rows[at(3), left] = nf_l[QUARTER : 2 * QUARTER, :]
        rows[at(2), right] = nf_r[0:QUARTER, :]
        rows[at(3), right] = nf_r[QUARTER : 2 * QUARTER, :]

    both = dot(rows[...], jnp.concatenate([gate_w[...], up_w[...]], axis=1))
    both = both.astype(BF16).astype(F32)
    gate_pad[...] = both[:, 0:128]
    up_pad[...] = both[:, 128:256]

    def conv(pad, taps):
        total = None
        for k in range(FCONV):
            term = taps[k : k + 1, :].astype(F32) * pad[pl.ds(RIM - FCONV + 1 + k, ROWS), :]
            total = term if total is None else total + term
        return total

    hid_ref[...] = (silu(conv(gate_pad, gate_t)) * conv(up_pad, up_t)).astype(BF16)


def run_widen(place, pieces, rim, weights, gate_t, up_t):
    tiles = FFL // 128
    whole = lambda shape: pl.BlockSpec(shape, lambda j: (0, 0))
    return pl.pallas_call(
        widen_kernel,
        grid=(tiles,),
        out_shape=jax.ShapeDtypeStruct((ROWS, FFL), BF16),
        in_specs=[
            SMEM,
            whole((QUARTER, HALF)),
            whole((QUARTER, HALF)),
            whole((QUARTER, HALF)),
            whole((QUARTER, HALF)),
            whole((2 * QUARTER, HALF)),
            whole((2 * QUARTER, HALF)),
            whole((RIM, D)),
            pl.BlockSpec((D, 128), lambda j: (0, j)),
            pl.BlockSpec((D, 128), lambda j: (0, j + FFL // 128)),
            pl.BlockSpec((FCONV, 128), lambda j: (0, j)),
            pl.BlockSpec((FCONV, 128), lambda j: (0, j)),
        ],
        out_specs=pl.BlockSpec((ROWS, 128), lambda j: (0, j)),
        scratch_shapes=[
            pltpu.VMEM((ROWS + RIM, D), BF16),
            pltpu.VMEM((ROWS + RIM, 128), F32),
            pltpu.VMEM((ROWS + RIM, 128), F32),
        ],
        name="widen",
    )(place, *pieces, rim, weights, weights, gate_t, up_t)


NARROW = 512


def shrink_kernel(place_ref, hid_ref, w_ref, out_ref):
    half = pl.program_id(0) // (HALF // NARROW)

    def rows_of(k):
        return hid_ref[pl.ds(pl.multiple_of(place_ref[half, k] * QUARTER, QUARTER), QUARTER), :]

    lhs = jnp.concatenate([rows_of(0), rows_of(1)], axis=0)
    out_ref[...] = dot_nt(lhs, w_ref[...]).astype(out_ref.dtype)


def run_shrink(place, hidden, weights, kind, name):
    return pl.pallas_call(
        shrink_kernel,
        grid=(D // NARROW,),
        out_shape=jax.ShapeDtypeStruct((2 * QUARTER, D), kind),
        in_specs=[
            SMEM,
            pl.BlockSpec((ROWS, FFL), lambda j: (0, 0)),
            pl.BlockSpec((NARROW, FFL), lambda j: (j, 2)),
        ],
        out_specs=pl.BlockSpec((2 * QUARTER, NARROW), lambda j: (0, j)),
        name=name,
    )(place, hidden, weights)


NEAR = [(0, 1), (1, 0), (2, 3), (3, 2)]
FAR = [(0, 3), (3, 0), (1, 2), (2, 1)]


def with_near(part):
    return lax.ppermute(part, "tp", NEAR)


def with_far(part):
    return lax.ppermute(part, "tp", FAR)


def summed_halves(keeps, sends):
    once_l = with_near(sends[0])
    once_r = with_far(sends[1])
    on_l = (keeps[0][QUARTER:] + once_l[QUARTER:].astype(F32)).astype(BF16)
    on_r = (keeps[1][QUARTER:] + once_r[QUARTER:].astype(F32)).astype(BF16)
    return (once_l, once_r), (with_far(on_l), with_near(on_r))


def next_positions(shard):
    count = lax.axis_size(SP)
    return lax.ppermute(shard, SP, [(i, i + 1) for i in range(count - 1)])


def shards(
    incoming_residual_stream,
    result_valve,
    channel_feed_matrix,
    memory_feed_matrix,
    memory_query_matrix,
    unsoftened_deltas,
    delta_offset,
    channel_fading_speed,
    extra_log_fading,
    bypass_factor,
    channel_feed_kernel,
    memory_feed_kernel,
    memory_query_kernel,
    cluster_scaling_vector,
    mixer_result_matrix,
    initial_scaling_vector,
    valve_matrix,
    widen_matrix,
    shrink_matrix,
    valve_filter_kernel,
    widen_filter_kernel,
    latter_scaling_vector,
):
    own = lax.axis_index("tp").astype(jnp.int32)
    near = own ^ 1
    far = 3 - own
    across = own ^ 2
    place = jnp.stack([own, near, far, across])
    sent = jnp.stack([jnp.stack([near, across]), jnp.stack([far, across])])
    held = jnp.stack([jnp.stack([own, far]), jnp.stack([own, near])])

    weights = lax.all_gather(
        jnp.concatenate([valve_matrix, widen_matrix, shrink_matrix.T], axis=1), SP, tiled=True
    )

    rim = next_positions(
        jnp.concatenate(
            [
                channel_feed_matrix[ROWS - 8 :],
                memory_feed_matrix[ROWS - 8 :],
                memory_query_matrix[ROWS - 8 :],
            ],
            axis=1,
        )
    )
    heads = jnp.stack([delta_offset, channel_fading_speed, bypass_factor])
    y_local, c_act, grow, message = run_local(
        channel_feed_matrix,
        memory_feed_matrix,
        memory_query_matrix,
        rim,
        channel_feed_kernel,
        memory_feed_kernel,
        memory_query_kernel,
        unsoftened_deltas,
        extra_log_fading,
        heads,
    )
    received = lax.all_to_all(message, SP, 0, 0, tiled=True)
    entering = lax.all_to_all(run_prefix(received), SP, 0, 0, tiled=True)
    send_l, send_r, keep_l, keep_r = run_project(
        place,
        y_local,
        c_act,
        grow,
        entering,
        result_valve,
        cluster_scaling_vector.reshape(1, CH),
        mixer_result_matrix,
    )
    onces, twices = summed_halves((keep_l, keep_r), (send_l, send_r))
    own_l, own_r = run_first_norm(
        (keep_l, keep_r),
        onces,
        twices,
        incoming_residual_stream,
        initial_scaling_vector.reshape(1, D),
    )
    far_l = with_far(own_l)
    near_r = with_near(own_r)
    nf_l = with_near(jnp.concatenate([own_l, far_l], axis=0))
    nf_r = with_far(jnp.concatenate([own_r, near_r], axis=0))
    tail = slice(QUARTER - RIM, QUARTER)
    tail2 = slice(2 * QUARTER - RIM, 2 * QUARTER)
    is_last = own == 3
    near_last = near == 3
    far_last = far == 3
    end_l = jnp.where(
        is_last,
        own_l[tail],
        jnp.where(far_last, far_l[tail], jnp.where(near_last, nf_l[tail], nf_l[tail2])),
    )
    end_r = jnp.where(
        is_last,
        own_r[tail],
        jnp.where(near_last, near_r[tail], jnp.where(far_last, nf_r[tail], nf_r[tail2])),
    )
    rim_rows = next_positions(jnp.concatenate([end_l, end_r], axis=1))
    hidden = run_widen(
        place,
        (own_l, own_r, far_l, near_r, nf_l, nf_r),
        rim_rows,
        weights,
        valve_filter_kernel,
        widen_filter_kernel,
    )
    sends = run_shrink(sent, hidden, weights, BF16, "shrink_sent")
    keeps = run_shrink(held, hidden, weights, F32, "shrink_held")
    halves = lambda both: (both[:, :HALF], both[:, HALF:])
    keep_halves = halves(keeps)
    onces, twices = summed_halves(keep_halves, halves(sends))
    return run_last_norm(
        keep_halves, onces, twices, (own_l, own_r), latter_scaling_vector.reshape(1, D)
    )


def solution(mesh):
    split = Mesh(mesh.devices.reshape(8, 4, 2, mesh.shape["tp"]), ("sp_0", "sp_1", "sp_2", "tp"))
    in_specs = (
        P(SP_TP, None),
        P(SP, "tp"),
        P(SP, "tp"),
        P(SP, "tp"),
        P(SP, "tp"),
        P(SP, "tp"),
        P("tp"),
        P("tp"),
        P(SP, "tp"),
        P("tp"),
        P(None, "tp"),
        P(None, "tp"),
        P(None, "tp"),
        P("tp"),
        P("tp", None),
        P(),
        P(SP, "tp"),
        P(SP, "tp"),
        P("tp", SP),
        P(None, "tp"),
        P(None, "tp"),
        P(),
    )
    out_specs = P(SP_TP, None)
    return jax.shard_map(
        shards, mesh=split, in_specs=in_specs, out_specs=out_specs, check_vma=False
    )
```

```python
import jax
import jax.numpy as jnp
from jax import lax
from jax.experimental import pallas as pl
from jax.experimental.pallas import tpu as pltpu
from jax.sharding import Mesh
from jax.sharding import PartitionSpec as P

HEADS = 32
HEAD_DIM = 64
GROUPS = 4
STATE = 128
CONV = 4
FCONV = 3
BLOCK = 128
SP = ("sp_0", "sp_1", "sp_2")
SP_TP = ("sp_0", "sp_1", "sp_2", "tp")

EPSILON = 1e-05
ALPHA = 2.0**0.25
F32 = jnp.float32
BF16 = jnp.bfloat16
NEG = -1e30

ROWS = 512
CH = 512
NH = 8
QUARTER = 128
HALFCH = 256
D = 2048
HALF = 1024
FFL = 1408

VMEM = pl.BlockSpec(memory_space=pltpu.VMEM)
SMEM = pl.BlockSpec(memory_space=pltpu.SMEM)
ANY = pl.BlockSpec(memory_space=pl.ANY)
HIGHEST = lax.Precision.HIGHEST


def dot(a, b):
    return jnp.dot(a, b, preferred_element_type=F32)


def dot_nt(a, b, precision=None):
    return lax.dot_general(
        a, b, (((1,), (1,)), ((), ())), precision=precision, preferred_element_type=F32
    )


def silu(v):
    return v / (1.0 + jnp.exp(-v))


def lane_pairs(column_of, rows):
    low = lax.broadcasted_iota(jnp.int32, (rows, 128), 1) < HEAD_DIM
    slabs = []
    for q in range(NH // 2):
        first = jnp.broadcast_to(column_of[:, 2 * q : 2 * q + 1], (rows, 128))
        second = jnp.broadcast_to(column_of[:, 2 * q + 1 : 2 * q + 2], (rows, 128))
        slabs.append(jnp.where(low, first, second))
    return slabs


def eye(n):
    line = lax.broadcasted_iota(jnp.int32, (n, n), 0)
    lane = lax.broadcasted_iota(jnp.int32, (n, n), 1)
    return jnp.where(line == lane, 1.0, 0.0).astype(F32)


def columns(rows):
    return dot_nt(eye(BLOCK), rows, precision=HIGHEST)


def decays(delta_ref, extra_ref, offset_ref, speed_ref):
    small = eye(NH)
    offset = jnp.sum(small * offset_ref[...], axis=1, keepdims=True)
    speed = jnp.sum(small * speed_ref[...], axis=1, keepdims=True)
    step_in = delta_ref[...] + offset
    step = jnp.maximum(step_in, 0.0) + jnp.log1p(jnp.exp(-jnp.abs(step_in)))
    return step, extra_ref[...] - speed * step


def running_sum(fading):
    line = lax.broadcasted_iota(jnp.int32, (BLOCK, BLOCK), 0)
    lane = lax.broadcasted_iota(jnp.int32, (BLOCK, BLOCK), 1)
    upper = jnp.where(line <= lane, 1.0, 0.0).astype(F32)
    return jnp.dot(fading, upper, precision=HIGHEST, preferred_element_type=F32)


def conv_at(pad, taps, start):
    total = None
    for k in range(CONV):
        term = taps[k : k + 1, :].astype(F32) * pad[pl.ds(start + 8 - CONV + 1 + k, BLOCK), :]
        total = term if total is None else total + term
    return silu(total)


def rim_kernel(x_ref, b_ref, c_ref, out_ref):
    out_ref[:, 0:CH] = x_ref[...]
    out_ref[:, CH : CH + STATE] = b_ref[...]
    out_ref[:, CH + STATE : CH + 2 * STATE] = c_ref[...]


def run_rim(x, b, c):
    last = lambda width: pl.BlockSpec((8, width), lambda i: (ROWS // 8 - 1, 0))
    return pl.pallas_call(
        rim_kernel,
        grid=(1,),
        out_shape=jax.ShapeDtypeStruct((8, CH + 2 * STATE), BF16),
        in_specs=[last(CH), last(STATE), last(STATE)],
        out_specs=pl.BlockSpec((8, CH + 2 * STATE), lambda i: (0, 0)),
        name="rim",
    )(x, b, c)


def state_kernel(
    x_ref, b_ref, rim_ref, xt_ref, bt_ref, delta_ref, extra_ref, offset_ref, speed_ref,
    x_out, b_out, state_out, msg_ref,
    xpad, bpad,
):
    xpad[0:8, :] = rim_ref[:, 0:CH].astype(F32)
    bpad[0:8, :] = rim_ref[:, CH : CH + STATE].astype(F32)
    xpad[8 : 8 + ROWS, :] = x_ref[...].astype(F32)
    bpad[8 : 8 + ROWS, :] = b_ref[...].astype(F32)
    step, fading = decays(delta_ref, extra_ref, offset_ref, speed_ref)
    state = [jnp.zeros((STATE, 128), F32) for _ in range(NH // 2)]
    base = jnp.zeros((NH, 1), F32)
    for i in range(ROWS // BLOCK):
        start = i * BLOCK
        rows = pl.ds(start, BLOCK)
        here = slice(start, start + BLOCK)
        cum = running_sum(fading[:, here])
        last = cum[:, BLOCK - 1 : BLOCK]
        to_end = lane_pairs(columns(step[:, here] * jnp.exp(last - cum)), BLOCK)
        kept = lane_pairs(columns(jnp.broadcast_to(jnp.exp(last), (NH, BLOCK)))[0:1, :], 1)
        x_act = conv_at(xpad, xt_ref, start).astype(BF16)
        b_act = conv_at(bpad, bt_ref, start).astype(BF16)
        x_out[rows, :] = x_act
        b_out[rows, :] = b_act
        b_turned = b_act.astype(F32).T.astype(BF16)
        for q in range(NH // 2):
            cols = slice(q * 128, (q + 1) * 128)
            fresh = dot(b_turned, (x_act[:, cols].astype(F32) * to_end[q]).astype(BF16))
            state[q] = fresh if i == 0 else state[q] * kept[q] + fresh
            if i < ROWS // BLOCK - 1:
                state_out[i, :, cols] = state[q].astype(BF16)
        base = base + last
    totals = lane_pairs(columns(jnp.broadcast_to(base, (NH, BLOCK)))[0:1, :], 1)
    for q in range(NH // 2):
        block = slice(q * 16, (q + 1) * 16)
        msg_ref[block, 0:8, :] = state[q].reshape(16, 8, 128).astype(BF16)
        left = totals[q]
        parts = []
        for _ in range(3):
            part = left.astype(BF16)
            parts.append(part.astype(F32))
            left = left - part.astype(F32)
        line = lax.broadcasted_iota(jnp.int32, (8, 128), 0)
        packed = jnp.where(line == 0, parts[0], jnp.where(line == 1, parts[1], parts[2]))
        packed = jnp.where(line < 3, packed, 0.0).astype(BF16)
        msg_ref[block, 8:16, :] = jnp.broadcast_to(packed[None], (16, 8, 128))


def run_state(x, b, rim, xt, bt, delta, extra, offset, speed):
    return pl.pallas_call(
        state_kernel,
        out_shape=(
            jax.ShapeDtypeStruct((ROWS, CH), BF16),
            jax.ShapeDtypeStruct((ROWS, STATE), BF16),
            jax.ShapeDtypeStruct((ROWS // BLOCK - 1, STATE, CH), BF16),
            jax.ShapeDtypeStruct((64, 16, 128), BF16),
        ),
        in_specs=[VMEM] * 9,
        out_specs=(VMEM,) * 4,
        scratch_shapes=[
            pltpu.VMEM((ROWS + 8, CH), F32),
            pltpu.VMEM((ROWS + 8, STATE), F32),
        ],
        name="local_state",
    )(x, b, rim, xt, bt, delta, extra, offset, speed)


def local_kernel(
    x_ref, b_ref, state_ref, c_ref, rim_ref, ct_ref, delta_ref, extra_ref, offset_ref, speed_ref,
    bypass_ref,
    y_ref, cact_ref, grow_ref,
    cpad,
):
    cpad[0:8, :] = rim_ref[:, CH + STATE : CH + 2 * STATE].astype(F32)
    cpad[8 : 8 + ROWS, :] = c_ref[...].astype(F32)
    step, fading = decays(delta_ref, extra_ref, offset_ref, speed_ref)
    bypass = lane_pairs(bypass_ref[...], 1)
    row = lax.broadcasted_iota(jnp.int32, (BLOCK, BLOCK), 0)
    col = lax.broadcasted_iota(jnp.int32, (BLOCK, BLOCK), 1)
    causal = row >= col
    low = col < HEAD_DIM
    base = jnp.zeros((NH, 1), F32)
    for i in range(ROWS // BLOCK):
        start = i * BLOCK
        rows = pl.ds(start, BLOCK)
        here = slice(start, start + BLOCK)
        cum = running_sum(fading[:, here])
        turned = columns(jnp.concatenate([cum, jnp.exp(cum), jnp.exp(base + cum)], axis=0))
        grow_ref[rows, :] = turned[:, 2 * NH : 3 * NH]
        grown = lane_pairs(turned[:, NH : 2 * NH], BLOCK)
        c_act = conv_at(cpad, ct_ref, start).astype(BF16)
        cact_ref[rows, :] = c_act
        affinity = dot_nt(c_act, b_ref[rows, :])
        for q in range(NH // 2):
            cols = slice(q * 128, (q + 1) * 128)
            x_here = x_ref[rows, cols]
            within = []
            for h in (2 * q, 2 * q + 1):
                between = turned[:, h : h + 1] - cum[h : h + 1, :]
                lag = jnp.exp(jnp.where(causal, between, NEG)) * step[h : h + 1, here]
                within.append(dot((affinity * lag).astype(BF16), x_here))
            total = jnp.where(low, within[0], within[1]) + bypass[q] * x_here.astype(F32)
            if i > 0:
                total = total + dot(c_act, state_ref[i - 1, :, cols]) * grown[q]
            y_ref[rows, cols] = total
        base = base + cum[:, BLOCK - 1 : BLOCK]


def run_local(x, b, states, c, rim, ct, delta, extra, offset, speed, bypass):
    return pl.pallas_call(
        local_kernel,
        out_shape=(
            jax.ShapeDtypeStruct((ROWS, CH), F32),
            jax.ShapeDtypeStruct((ROWS, STATE), BF16),
            jax.ShapeDtypeStruct((ROWS, NH), F32),
        ),
        in_specs=[VMEM] * 11,
        out_specs=(VMEM,) * 3,
        scratch_shapes=[pltpu.VMEM((ROWS + 8, STATE), F32)],
        name="local_mixer",
    )(x, b, states, c, rim, ct, delta, extra, offset, speed, bypass)


def prefix_kernel(in_ref, out_ref):
    entering = jnp.zeros((8, 128), F32)
    for j in range(64):
        out_ref[j] = entering.astype(BF16)
        piece = in_ref[j].astype(F32)
        total = piece[8:9, :] + piece[9:10, :] + piece[10:11, :]
        entering = entering * jnp.exp(total) + piece[0:8, :]


def run_prefix(received):
    return pl.pallas_call(
        prefix_kernel,
        out_shape=jax.ShapeDtypeStruct((64, 8, 128), BF16),
        in_specs=[VMEM],
        out_specs=VMEM,
        name="state_prefix",
    )(received)


def gate_kernel(y_ref, cact_ref, grow_ref, in_ref, valve_ref, scale_ref, out_l, out_r):
    for i in range(ROWS // BLOCK):
        rows = pl.ds(i * BLOCK, BLOCK)
        grown = lane_pairs(grow_ref[rows, :], BLOCK)
        c_act = cact_ref[rows, :]
        gated = []
        square = jnp.zeros((BLOCK, 1), F32)
        for q in range(NH // 2):
            cols = slice(q * 128, (q + 1) * 128)
            entering = in_ref[q * 16 : (q + 1) * 16].astype(F32).reshape(STATE, 128).astype(BF16)
            y = y_ref[rows, cols] + dot(c_act, entering) * grown[q]
            y = y * silu(valve_ref[rows, cols].astype(F32))
            gated.append(y)
            square = square + jnp.sum(y * y, axis=-1, keepdims=True)
        factor = lax.rsqrt(square * (1.0 / CH) + EPSILON)
        for q in range(NH // 2):
            cols = slice(q * 128, (q + 1) * 128)
            half = (out_l, out_r)[q // 2]
            half[rows, (q % 2) * 128 : (q % 2 + 1) * 128] = (
                gated[q] * factor * scale_ref[0:1, cols]
            ).astype(BF16)


def run_gate(y, cact, grow, entering, valve, scale):
    return pl.pallas_call(
        gate_kernel,
        out_shape=(jax.ShapeDtypeStruct((ROWS, HALFCH), BF16),) * 2,
        in_specs=[VMEM] * 6,
        out_specs=(VMEM,) * 2,
        name="gate_norm",
    )(y, cact, grow, entering, valve, scale)


RIM = 16
CHUNK = 512


def project_kernel(
    place_ref, scale_ref, own_w, near_w, far_w, across_w, near_x, far_x, across_x,
    own_l, own_r, near_l, near_r, far_l, far_r, across_l, across_r,
    own_res, near_res, far_res, across_res,
    out_ref, tail_ref,
    weight, acts, res, total, w_sems, a_sems, r_sems,
):
    core = place_ref[4]
    mine = pl.ds(pl.multiple_of(core * HALF, HALF), HALF)
    other = pl.ds(pl.multiple_of((1 - core) * HALF, HALF), HALF)
    started = []

    def start(source, target, sem):
        copy = pltpu.make_async_copy(source, target, sem)
        copy.start()
        return copy

    act_copies = []
    lefts = (own_l, near_l, far_l, across_l)
    rights = (own_r, near_r, far_r, across_r)
    for k in range(4):
        at = k * CH
        act_copies.append(start(lefts[k], acts.at[:, at : at + HALFCH], a_sems.at[2 * k]))
        act_copies.append(
            start(rights[k], acts.at[:, at + HALFCH : at + CH], a_sems.at[2 * k + 1])
        )
    for n in range(D // CHUNK):
        cols = slice(n * CHUNK, (n + 1) * CHUNK)
        started.append(start(own_w.at[:, cols], weight.at[0:CH, cols], w_sems.at[n]))
    for k, (first, second) in enumerate(((near_w, near_x), (far_w, far_x), (across_w, across_x))):
        block = slice((k + 1) * CH, (k + 2) * CH)
        started.append(start(first, weight.at[block, mine], w_sems.at[4 + 2 * k]))
        started.append(start(second, weight.at[block, other], w_sems.at[5 + 2 * k]))
    res_copies = []
    for k, source in enumerate((own_res, near_res, far_res, across_res)):
        rows = pl.ds(pl.multiple_of(place_ref[k] * QUARTER, QUARTER), QUARTER)
        res_copies.append(start(source, res.at[rows, :], r_sems.at[k]))
    for copy in act_copies + started:
        copy.wait()
    for n in range(D // CHUNK):
        cols = slice(n * CHUNK, (n + 1) * CHUNK)
        total[:, cols] = dot(acts[...], weight[:, cols])
    for copy in res_copies:
        copy.wait()
    for i in range(ROWS // 64):
        rows = slice(i * 64, (i + 1) * 64)
        values = total[rows, :] + ALPHA * res[rows, :].astype(F32)
        centred = values - jnp.sum(values, axis=-1, keepdims=True) * (1.0 / D)
        spread = jnp.sum(centred * centred, axis=-1, keepdims=True) * (1.0 / D)
        normed = (centred * lax.rsqrt(spread + EPSILON) * scale_ref[...]).astype(BF16)
        out_ref[rows, :] = normed
        if i == ROWS // 64 - 1:
            tail_ref[...] = normed[64 - RIM :, :]


def run_project(place, scale, weights, acts, residuals):
    return pl.pallas_call(
        project_kernel,
        out_shape=(
            jax.ShapeDtypeStruct((ROWS, D), BF16),
            jax.ShapeDtypeStruct((RIM, D), BF16),
        ),
        in_specs=[SMEM, VMEM] + [ANY] * 19,
        out_specs=(VMEM, VMEM),
        scratch_shapes=[
            pltpu.VMEM((D, D), BF16),
            pltpu.VMEM((ROWS, D), BF16),
            pltpu.VMEM((ROWS, D), BF16),
            pltpu.VMEM((ROWS, D), F32),
            pltpu.SemaphoreType.DMA((10,)),
            pltpu.SemaphoreType.DMA((8,)),
            pltpu.SemaphoreType.DMA((4,)),
        ],
        compiler_params=pltpu.CompilerParams(vmem_limit_bytes=48 * 1024 * 1024),
        name="project_norm",
    )(place, scale, *weights, *acts, *residuals)


TILES = FFL // 128
NARROW = 512


def down_copies(w_ref, down, sems):
    return [
        pltpu.make_async_copy(
            w_ref.at[n * NARROW : (n + 1) * NARROW, 2 * FFL : 3 * FFL],
            down.at[n * NARROW : (n + 1) * NARROW, :],
            sems.at[n],
        )
        for n in range(D // NARROW)
    ]


def two_quarters(hid, place_ref, half):
    def rows_of(k):
        return hid[pl.ds(pl.multiple_of(place_ref[half, k] * QUARTER, QUARTER), QUARTER), :]

    return jnp.concatenate([rows_of(0), rows_of(1)], axis=0)


def widen_kernel(
    sent_ref, gate_t, up_t, normed, rim, w_ref,
    hid_out, send_l, send_r,
    rows, wide, down, hid, gate_pad, up_pad, row_sems, wide_sems, down_sems, out_sem,
):
    row_copies = [
        pltpu.make_async_copy(rim, rows.at[0:RIM, :], row_sems.at[0]),
        pltpu.make_async_copy(normed, rows.at[RIM : RIM + ROWS, :], row_sems.at[1]),
    ]

    def wide_copies(j):
        at = j * 128
        if not isinstance(j, int):
            at = pl.multiple_of(at, 128)
        return (
            pltpu.make_async_copy(
                w_ref.at[:, pl.ds(at, 128)], wide.at[j, :, 0:128], wide_sems.at[j, 0]
            ),
            pltpu.make_async_copy(
                w_ref.at[:, pl.ds(FFL + at, 128)], wide.at[j, :, 128:256], wide_sems.at[j, 1]
            ),
        )

    downs = down_copies(w_ref, down, down_sems)
    for copy in row_copies:
        copy.start()
    for j in range(TILES):
        for copy in wide_copies(j):
            copy.start()
    for copy in downs:
        copy.start()
    for copy in row_copies:
        copy.wait()

    def conv(pad, taps, at):
        total = None
        for k in range(FCONV):
            tap = taps[k : k + 1, pl.ds(at, 128)].astype(F32)
            term = tap * pad[pl.ds(RIM - FCONV + 1 + k, ROWS), :]
            total = term if total is None else total + term
        return total

    def tile(j, carry):
        for copy in wide_copies(j):
            copy.wait()
        at = pl.multiple_of(j * 128, 128)
        both = dot(rows[...], wide[j]).astype(BF16).astype(F32)
        gate_pad[...] = both[:, 0:128]
        up_pad[...] = both[:, 128:256]
        hid[:, pl.ds(at, 128)] = (
            silu(conv(gate_pad, gate_t, at)) * conv(up_pad, up_t, at)
        ).astype(BF16)
        return carry

    lax.fori_loop(0, TILES, tile, 0)
    stored = pltpu.make_async_copy(hid, hid_out, out_sem)
    stored.start()
    for copy in downs:
        copy.wait()
    send_l[...] = dot_nt(two_quarters(hid, sent_ref, 0), down[0:HALF, :]).astype(BF16)
    send_r[...] = dot_nt(two_quarters(hid, sent_ref, 1), down[HALF:D, :]).astype(BF16)
    stored.wait()


def run_widen(sent, normed, rim, weights, gate_t, up_t):
    return pl.pallas_call(
        widen_kernel,
        out_shape=(
            jax.ShapeDtypeStruct((ROWS, FFL), BF16),
            jax.ShapeDtypeStruct((2 * QUARTER, HALF), BF16),
            jax.ShapeDtypeStruct((2 * QUARTER, HALF), BF16),
        ),
        in_specs=[SMEM, VMEM, VMEM, ANY, ANY, ANY],
        out_specs=(ANY, VMEM, VMEM),
        scratch_shapes=[
            pltpu.VMEM((ROWS + RIM, D), BF16),
            pltpu.VMEM((TILES, D, 256), BF16),
            pltpu.VMEM((D, FFL), BF16),
            pltpu.VMEM((ROWS, FFL), BF16),
            pltpu.VMEM((ROWS + RIM, 128), F32),
            pltpu.VMEM((ROWS + RIM, 128), F32),
            pltpu.SemaphoreType.DMA((2,)),
            pltpu.SemaphoreType.DMA((TILES, 2)),
            pltpu.SemaphoreType.DMA((D // NARROW,)),
            pltpu.SemaphoreType.DMA,
        ],
        compiler_params=pltpu.CompilerParams(vmem_limit_bytes=48 * 1024 * 1024),
        name="widen",
    )(sent, gate_t, up_t, normed, rim, weights)


def held_kernel(
    held_ref, hid_ref, w_ref, own_l, pass_l, own_r, pass_r, hid, down, hid_sem, down_sems
):
    copies = [pltpu.make_async_copy(hid_ref, hid, hid_sem)] + down_copies(w_ref, down, down_sems)
    for copy in copies:
        copy.start()
    for copy in copies:
        copy.wait()
    left = dot_nt(two_quarters(hid, held_ref, 0), down[0:HALF, :])
    own_l[...] = left[0:QUARTER, :]
    pass_l[...] = left[QUARTER:, :]
    right = dot_nt(two_quarters(hid, held_ref, 1), down[HALF:D, :])
    own_r[...] = right[0:QUARTER, :]
    pass_r[...] = right[QUARTER:, :]


def run_held(held, hidden, weights):
    return pl.pallas_call(
        held_kernel,
        out_shape=(jax.ShapeDtypeStruct((QUARTER, HALF), F32),) * 4,
        in_specs=[SMEM, ANY, ANY],
        out_specs=(VMEM,) * 4,
        scratch_shapes=[
            pltpu.VMEM((ROWS, FFL), BF16),
            pltpu.VMEM((D, FFL), BF16),
            pltpu.SemaphoreType.DMA,
            pltpu.SemaphoreType.DMA((D // NARROW,)),
        ],
        name="shrink_held",
    )(held, hidden, weights)


def add_kernel(pass_l, pass_r, once_l, once_r, out_l, out_r):
    out_l[...] = (pass_l[...] + once_l[...].astype(F32)).astype(BF16)
    out_r[...] = (pass_r[...] + once_r[...].astype(F32)).astype(BF16)


def run_add(passes, onces):
    step = QUARTER // 2
    block = pl.BlockSpec((step, HALF), lambda i: (i, 0))
    lower = pl.BlockSpec((step, HALF), lambda i: (i + 2, 0))
    return pl.pallas_call(
        add_kernel,
        grid=(2,),
        out_shape=(jax.ShapeDtypeStruct((QUARTER, HALF), BF16),) * 2,
        in_specs=[block, block, lower, lower],
        out_specs=(block, block),
        name="round_sum",
    )(*passes, *onces)


def last_norm_kernel(
    place_ref, own_l, own_r, once_l, once_r, twice_l, twice_r, res_ref, scale_ref, out_ref
):
    left = own_l[...] + once_l[...].astype(F32) + twice_l[...].astype(F32)
    right = own_r[...] + once_r[...].astype(F32) + twice_r[...].astype(F32)
    left = left + ALPHA * res_ref[:, 0:HALF].astype(F32)
    right = right + ALPHA * res_ref[:, HALF:D].astype(F32)
    mean = (jnp.sum(left, axis=-1, keepdims=True) + jnp.sum(right, axis=-1, keepdims=True)) * (
        1.0 / D
    )
    left = left - mean
    right = right - mean
    spread = (
        jnp.sum(left * left, axis=-1, keepdims=True)
        + jnp.sum(right * right, axis=-1, keepdims=True)
    ) * (1.0 / D)
    factor = lax.rsqrt(spread + EPSILON)
    out_ref[:, 0:HALF] = (left * factor * scale_ref[0:1, 0:HALF]).astype(BF16)
    out_ref[:, HALF:D] = (right * factor * scale_ref[0:1, HALF:D]).astype(BF16)


def run_last_norm(place, owns, onces, twices, normed, scale):
    step = QUARTER // 2
    block = pl.BlockSpec((step, HALF), lambda i, p: (i, 0))
    return pl.pallas_call(
        last_norm_kernel,
        grid_spec=pltpu.PrefetchScalarGridSpec(
            num_scalar_prefetch=1,
            grid=(2,),
            in_specs=[block] * 6
            + [
                pl.BlockSpec((step, D), lambda i, p: (2 * p[0] + i, 0)),
                pl.BlockSpec((1, D), lambda i, p: (0, 0)),
            ],
            out_specs=pl.BlockSpec((step, D), lambda i, p: (i, 0)),
        ),
        out_shape=jax.ShapeDtypeStruct((QUARTER, D), BF16),
        name="last_norm",
    )(place, *owns, *onces, *twices, normed, scale)


NEAR = [(0, 1), (1, 0), (2, 3), (3, 2)]
FAR = [(0, 3), (3, 0), (1, 2), (2, 1)]
ACROSS = [(0, 2), (2, 0), (1, 3), (3, 1)]


def with_near(part):
    return lax.ppermute(part, "tp", NEAR)


def with_far(part):
    return lax.ppermute(part, "tp", FAR)


def with_across(part):
    return lax.ppermute(part, "tp", ACROSS)


def with_core(part):
    return lax.ppermute(part, "sp_2", [(0, 1), (1, 0)])


def next_positions(shard):
    count = lax.axis_size(SP)
    return lax.ppermute(shard, SP, [(i, i + 1) for i in range(count - 1)])


def shards(
    incoming_residual_stream,
    result_valve,
    channel_feed_matrix,
    memory_feed_matrix,
    memory_query_matrix,
    unsoftened_deltas,
    delta_offset,
    channel_fading_speed,
    extra_log_fading,
    bypass_factor,
    channel_feed_kernel,
    memory_feed_kernel,
    memory_query_kernel,
    cluster_scaling_vector,
    mixer_result_matrix,
    initial_scaling_vector,
    valve_matrix,
    widen_matrix,
    shrink_matrix,
    valve_filter_kernel,
    widen_filter_kernel,
    latter_scaling_vector,
):
    own = lax.axis_index("tp").astype(jnp.int32)
    core = lax.axis_index("sp_2").astype(jnp.int32)
    near = own ^ 1
    far = 3 - own
    across = own ^ 2
    place = jnp.stack([own, near, far, across, core])
    sent = jnp.stack([jnp.stack([near, across]), jnp.stack([far, across])])
    held = jnp.stack([jnp.stack([own, far]), jnp.stack([own, near])])

    weights = lax.all_gather(
        jnp.concatenate([valve_matrix, widen_matrix, shrink_matrix.T], axis=1), SP, tiled=True
    )

    rim = next_positions(run_rim(channel_feed_matrix, memory_feed_matrix, memory_query_matrix))
    drives = (
        unsoftened_deltas.T,
        extra_log_fading.T,
        delta_offset.reshape(1, NH),
        channel_fading_speed.reshape(1, NH),
    )
    x_act, b_act, states, message = run_state(
        channel_feed_matrix,
        memory_feed_matrix,
        rim,
        channel_feed_kernel,
        memory_feed_kernel,
        *drives,
    )
    received = lax.all_to_all(message, SP, 0, 0, tiled=True)

    w_half = lax.dynamic_slice(mixer_result_matrix, (0, core * HALF), (CH, HALF))
    w_mine = (with_near(w_half), with_far(w_half), with_across(w_half))
    w_other = tuple(with_core(part) for part in w_mine)
    residuals = (
        incoming_residual_stream,
        with_near(incoming_residual_stream),
        with_far(incoming_residual_stream),
        with_across(incoming_residual_stream),
    )

    y_local, c_act, grow = run_local(
        x_act,
        b_act,
        states,
        memory_query_matrix,
        rim,
        memory_query_kernel,
        *drives,
        bypass_factor.reshape(1, NH),
    )
    entering = lax.all_to_all(run_prefix(received), SP, 0, 0, tiled=True)
    y_l, y_r = run_gate(
        y_local, c_act, grow, entering, result_valve, cluster_scaling_vector.reshape(1, CH)
    )
    far_l = with_far(y_l)
    near_r = with_near(y_r)
    near_l = with_near(y_l)
    far_r = with_far(y_r)
    across_l = with_near(far_l)
    across_r = with_far(near_r)
    normed, tail = run_project(
        place,
        initial_scaling_vector.reshape(1, D),
        (mixer_result_matrix, *w_mine, *w_other),
        (y_l, y_r, near_l, near_r, far_l, far_r, across_l, across_r),
        residuals,
    )
    hidden, send_l, send_r = run_widen(
        sent, normed, next_positions(tail), weights, valve_filter_kernel, widen_filter_kernel
    )
    onces = (with_near(send_l), with_far(send_r))
    own_l, pass_l, own_r, pass_r = run_held(held, hidden, weights)
    on_l, on_r = run_add((pass_l, pass_r), onces)
    twices = (with_far(on_l), with_near(on_r))
    return run_last_norm(
        place, (own_l, own_r), onces, twices, normed, latter_scaling_vector.reshape(1, D)
    )


def solution(mesh):
    split = Mesh(mesh.devices.reshape(8, 4, 2, mesh.shape["tp"]), ("sp_0", "sp_1", "sp_2", "tp"))
    in_specs = (
        P(SP_TP, None),
        P(SP, "tp"),
        P(SP, "tp"),
        P(SP, "tp"),
        P(SP, "tp"),
        P(SP, "tp"),
        P("tp"),
        P("tp"),
        P(SP, "tp"),
        P("tp"),
        P(None, "tp"),
        P(None, "tp"),
        P(None, "tp"),
        P("tp"),
        P("tp", None),
        P(),
        P(SP, "tp"),
        P(SP, "tp"),
        P("tp", SP),
        P(None, "tp"),
        P(None, "tp"),
        P(),
    )
    out_specs = P(SP_TP, None)
    return jax.shard_map(
        shards, mesh=split, in_specs=in_specs, out_specs=out_specs, check_vma=False
    )
```

```python
import jax
import jax.numpy as jnp
from jax import lax
from jax.experimental import pallas as pl
from jax.experimental.pallas import tpu as pltpu
from jax.sharding import Mesh
from jax.sharding import PartitionSpec as P

HEAD_DIM = 64
STATE = 128
CONV = 4
FCONV = 3
BLOCK = 128
SP = ("sp_0", "sp_1", "sp_2")
SP_TP = ("sp_0", "sp_1", "sp_2", "tp")

EPSILON = 1e-05
ALPHA = 2.0**0.25
F32 = jnp.float32
BF16 = jnp.bfloat16
NEG = -1e30

ROWS = 512
CH = 512
NH = 8
QUARTER = 128
HALFCH = 256
D = 2048
HALF = 1024
FFL = 1408

VMEM = pl.BlockSpec(memory_space=pltpu.VMEM)
SMEM = pl.BlockSpec(memory_space=pltpu.SMEM)
ANY = pl.BlockSpec(memory_space=pl.ANY)
HIGHEST = lax.Precision.HIGHEST
MIB = 1024 * 1024


def limit(mib):
    return pltpu.CompilerParams(vmem_limit_bytes=mib * MIB)


def close(value):
    return pltpu.with_memory_space_constraint(value, pltpu.VMEM)


def close_out(shape, kind):
    return pltpu.VMEM(shape, kind)


def away(*values):
    return tuple(pltpu.with_memory_space_constraint(value, pltpu.HBM) for value in values)


def away_out(shape, kind):
    return pltpu.HBM(shape, kind)


def dot(a, b):
    return jnp.dot(a, b, preferred_element_type=F32)


def dot_nt(a, b, precision=None):
    return lax.dot_general(
        a, b, (((1,), (1,)), ((), ())), precision=precision, preferred_element_type=F32
    )


def silu(v):
    return v / (1.0 + jnp.exp(-v))


def lane_pairs(column_of, rows):
    low = lax.broadcasted_iota(jnp.int32, (rows, 128), 1) < HEAD_DIM
    slabs = []
    for q in range(NH // 2):
        first = jnp.broadcast_to(column_of[:, 2 * q : 2 * q + 1], (rows, 128))
        second = jnp.broadcast_to(column_of[:, 2 * q + 1 : 2 * q + 2], (rows, 128))
        slabs.append(jnp.where(low, first, second))
    return slabs


def eye(n):
    line = lax.broadcasted_iota(jnp.int32, (n, n), 0)
    lane = lax.broadcasted_iota(jnp.int32, (n, n), 1)
    return jnp.where(line == lane, 1.0, 0.0).astype(F32)


def columns(rows):
    return dot_nt(eye(BLOCK), rows, precision=HIGHEST)


def down_column(ref):
    return jnp.sum(eye(NH) * ref[...], axis=1, keepdims=True)


def decays(delta, extra, offset, speed):
    step_in = delta + offset
    step = jnp.maximum(step_in, 0.0) + jnp.log1p(jnp.exp(-jnp.abs(step_in)))
    return step, extra - speed * step


def running_sum(fading):
    line = lax.broadcasted_iota(jnp.int32, (BLOCK, BLOCK), 0)
    lane = lax.broadcasted_iota(jnp.int32, (BLOCK, BLOCK), 1)
    upper = jnp.where(line <= lane, 1.0, 0.0).astype(F32)
    return jnp.dot(fading, upper, precision=HIGHEST, preferred_element_type=F32)


def conv_at(pad, taps, start):
    total = None
    for k in range(CONV):
        term = taps[k : k + 1, :].astype(F32) * pad[pl.ds(start + 8 - CONV + 1 + k, BLOCK), :]
        total = term if total is None else total + term
    return silu(total)


def conv_next(pad, taps, block):
    pad[8 : 8 + BLOCK, :] = block.astype(F32)
    total = None
    for k in range(CONV):
        term = taps[k : k + 1, :].astype(F32) * pad[pl.ds(8 - CONV + 1 + k, BLOCK), :]
        total = term if total is None else total + term
    pad[0:8, :] = pad[BLOCK : BLOCK + 8, :]
    return silu(total)


def rim_kernel(x_ref, b_ref, c_ref, out_ref):
    out_ref[:, 0:CH] = x_ref[...]
    out_ref[:, CH : CH + STATE] = b_ref[...]
    out_ref[:, CH + STATE : CH + 2 * STATE] = c_ref[...]


def run_rim(x, b, c):
    last = lambda width: pl.BlockSpec((8, width), lambda i: (ROWS // 8 - 1, 0))
    return pl.pallas_call(
        rim_kernel,
        grid=(1,),
        out_shape=close_out((8, CH + 2 * STATE), BF16),
        in_specs=[last(CH), last(STATE), last(STATE)],
        out_specs=pl.BlockSpec((8, CH + 2 * STATE), lambda i: (0, 0)),
        name="rim",
    )(*away(x, b, c))


def state_kernel(
    x_ref, b_ref, rim_ref, xt_ref, bt_ref, delta_ref, extra_ref, offset_ref, speed_ref,
    x_out, b_out, state_out, msg_ref,
    xpad, bpad,
):
    xpad[0:8, :] = rim_ref[:, 0:CH].astype(F32)
    bpad[0:8, :] = rim_ref[:, CH : CH + STATE].astype(F32)
    xpad[8 : 8 + ROWS, :] = x_ref[...].astype(F32)
    bpad[8 : 8 + ROWS, :] = b_ref[...].astype(F32)
    step, fading = decays(
        delta_ref[...], extra_ref[...], down_column(offset_ref), down_column(speed_ref)
    )
    state = [jnp.zeros((STATE, 128), F32) for _ in range(NH // 2)]
    base = jnp.zeros((NH, 1), F32)
    for i in range(ROWS // BLOCK):
        start = i * BLOCK
        rows = pl.ds(start, BLOCK)
        here = slice(start, start + BLOCK)
        cum = running_sum(fading[:, here])
        last = cum[:, BLOCK - 1 : BLOCK]
        to_end = lane_pairs(columns(step[:, here] * jnp.exp(last - cum)), BLOCK)
        kept = lane_pairs(columns(jnp.broadcast_to(jnp.exp(last), (NH, BLOCK)))[0:1, :], 1)
        x_act = conv_at(xpad, xt_ref, start).astype(BF16)
        b_act = conv_at(bpad, bt_ref, start).astype(BF16)
        x_out[rows, :] = x_act
        b_out[rows, :] = b_act
        b_turned = b_act.astype(F32).T.astype(BF16)
        for q in range(NH // 2):
            cols = slice(q * 128, (q + 1) * 128)
            fresh = dot(b_turned, (x_act[:, cols].astype(F32) * to_end[q]).astype(BF16))
            state[q] = fresh if i == 0 else state[q] * kept[q] + fresh
            if i < ROWS // BLOCK - 1:
                state_out[i, :, cols] = state[q].astype(BF16)
        base = base + last
    totals = lane_pairs(columns(jnp.broadcast_to(base, (NH, BLOCK)))[0:1, :], 1)
    for q in range(NH // 2):
        block = slice(q * 16, (q + 1) * 16)
        msg_ref[block, 0:8, :] = state[q].reshape(16, 8, 128).astype(BF16)
        left = totals[q]
        parts = []
        for _ in range(3):
            part = left.astype(BF16)
            parts.append(part.astype(F32))
            left = left - part.astype(F32)
        line = lax.broadcasted_iota(jnp.int32, (8, 128), 0)
        packed = jnp.where(line == 0, parts[0], jnp.where(line == 1, parts[1], parts[2]))
        packed = jnp.where(line < 3, packed, 0.0).astype(BF16)
        msg_ref[block, 8:16, :] = jnp.broadcast_to(packed[None], (16, 8, 128))


def run_state(x, b, rim, xt, bt, delta, extra, offset, speed):
    return pl.pallas_call(
        state_kernel,
        out_shape=(
            away_out((ROWS, CH), BF16),
            away_out((ROWS, STATE), BF16),
            away_out((ROWS // BLOCK - 1, STATE, CH), BF16),
            close_out((64, 16, 128), BF16),
        ),
        compiler_params=limit(24),
        in_specs=[VMEM] * 9,
        out_specs=(VMEM,) * 4,
        scratch_shapes=[
            pltpu.VMEM((ROWS + 8, CH), F32),
            pltpu.VMEM((ROWS + 8, STATE), F32),
        ],
        name="local_state",
    )(*away(x, b), close(rim), *away(xt, bt, delta, extra, offset, speed))


def local_kernel(
    x_ref, b_ref, state_ref, c_ref, rim_ref, ct_ref, delta_ref, extra_ref, offset_ref, speed_ref,
    bypass_ref,
    y_ref, cact_ref, grow_ref,
    cpad,
):
    cpad[0:8, :] = rim_ref[:, CH + STATE : CH + 2 * STATE].astype(F32)
    offset = down_column(offset_ref)
    speed = down_column(speed_ref)
    bypass = lane_pairs(bypass_ref[...], 1)
    row = lax.broadcasted_iota(jnp.int32, (BLOCK, BLOCK), 0)
    col = lax.broadcasted_iota(jnp.int32, (BLOCK, BLOCK), 1)
    causal = row >= col
    low = col < HEAD_DIM

    def block_step(i, base):
        rows = pl.ds(pl.multiple_of(i * BLOCK, BLOCK), BLOCK)
        step, fading = decays(delta_ref[:, rows], extra_ref[:, rows], offset, speed)
        cum = running_sum(fading)
        turned = columns(jnp.concatenate([cum, jnp.exp(cum), jnp.exp(base + cum)], axis=0))
        grow_ref[rows, :] = turned[:, 2 * NH : 3 * NH]
        grown = lane_pairs(turned[:, NH : 2 * NH], BLOCK)
        c_act = conv_next(cpad, ct_ref, c_ref[rows, :]).astype(BF16)
        cact_ref[rows, :] = c_act
        affinity = dot_nt(c_act, b_ref[rows, :])
        for q in range(NH // 2):
            cols = slice(q * 128, (q + 1) * 128)
            x_here = x_ref[rows, cols]
            within = []
            for h in (2 * q, 2 * q + 1):
                between = turned[:, h : h + 1] - cum[h : h + 1, :]
                lag = jnp.exp(jnp.where(causal, between, NEG)) * step[h : h + 1, :]
                within.append(dot((affinity * lag).astype(BF16), x_here))
            total = jnp.where(low, within[0], within[1]) + bypass[q] * x_here.astype(F32)
            carried = dot(c_act, state_ref[jnp.maximum(i - 1, 0), :, cols]) * grown[q]
            y_ref[rows, cols] = total + jnp.where(i > 0, carried, 0.0)
        return base + cum[:, BLOCK - 1 : BLOCK]

    lax.fori_loop(0, ROWS // BLOCK, block_step, jnp.zeros((NH, 1), F32))


def run_local(x, b, states, c, rim, ct, delta, extra, offset, speed, bypass):
    return pl.pallas_call(
        local_kernel,
        out_shape=(
            away_out((ROWS, CH), F32),
            away_out((ROWS, STATE), BF16),
            away_out((ROWS, NH), F32),
        ),
        compiler_params=limit(24),
        in_specs=[VMEM] * 11,
        out_specs=(VMEM,) * 3,
        scratch_shapes=[pltpu.VMEM((BLOCK + 8, STATE), F32)],
        name="local_mixer",
    )(*away(x, b, states, c), close(rim), *away(ct, delta, extra, offset, speed, bypass))


def prefix_kernel(in_ref, out_ref):
    entering = jnp.zeros((8, 128), F32)
    for j in range(64):
        out_ref[j] = entering.astype(BF16)
        piece = in_ref[j].astype(F32)
        total = piece[8:9, :] + piece[9:10, :] + piece[10:11, :]
        entering = entering * jnp.exp(total) + piece[0:8, :]


def run_prefix(received):
    return pl.pallas_call(
        prefix_kernel,
        out_shape=close_out((64, 8, 128), BF16),
        compiler_params=limit(8),
        in_specs=[VMEM],
        out_specs=VMEM,
        name="state_prefix",
    )(close(received))


def gate_kernel(y_ref, cact_ref, grow_ref, in_ref, valve_ref, scale_ref, out_l, out_r, tail_ref):
    for i in range(ROWS // BLOCK):
        rows = pl.ds(i * BLOCK, BLOCK)
        grown = lane_pairs(grow_ref[rows, :], BLOCK)
        c_act = cact_ref[rows, :]
        gated = []
        square = jnp.zeros((BLOCK, 1), F32)
        for q in range(NH // 2):
            cols = slice(q * 128, (q + 1) * 128)
            entering = in_ref[q * 16 : (q + 1) * 16].astype(F32).reshape(STATE, 128).astype(BF16)
            y = y_ref[rows, cols] + dot(c_act, entering) * grown[q]
            y = y * silu(valve_ref[rows, cols].astype(F32))
            gated.append(y)
            square = square + jnp.sum(y * y, axis=-1, keepdims=True)
        factor = lax.rsqrt(square * (1.0 / CH) + EPSILON)
        for q in range(NH // 2):
            cols = slice(q * 128, (q + 1) * 128)
            half = (out_l, out_r)[q // 2]
            done = (gated[q] * factor * scale_ref[0:1, cols]).astype(BF16)
            half[rows, (q % 2) * 128 : (q % 2 + 1) * 128] = done
            if i == ROWS // BLOCK - 1:
                tail_ref[:, cols] = done[BLOCK - RIM :, :]


def run_gate(y, cact, grow, entering, valve, scale):
    return pl.pallas_call(
        gate_kernel,
        out_shape=(
            away_out((ROWS, HALFCH), BF16),
            away_out((ROWS, HALFCH), BF16),
            away_out((RIM, CH), BF16),
        ),
        compiler_params=limit(16),
        in_specs=[VMEM] * 6,
        out_specs=(VMEM,) * 3,
        name="gate_norm",
    )(*away(y, cact, grow), close(entering), *away(valve, scale))


RIM = 16
CHUNK = 512


def project_kernel(
    place_ref, scale_ref, near_l, far_r, across_l, across_r,
    own_l, own_r, near_r, far_l, own_t, near_t, far_t, across_t, res_t, own_w, near_w, far_w, across_w, other_w,
    own_res, near_res, far_res, across_res,
    out_ref,
    weight, early, tails, tail_res, res, total, w_sems, e_sems, t_sems, r_sems,
):
    core = place_ref[4]
    columns_of = (
        pl.ds(pl.multiple_of(core * HALF, HALF), HALF),
        pl.ds(pl.multiple_of((1 - core) * HALF, HALF), HALF),
    )
    others = [other_w.at[k * CH : (k + 1) * CH, :] for k in range(3)]
    arrived = ((near_w, far_w, across_w), others)
    copies = ([], [])
    for half in range(2):
        sources = (own_w.at[:, columns_of[half]], *arrived[half])
        for k, source in enumerate(sources):
            target = weight.at[half, k * CH : (k + 1) * CH, :]
            copies[half].append(pltpu.make_async_copy(source, target, w_sems.at[half, k]))
    res_copies = []
    for k, source in enumerate((own_res, near_res, far_res, across_res)):
        rows = pl.ds(pl.multiple_of(place_ref[k] * QUARTER, QUARTER), QUARTER)
        res_copies.append(pltpu.make_async_copy(source, res.at[rows, :], r_sems.at[k]))
    early_copies = [
        pltpu.make_async_copy(source, early.at[k], e_sems.at[k])
        for k, source in enumerate((own_l, own_r, near_r, far_l))
    ]
    early_copies += [
        pltpu.make_async_copy(source, tails.at[k], t_sems.at[k])
        for k, source in enumerate((own_t, near_t, far_t, across_t))
    ]
    early_copies.append(pltpu.make_async_copy(res_t, tail_res, t_sems.at[4]))
    acts = (early.at[0], early.at[1], near_l, early.at[2], early.at[3], far_r, across_l, across_r)
    for copy in early_copies + copies[0]:
        copy.start()
    for copy in early_copies + copies[0]:
        copy.wait()
    for copy in copies[1] + res_copies:
        copy.start()
    for half in range(2):
        if half == 1:
            for copy in copies[1]:
                copy.wait()
        for n in range(HALF // CHUNK):
            cols = slice(n * CHUNK, (n + 1) * CHUNK)
            part = None
            for k, act in enumerate(acts):
                side = slice((k % 2) * HALFCH, (k % 2 + 1) * HALFCH)
                lhs = jnp.concatenate([tails[k // 2, :, side], act[...]], axis=0)
                term = dot(lhs, weight[half, k * HALFCH : (k + 1) * HALFCH, cols])
                part = term if part is None else part + term
            start = pl.multiple_of((core if half == 0 else 1 - core) * HALF + n * CHUNK, CHUNK)
            total[:, pl.ds(start, CHUNK)] = part
    for copy in res_copies:
        copy.wait()

    def norm(values):
        centred = values - jnp.sum(values, axis=-1, keepdims=True) * (1.0 / D)
        spread = jnp.sum(centred * centred, axis=-1, keepdims=True) * (1.0 / D)
        return (centred * lax.rsqrt(spread + EPSILON) * scale_ref[...]).astype(BF16)

    out_ref[0:RIM, :] = norm(total[0:RIM, :] + ALPHA * tail_res[...].astype(F32))

    def norm_rows(i, carry):
        rows = pl.ds(pl.multiple_of(i * 64, 64), 64)
        shifted = pl.ds(pl.multiple_of(RIM + i * 64, 16), 64)
        out_ref[shifted, :] = norm(total[shifted, :] + ALPHA * res[rows, :].astype(F32))
        return carry

    lax.fori_loop(0, ROWS // 64, norm_rows, 0)


def run_project(place, scale, weights, acts, tails, residuals):
    return pl.pallas_call(
        project_kernel,
        out_shape=close_out((RIM + ROWS, D), BF16),
        in_specs=[SMEM] + [VMEM] * 5 + [ANY] * 18,
        out_specs=VMEM,
        scratch_shapes=[
            pltpu.VMEM((2, D, HALF), BF16),
            pltpu.VMEM((4, ROWS, HALFCH), BF16),
            pltpu.VMEM((4, RIM, CH), BF16),
            pltpu.VMEM((RIM, D), BF16),
            pltpu.VMEM((ROWS, D), BF16),
            pltpu.VMEM((RIM + ROWS, D), F32),
            pltpu.SemaphoreType.DMA((2, 4)),
            pltpu.SemaphoreType.DMA((4,)),
            pltpu.SemaphoreType.DMA((5,)),
            pltpu.SemaphoreType.DMA((4,)),
        ],
        compiler_params=limit(30),
        name="project_norm",
    )(
        place,
        *away(scale),
        *[close(acts[k]) for k in (2, 5, 6, 7)],
        *away(*[acts[k] for k in (0, 1, 3, 4)], *tails, *weights, *residuals),
    )


TILES = FFL // 128
NARROW = 512


def down_copies(w_ref, down, sems):
    return [
        pltpu.make_async_copy(
            w_ref.at[n * NARROW : (n + 1) * NARROW, 2 * FFL : 3 * FFL],
            down.at[n * NARROW : (n + 1) * NARROW, :],
            sems.at[n],
        )
        for n in range(D // NARROW)
    ]


def two_quarters(hid, place_ref, half):
    def rows_of(k):
        return hid[pl.ds(pl.multiple_of(place_ref[half, k] * QUARTER, QUARTER), QUARTER), :]

    return jnp.concatenate([rows_of(0), rows_of(1)], axis=0)


AHEAD = 4
STRIP = 512


def widen_kernel(
    sent_ref, gate_t, up_t, rows, w_ref,
    hid, down, send_l, send_r,
    wide, gate_pad, up_pad, wide_sems, down_sems,
):
    def wide_copies(j):
        at = j * 128
        if not isinstance(j, int):
            at = pl.multiple_of(at, 128)
        return (
            pltpu.make_async_copy(
                w_ref.at[:, pl.ds(at, 128)], wide.at[j, :, 0:128], wide_sems.at[j, 0]
            ),
            pltpu.make_async_copy(
                w_ref.at[:, pl.ds(FFL + at, 128)], wide.at[j, :, 128:256], wide_sems.at[j, 1]
            ),
        )

    downs = down_copies(w_ref, down, down_sems)
    for j in range(AHEAD):
        for copy in wide_copies(j):
            copy.start()

    def conv(pad, taps, at):
        total = None
        for k in range(FCONV):
            tap = taps[k : k + 1, pl.ds(at, 128)].astype(F32)
            term = tap * pad[pl.ds(RIM - FCONV + 1 + k, ROWS), :]
            total = term if total is None else total + term
        return total

    def tile(j, carry):
        for copy in wide_copies(j):
            copy.wait()

        @pl.when(j + AHEAD < TILES)
        def _():
            for copy in wide_copies(j + AHEAD):
                copy.start()

        @pl.when(j + AHEAD == TILES)
        def _():
            for copy in downs:
                copy.start()

        at = pl.multiple_of(j * 128, 128)
        both = dot(rows[...], wide[j]).astype(BF16).astype(F32)
        gate_pad[...] = both[:, 0:128]
        up_pad[...] = both[:, 128:256]
        hid[:, pl.ds(at, 128)] = (
            silu(conv(gate_pad, gate_t, at)) * conv(up_pad, up_t, at)
        ).astype(BF16)
        return carry

    lax.fori_loop(0, TILES, tile, 0)
    for copy in downs:
        copy.wait()
    send_l[...] = dot_nt(two_quarters(hid, sent_ref, 0), down[0:STRIP, :]).astype(BF16)
    send_r[...] = dot_nt(two_quarters(hid, sent_ref, 1), down[HALF : HALF + STRIP, :]).astype(BF16)


def run_widen(sent, rows, weights, gate_t, up_t):
    return pl.pallas_call(
        widen_kernel,
        out_shape=(
            close_out((ROWS, FFL), BF16),
            close_out((D, FFL), BF16),
            close_out((2 * QUARTER, STRIP), BF16),
            close_out((2 * QUARTER, STRIP), BF16),
        ),
        in_specs=[SMEM, VMEM, VMEM, VMEM, ANY],
        out_specs=(VMEM,) * 4,
        scratch_shapes=[
            pltpu.VMEM((TILES, D, 256), BF16),
            pltpu.VMEM((ROWS + RIM, 128), F32),
            pltpu.VMEM((ROWS + RIM, 128), F32),
            pltpu.SemaphoreType.DMA((TILES, 2)),
            pltpu.SemaphoreType.DMA((D // NARROW,)),
        ],
        compiler_params=limit(24),
        name="widen",
    )(sent, *away(gate_t, up_t), close(rows), *away(weights))


def sent_kernel(sent_ref, hid, down, send_l, send_r):
    send_l[...] = dot_nt(two_quarters(hid, sent_ref, 0), down[STRIP:HALF, :]).astype(BF16)
    send_r[...] = dot_nt(two_quarters(hid, sent_ref, 1), down[HALF + STRIP : D, :]).astype(BF16)


def run_sent(sent, hidden, down):
    return pl.pallas_call(
        sent_kernel,
        out_shape=(close_out((2 * QUARTER, STRIP), BF16),) * 2,
        in_specs=[SMEM, VMEM, VMEM],
        out_specs=(VMEM,) * 2,
        compiler_params=limit(8),
        name="shrink_sent",
    )(sent, close(hidden), close(down))


def held_kernel(held_ref, hid, down, own, pass_1, pass_2):
    for half in range(2):
        both = dot_nt(two_quarters(hid, held_ref, half), down[half * HALF : (half + 1) * HALF, :])
        own[:, half * HALF : (half + 1) * HALF] = both[0:QUARTER, :]
        pass_1[:, half * STRIP : (half + 1) * STRIP] = both[QUARTER:, 0:STRIP]
        pass_2[:, half * STRIP : (half + 1) * STRIP] = both[QUARTER:, STRIP:HALF]


def run_held(held, hidden, down):
    return pl.pallas_call(
        held_kernel,
        out_shape=(
            close_out((QUARTER, D), F32),
            close_out((QUARTER, HALF), F32),
            close_out((QUARTER, HALF), F32),
        ),
        in_specs=[SMEM, VMEM, VMEM],
        out_specs=(VMEM,) * 3,
        compiler_params=limit(8),
        name="shrink_held",
    )(held, close(hidden), close(down))


def add_kernel(passed, once_l, once_r, out_l, out_r):
    out_l[...] = (passed[:, 0:STRIP] + once_l[QUARTER:, :].astype(F32)).astype(BF16)
    out_r[...] = (passed[:, STRIP:] + once_r[QUARTER:, :].astype(F32)).astype(BF16)


def run_add(passed, once_l, once_r):
    return pl.pallas_call(
        add_kernel,
        out_shape=(close_out((QUARTER, STRIP), BF16),) * 2,
        in_specs=[VMEM] * 3,
        out_specs=(VMEM,) * 2,
        compiler_params=limit(8),
        name="round_sum",
    )(close(passed), close(once_l), close(once_r))


def last_norm_kernel(place_ref, own, l_1, r_1, l_2, r_2, ll_1, rr_1, ll_2, rr_2, res_ref, scale_ref, out_ref):
    for i in range(2):
        rows = slice(i * 64, (i + 1) * 64)
        kept = pl.ds(pl.multiple_of(RIM + place_ref[0] * QUARTER + i * 64, 16), 64)
        parts = []
        for k, (once, twice) in enumerate(((l_1, ll_1), (l_2, ll_2), (r_1, rr_1), (r_2, rr_2))):
            cols = slice(k * STRIP, (k + 1) * STRIP)
            part = own[rows, cols] + once[rows, :].astype(F32) + twice[rows, :].astype(F32)
            parts.append(part + ALPHA * res_ref[kept, cols].astype(F32))
        values = jnp.concatenate(parts, axis=1)
        centred = values - jnp.sum(values, axis=-1, keepdims=True) * (1.0 / D)
        spread = jnp.sum(centred * centred, axis=-1, keepdims=True) * (1.0 / D)
        out_ref[rows, :] = (centred * lax.rsqrt(spread + EPSILON) * scale_ref[...]).astype(BF16)


def run_last_norm(place, own, onces, twices, rows, scale):
    kept = [close(part) for part in (own, *onces, *twices, rows)]
    return pl.pallas_call(
        last_norm_kernel,
        out_shape=jax.ShapeDtypeStruct((QUARTER, D), BF16),
        in_specs=[SMEM] + [VMEM] * 11,
        out_specs=VMEM,
        compiler_params=limit(8),
        name="last_norm",
    )(place, *kept, *away(scale))


NEAR = [(0, 1), (1, 0), (2, 3), (3, 2)]
FAR = [(0, 3), (3, 0), (1, 2), (2, 1)]


def with_near(part):
    return lax.ppermute(part, "tp", NEAR)


def with_far(part):
    return lax.ppermute(part, "tp", FAR)


def forwarded(far_part, near_part):
    part = jnp.where(lax.axis_index("sp_2") == 0, far_part, near_part)
    pairs = [(i, j) for i, j in NEAR] + [(4 + i, 4 + j) for i, j in FAR]
    return lax.ppermute(part, ("sp_2", "tp"), pairs)


def with_core(part):
    return lax.ppermute(part, "sp_2", [(0, 1), (1, 0)])


def next_positions(shard):
    count = lax.axis_size(SP)
    return lax.ppermute(shard, SP, [(i, i + 1) for i in range(count - 1)])


def shards(
    incoming_residual_stream,
    result_valve,
    channel_feed_matrix,
    memory_feed_matrix,
    memory_query_matrix,
    unsoftened_deltas,
    delta_offset,
    channel_fading_speed,
    extra_log_fading,
    bypass_factor,
    channel_feed_kernel,
    memory_feed_kernel,
    memory_query_kernel,
    cluster_scaling_vector,
    mixer_result_matrix,
    initial_scaling_vector,
    valve_matrix,
    widen_matrix,
    shrink_matrix,
    valve_filter_kernel,
    widen_filter_kernel,
    latter_scaling_vector,
):
    own = lax.axis_index("tp").astype(jnp.int32)
    core = lax.axis_index("sp_2").astype(jnp.int32)
    near = own ^ 1
    far = 3 - own
    across = own ^ 2
    place = jnp.stack([own, near, far, across, core])
    sent = jnp.stack([jnp.stack([near, across]), jnp.stack([far, across])])
    held = jnp.stack([jnp.stack([own, far]), jnp.stack([own, near])])

    weights = lax.all_gather(
        jnp.concatenate([valve_matrix, widen_matrix, shrink_matrix.T], axis=1), SP, tiled=True
    )

    rim = run_rim(channel_feed_matrix, memory_feed_matrix, memory_query_matrix)
    _, projection, residual = lax.optimization_barrier(
        (rim, mixer_result_matrix, incoming_residual_stream)
    )
    rim = next_positions(rim)
    drives = (
        unsoftened_deltas.T,
        extra_log_fading.T,
        delta_offset.reshape(1, NH),
        channel_fading_speed.reshape(1, NH),
    )
    x_act, b_act, states, message = run_state(
        channel_feed_matrix,
        memory_feed_matrix,
        rim,
        channel_feed_kernel,
        memory_feed_kernel,
        *drives,
    )
    received = lax.all_to_all(message, SP, 0, 0, tiled=True)

    w_half = lax.dynamic_slice(projection, (0, core * HALF), (CH, HALF))
    w_near = with_near(w_half)
    w_far = with_far(w_half)
    res_near = with_near(residual)
    res_far = with_far(residual)

    y_local, c_act, grow = run_local(
        x_act,
        b_act,
        states,
        memory_query_matrix,
        rim,
        memory_query_kernel,
        *drives,
        bypass_factor.reshape(1, NH),
    )
    prefix = run_prefix(received)
    entering = lax.all_to_all(prefix, SP, 0, 0, tiled=True)
    late = lax.optimization_barrier((y_local, w_near, w_far, res_near, res_far))
    w_across = forwarded(late[2], late[1])
    res_across = forwarded(late[4], late[3])
    y_l, y_r, tail = run_gate(
        y_local, c_act, grow, entering, result_valve, cluster_scaling_vector.reshape(1, CH)
    )
    swap = lax.optimization_barrier((w_near, w_far, w_across, y_l))[:3]
    w_other = with_core(jnp.concatenate(swap, axis=0))
    tail_own = next_positions(tail)
    far_l = with_far(y_l)
    near_r = with_near(y_r)
    near_l = with_near(y_l)
    far_r = with_far(y_r)
    tail_near = with_near(tail_own)
    tail_far = with_far(tail_own)
    tail_across = forwarded(tail_far, tail_near)
    ends = [
        jnp.where(at == 3, part[QUARTER - RIM :], jnp.zeros((RIM, D), BF16))
        for at, part in ((own, residual), (near, res_near), (far, res_far), (across, res_across))
    ]
    res_tail = next_positions(ends[0] + ends[1] + ends[2] + ends[3])
    across_l = with_near(far_l)
    across_r = with_far(near_r)
    rows = run_project(
        place,
        initial_scaling_vector.reshape(1, D),
        (mixer_result_matrix, w_near, w_far, w_across, w_other),
        (y_l, y_r, near_l, near_r, far_l, far_r, across_l, across_r),
        (tail_own, tail_near, tail_far, tail_across, res_tail),
        (residual, res_near, res_far, res_across),
    )
    hidden, down, send_l1, send_r1 = run_widen(
        sent, rows, weights, valve_filter_kernel, widen_filter_kernel
    )
    l_1 = with_near(send_l1)
    r_1 = with_far(send_r1)
    send_l2, send_r2 = run_sent(sent, hidden, down)
    l_2 = with_near(send_l2)
    r_2 = with_far(send_r2)
    kept, pass_1, pass_2 = run_held(held, hidden, down)
    on_l1, on_r1 = run_add(pass_1, l_1, r_1)
    ll_1 = with_far(on_l1)
    rr_1 = with_near(on_r1)
    on_l2, on_r2 = run_add(pass_2, l_2, r_2)
    ll_2 = with_far(on_l2)
    rr_2 = with_near(on_r2)
    return run_last_norm(
        place,
        kept,
        (l_1, r_1, l_2, r_2),
        (ll_1, rr_1, ll_2, rr_2),
        rows,
        latter_scaling_vector.reshape(1, D),
    )


def solution(mesh):
    split = Mesh(mesh.devices.reshape(8, 4, 2, mesh.shape["tp"]), ("sp_0", "sp_1", "sp_2", "tp"))
    in_specs = (
        P(SP_TP, None),
        P(SP, "tp"),
        P(SP, "tp"),
        P(SP, "tp"),
        P(SP, "tp"),
        P(SP, "tp"),
        P("tp"),
        P("tp"),
        P(SP, "tp"),
        P("tp"),
        P(None, "tp"),
        P(None, "tp"),
        P(None, "tp"),
        P("tp"),
        P("tp", None),
        P(),
        P(SP, "tp"),
        P(SP, "tp"),
        P("tp", SP),
        P(None, "tp"),
        P(None, "tp"),
        P(),
    )
    out_specs = P(SP_TP, None)

    return jax.shard_map(
        shards, mesh=split, in_specs=in_specs, out_specs=out_specs, check_vma=False
    )
```

```python
import jax
import jax.numpy as jnp
from jax import lax
from jax.experimental import pallas as pl
from jax.experimental.pallas import tpu as pltpu
from jax.sharding import Mesh
from jax.sharding import PartitionSpec as P

HEAD_DIM = 64
STATE = 128
CONV = 4
FCONV = 3
BLOCK = 128
SP = ("sp_0", "sp_1", "sp_2")
SP_TP = ("sp_0", "sp_1", "sp_2", "tp")

EPSILON = 1e-05
ALPHA = 2.0**0.25
F32 = jnp.float32
BF16 = jnp.bfloat16
NEG = -1e30

ROWS = 512
CH = 512
NH = 8
QUARTER = 128
HALFCH = 256
D = 2048
HALF = 1024
FFL = 1408

VMEM = pl.BlockSpec(memory_space=pltpu.VMEM)
SMEM = pl.BlockSpec(memory_space=pltpu.SMEM)
ANY = pl.BlockSpec(memory_space=pl.ANY)
HIGHEST = lax.Precision.HIGHEST
MIB = 1024 * 1024


def limit(mib):
    return pltpu.CompilerParams(vmem_limit_bytes=mib * MIB)


def close(value):
    return pltpu.with_memory_space_constraint(value, pltpu.VMEM)


def close_out(shape, kind):
    return pltpu.VMEM(shape, kind)


def away(*values):
    return tuple(pltpu.with_memory_space_constraint(value, pltpu.HBM) for value in values)


def away_out(shape, kind):
    return pltpu.HBM(shape, kind)


def dot(a, b):
    return jnp.dot(a, b, preferred_element_type=F32)


def dot_nt(a, b, precision=None):
    return lax.dot_general(
        a, b, (((1,), (1,)), ((), ())), precision=precision, preferred_element_type=F32
    )


def silu(v):
    return v / (1.0 + jnp.exp(-v))


def lane_pairs(column_of, rows):
    low = lax.broadcasted_iota(jnp.int32, (rows, 128), 1) < HEAD_DIM
    slabs = []
    for q in range(NH // 2):
        first = jnp.broadcast_to(column_of[:, 2 * q : 2 * q + 1], (rows, 128))
        second = jnp.broadcast_to(column_of[:, 2 * q + 1 : 2 * q + 2], (rows, 128))
        slabs.append(jnp.where(low, first, second))
    return slabs


def eye(n):
    line = lax.broadcasted_iota(jnp.int32, (n, n), 0)
    lane = lax.broadcasted_iota(jnp.int32, (n, n), 1)
    return jnp.where(line == lane, 1.0, 0.0).astype(F32)


def columns(rows):
    return dot_nt(eye(BLOCK), rows, precision=HIGHEST)


def down_column(ref):
    return jnp.sum(eye(NH) * ref[...], axis=1, keepdims=True)


def decays(delta, extra, offset, speed):
    step_in = delta + offset
    step = jnp.maximum(step_in, 0.0) + jnp.log1p(jnp.exp(-jnp.abs(step_in)))
    return step, extra - speed * step


def running_sum(fading):
    line = lax.broadcasted_iota(jnp.int32, (BLOCK, BLOCK), 0)
    lane = lax.broadcasted_iota(jnp.int32, (BLOCK, BLOCK), 1)
    upper = jnp.where(line <= lane, 1.0, 0.0).astype(F32)
    return jnp.dot(fading, upper, precision=HIGHEST, preferred_element_type=F32)


def conv_at(pad, taps, start):
    total = None
    for k in range(CONV):
        term = taps[k : k + 1, :].astype(F32) * pad[pl.ds(start + 8 - CONV + 1 + k, BLOCK), :]
        total = term if total is None else total + term
    return silu(total)


def conv_next(pad, taps, block):
    pad[8 : 8 + BLOCK, :] = block.astype(F32)
    total = None
    for k in range(CONV):
        term = taps[k : k + 1, :].astype(F32) * pad[pl.ds(8 - CONV + 1 + k, BLOCK), :]
        total = term if total is None else total + term
    pad[0:8, :] = pad[BLOCK : BLOCK + 8, :]
    return silu(total)


def rim_kernel(x_ref, b_ref, c_ref, out_ref):
    out_ref[:, 0:CH] = x_ref[...]
    out_ref[:, CH : CH + STATE] = b_ref[...]
    out_ref[:, CH + STATE : CH + 2 * STATE] = c_ref[...]


def run_rim(x, b, c):
    last = lambda width: pl.BlockSpec((8, width), lambda i: (ROWS // 8 - 1, 0))
    return pl.pallas_call(
        rim_kernel,
        grid=(1,),
        out_shape=close_out((8, CH + 2 * STATE), BF16),
        in_specs=[last(CH), last(STATE), last(STATE)],
        out_specs=pl.BlockSpec((8, CH + 2 * STATE), lambda i: (0, 0)),
        name="rim",
    )(*away(x, b, c))


def state_kernel(
    x_ref, b_ref, rim_ref, xt_ref, bt_ref, delta_ref, extra_ref, offset_ref, speed_ref,
    x_out, b_out, state_out, msg_ref,
    xpad, bpad,
):
    xpad[0:8, :] = rim_ref[:, 0:CH].astype(F32)
    bpad[0:8, :] = rim_ref[:, CH : CH + STATE].astype(F32)
    xpad[8 : 8 + ROWS, :] = x_ref[...].astype(F32)
    bpad[8 : 8 + ROWS, :] = b_ref[...].astype(F32)
    step, fading = decays(
        delta_ref[...], extra_ref[...], down_column(offset_ref), down_column(speed_ref)
    )
    state = [jnp.zeros((STATE, 128), F32) for _ in range(NH // 2)]
    base = jnp.zeros((NH, 1), F32)
    for i in range(ROWS // BLOCK):
        start = i * BLOCK
        rows = pl.ds(start, BLOCK)
        here = slice(start, start + BLOCK)
        cum = running_sum(fading[:, here])
        last = cum[:, BLOCK - 1 : BLOCK]
        to_end = lane_pairs(columns(step[:, here] * jnp.exp(last - cum)), BLOCK)
        kept = lane_pairs(columns(jnp.broadcast_to(jnp.exp(last), (NH, BLOCK)))[0:1, :], 1)
        x_act = conv_at(xpad, xt_ref, start).astype(BF16)
        b_act = conv_at(bpad, bt_ref, start).astype(BF16)
        x_out[rows, :] = x_act
        b_out[rows, :] = b_act
        b_turned = b_act.astype(F32).T.astype(BF16)
        for q in range(NH // 2):
            cols = slice(q * 128, (q + 1) * 128)
            fresh = dot(b_turned, (x_act[:, cols].astype(F32) * to_end[q]).astype(BF16))
            state[q] = fresh if i == 0 else state[q] * kept[q] + fresh
            if i < ROWS // BLOCK - 1:
                state_out[i, :, cols] = state[q].astype(BF16)
        base = base + last
    totals = lane_pairs(columns(jnp.broadcast_to(base, (NH, BLOCK)))[0:1, :], 1)
    for q in range(NH // 2):
        block = slice(q * 16, (q + 1) * 16)
        msg_ref[block, 0:8, :] = state[q].reshape(16, 8, 128).astype(BF16)
        left = totals[q]
        parts = []
        for _ in range(3):
            part = left.astype(BF16)
            parts.append(part.astype(F32))
            left = left - part.astype(F32)
        line = lax.broadcasted_iota(jnp.int32, (8, 128), 0)
        packed = jnp.where(line == 0, parts[0], jnp.where(line == 1, parts[1], parts[2]))
        packed = jnp.where(line < 3, packed, 0.0).astype(BF16)
        msg_ref[block, 8:16, :] = jnp.broadcast_to(packed[None], (16, 8, 128))


def run_state(x, b, rim, xt, bt, delta, extra, offset, speed):
    return pl.pallas_call(
        state_kernel,
        out_shape=(
            away_out((ROWS, CH), BF16),
            away_out((ROWS, STATE), BF16),
            away_out((ROWS // BLOCK - 1, STATE, CH), BF16),
            close_out((64, 16, 128), BF16),
        ),
        compiler_params=limit(24),
        in_specs=[VMEM] * 9,
        out_specs=(VMEM,) * 4,
        scratch_shapes=[
            pltpu.VMEM((ROWS + 8, CH), F32),
            pltpu.VMEM((ROWS + 8, STATE), F32),
        ],
        name="local_state",
    )(*away(x, b), close(rim), *away(xt, bt, delta, extra, offset, speed))


def local_kernel(
    x_ref, b_ref, state_ref, c_ref, rim_ref, ct_ref, delta_ref, extra_ref, offset_ref, speed_ref,
    bypass_ref,
    y_ref, cact_ref, grow_ref,
    cpad,
):
    cpad[0:8, :] = rim_ref[:, CH + STATE : CH + 2 * STATE].astype(F32)
    offset = down_column(offset_ref)
    speed = down_column(speed_ref)
    bypass = lane_pairs(bypass_ref[...], 1)
    row = lax.broadcasted_iota(jnp.int32, (BLOCK, BLOCK), 0)
    col = lax.broadcasted_iota(jnp.int32, (BLOCK, BLOCK), 1)
    causal = row >= col
    low = col < HEAD_DIM

    def block_step(i, base):
        rows = pl.ds(pl.multiple_of(i * BLOCK, BLOCK), BLOCK)
        step, fading = decays(delta_ref[:, rows], extra_ref[:, rows], offset, speed)
        cum = running_sum(fading)
        turned = columns(jnp.concatenate([cum, jnp.exp(cum), jnp.exp(base + cum)], axis=0))
        grow_ref[rows, :] = turned[:, 2 * NH : 3 * NH]
        grown = lane_pairs(turned[:, NH : 2 * NH], BLOCK)
        c_act = conv_next(cpad, ct_ref, c_ref[rows, :]).astype(BF16)
        cact_ref[rows, :] = c_act
        affinity = dot_nt(c_act, b_ref[rows, :])
        for q in range(NH // 2):
            cols = slice(q * 128, (q + 1) * 128)
            x_here = x_ref[rows, cols]
            within = []
            for h in (2 * q, 2 * q + 1):
                between = turned[:, h : h + 1] - cum[h : h + 1, :]
                lag = jnp.exp(jnp.where(causal, between, NEG)) * step[h : h + 1, :]
                within.append(dot((affinity * lag).astype(BF16), x_here))
            total = jnp.where(low, within[0], within[1]) + bypass[q] * x_here.astype(F32)
            carried = dot(c_act, state_ref[jnp.maximum(i - 1, 0), :, cols]) * grown[q]
            y_ref[rows, cols] = total + jnp.where(i > 0, carried, 0.0)
        return base + cum[:, BLOCK - 1 : BLOCK]

    lax.fori_loop(0, ROWS // BLOCK, block_step, jnp.zeros((NH, 1), F32))


def run_local(x, b, states, c, rim, ct, delta, extra, offset, speed, bypass):
    return pl.pallas_call(
        local_kernel,
        out_shape=(
            away_out((ROWS, CH), F32),
            away_out((ROWS, STATE), BF16),
            away_out((ROWS, NH), F32),
        ),
        compiler_params=limit(24),
        in_specs=[VMEM] * 11,
        out_specs=(VMEM,) * 3,
        scratch_shapes=[pltpu.VMEM((BLOCK + 8, STATE), F32)],
        name="local_mixer",
    )(*away(x, b, states, c), close(rim), *away(ct, delta, extra, offset, speed, bypass))


def prefix_kernel(in_ref, out_ref):
    entering = jnp.zeros((8, 128), F32)
    for j in range(64):
        out_ref[j] = entering.astype(BF16)
        piece = in_ref[j].astype(F32)
        total = piece[8:9, :] + piece[9:10, :] + piece[10:11, :]
        entering = entering * jnp.exp(total) + piece[0:8, :]


def run_prefix(received):
    return pl.pallas_call(
        prefix_kernel,
        out_shape=close_out((64, 8, 128), BF16),
        compiler_params=limit(8),
        in_specs=[VMEM],
        out_specs=VMEM,
        name="state_prefix",
    )(close(received))


def gate_kernel(y_ref, cact_ref, grow_ref, in_ref, valve_ref, scale_ref, out_l, out_r):
    for i in range(ROWS // BLOCK):
        rows = pl.ds(i * BLOCK, BLOCK)
        grown = lane_pairs(grow_ref[rows, :], BLOCK)
        c_act = cact_ref[rows, :]
        gated = []
        square = jnp.zeros((BLOCK, 1), F32)
        for q in range(NH // 2):
            cols = slice(q * 128, (q + 1) * 128)
            entering = in_ref[q * 16 : (q + 1) * 16].astype(F32).reshape(STATE, 128).astype(BF16)
            y = y_ref[rows, cols] + dot(c_act, entering) * grown[q]
            y = y * silu(valve_ref[rows, cols].astype(F32))
            gated.append(y)
            square = square + jnp.sum(y * y, axis=-1, keepdims=True)
        factor = lax.rsqrt(square * (1.0 / CH) + EPSILON)
        for q in range(NH // 2):
            cols = slice(q * 128, (q + 1) * 128)
            half = (out_l, out_r)[q // 2]
            half[rows, (q % 2) * 128 : (q % 2 + 1) * 128] = (
                gated[q] * factor * scale_ref[0:1, cols]
            ).astype(BF16)


def run_gate(y, cact, grow, entering, valve, scale):
    return pl.pallas_call(
        gate_kernel,
        out_shape=(
            away_out((ROWS, HALFCH), BF16),
            away_out((ROWS, HALFCH), BF16),
        ),
        compiler_params=limit(16),
        in_specs=[VMEM] * 6,
        out_specs=(VMEM,) * 2,
        name="gate_norm",
    )(*away(y, cact, grow), close(entering), *away(valve, scale))


RIM = 16
CHUNK = 512


def project_kernel(
    place_ref, scale_ref, near_l, far_r, across_l, across_r,
    own_l, own_r, near_r, far_l, own_w, near_w, far_w, across_w, near_x, far_x, across_x,
    own_res, near_res, far_res, across_res,
    out_ref, tail_ref,
    weight, early, res, total, w_sems, e_sems, r_sems,
):
    core = place_ref[4]
    columns_of = (
        pl.ds(pl.multiple_of(core * HALF, HALF), HALF),
        pl.ds(pl.multiple_of((1 - core) * HALF, HALF), HALF),
    )
    arrived = ((near_w, far_w, across_w), (near_x, far_x, across_x))
    copies = ([], [])
    for half in range(2):
        sources = (own_w.at[:, columns_of[half]], *arrived[half])
        for k, source in enumerate(sources):
            target = weight.at[half, k * CH : (k + 1) * CH, :]
            copies[half].append(pltpu.make_async_copy(source, target, w_sems.at[half, k]))
    res_copies = []
    for k, source in enumerate((own_res, near_res, far_res, across_res)):
        rows = pl.ds(pl.multiple_of(place_ref[k] * QUARTER, QUARTER), QUARTER)
        res_copies.append(pltpu.make_async_copy(source, res.at[rows, :], r_sems.at[k]))
    early_copies = [
        pltpu.make_async_copy(source, early.at[k], e_sems.at[k])
        for k, source in enumerate((own_l, own_r, near_r, far_l))
    ]
    acts = (early.at[0], early.at[1], near_l, early.at[2], early.at[3], far_r, across_l, across_r)
    for copy in early_copies + copies[0]:
        copy.start()
    for copy in early_copies + copies[0]:
        copy.wait()
    for copy in copies[1] + res_copies:
        copy.start()
    for half in range(2):
        if half == 1:
            for copy in copies[1]:
                copy.wait()
        for n in range(HALF // CHUNK):
            cols = slice(n * CHUNK, (n + 1) * CHUNK)
            part = None
            for k, act in enumerate(acts):
                term = dot(act[...], weight[half, k * HALFCH : (k + 1) * HALFCH, cols])
                part = term if part is None else part + term
            start = pl.multiple_of((core if half == 0 else 1 - core) * HALF + n * CHUNK, CHUNK)
            total[:, pl.ds(start, CHUNK)] = part
    for copy in res_copies:
        copy.wait()

    def norm(values):
        centred = values - jnp.sum(values, axis=-1, keepdims=True) * (1.0 / D)
        spread = jnp.sum(centred * centred, axis=-1, keepdims=True) * (1.0 / D)
        return (centred * lax.rsqrt(spread + EPSILON) * scale_ref[...]).astype(BF16)


    def norm_rows(i, carry):
        rows = pl.ds(pl.multiple_of(i * 64, 64), 64)
        out_ref[rows, :] = norm(total[rows, :] + ALPHA * res[rows, :].astype(F32))
        return carry

    lax.fori_loop(0, ROWS // 64, norm_rows, 0)
    tail_ref[...] = out_ref[ROWS - RIM : ROWS, :]


def run_project(place, scale, weights, acts, residuals):
    return pl.pallas_call(
        project_kernel,
        out_shape=(close_out((ROWS, D), BF16), close_out((RIM, D), BF16)),
        in_specs=[SMEM] + [VMEM] * 5 + [ANY] * 15,
        out_specs=(VMEM, VMEM),
        scratch_shapes=[
            pltpu.VMEM((2, D, HALF), BF16),
            pltpu.VMEM((4, ROWS, HALFCH), BF16),
            pltpu.VMEM((ROWS, D), BF16),
            pltpu.VMEM((ROWS, D), F32),
            pltpu.SemaphoreType.DMA((2, 4)),
            pltpu.SemaphoreType.DMA((4,)),
            pltpu.SemaphoreType.DMA((4,)),
        ],
        compiler_params=limit(30),
        name="project_norm",
    )(
        place,
        *away(scale),
        *[close(acts[k]) for k in (2, 5, 6, 7)],
        *away(*[acts[k] for k in (0, 1, 3, 4)], *weights, *residuals),
    )


TILES = FFL // 128
NARROW = 512


def down_copies(w_ref, down, sems):
    return [
        pltpu.make_async_copy(
            w_ref.at[n * NARROW : (n + 1) * NARROW, 2 * FFL : 3 * FFL],
            down.at[n * NARROW : (n + 1) * NARROW, :],
            sems.at[n],
        )
        for n in range(D // NARROW)
    ]


def two_quarters(hid, place_ref, half):
    def rows_of(k):
        return hid[pl.ds(pl.multiple_of(place_ref[half, k] * QUARTER, QUARTER), QUARTER), :]

    return jnp.concatenate([rows_of(0), rows_of(1)], axis=0)


AHEAD = 4
STRIP = 512


def widen_kernel(
    sent_ref, gate_t, up_t, normed, rim, w_ref,
    hid, down, send_l, send_r,
    wide, gate_pad, up_pad, wide_sems, down_sems,
):
    def wide_copies(j):
        at = j * 128
        if not isinstance(j, int):
            at = pl.multiple_of(at, 128)
        return (
            pltpu.make_async_copy(
                w_ref.at[:, pl.ds(at, 128)], wide.at[j, :, 0:128], wide_sems.at[j, 0]
            ),
            pltpu.make_async_copy(
                w_ref.at[:, pl.ds(FFL + at, 128)], wide.at[j, :, 128:256], wide_sems.at[j, 1]
            ),
        )

    downs = down_copies(w_ref, down, down_sems)
    for j in range(AHEAD):
        for copy in wide_copies(j):
            copy.start()

    def conv(pad, taps, at):
        total = None
        for k in range(FCONV):
            tap = taps[k : k + 1, pl.ds(at, 128)].astype(F32)
            term = tap * pad[pl.ds(RIM - FCONV + 1 + k, ROWS), :]
            total = term if total is None else total + term
        return total

    def tile(j, carry):
        for copy in wide_copies(j):
            copy.wait()

        @pl.when(j + AHEAD < TILES)
        def _():
            for copy in wide_copies(j + AHEAD):
                copy.start()

        @pl.when(j + AHEAD == TILES)
        def _():
            for copy in downs:
                copy.start()

        at = pl.multiple_of(j * 128, 128)
        rows = jnp.concatenate([rim[...], normed[...]], axis=0)
        both = dot(rows, wide[j]).astype(BF16).astype(F32)
        gate_pad[...] = both[:, 0:128]
        up_pad[...] = both[:, 128:256]
        hid[:, pl.ds(at, 128)] = (
            silu(conv(gate_pad, gate_t, at)) * conv(up_pad, up_t, at)
        ).astype(BF16)
        return carry

    lax.fori_loop(0, TILES, tile, 0)
    for copy in downs:
        copy.wait()
    send_l[...] = dot_nt(two_quarters(hid, sent_ref, 0), down[0:STRIP, :]).astype(BF16)
    send_r[...] = dot_nt(two_quarters(hid, sent_ref, 1), down[HALF : HALF + STRIP, :]).astype(BF16)


def run_widen(sent, normed, rim, weights, gate_t, up_t):
    return pl.pallas_call(
        widen_kernel,
        out_shape=(
            close_out((ROWS, FFL), BF16),
            close_out((D, FFL), BF16),
            close_out((2 * QUARTER, STRIP), BF16),
            close_out((2 * QUARTER, STRIP), BF16),
        ),
        in_specs=[SMEM, VMEM, VMEM, VMEM, VMEM, ANY],
        out_specs=(VMEM,) * 4,
        scratch_shapes=[
            pltpu.VMEM((TILES, D, 256), BF16),
            pltpu.VMEM((ROWS + RIM, 128), F32),
            pltpu.VMEM((ROWS + RIM, 128), F32),
            pltpu.SemaphoreType.DMA((TILES, 2)),
            pltpu.SemaphoreType.DMA((D // NARROW,)),
        ],
        compiler_params=limit(24),
        name="widen",
    )(sent, *away(gate_t, up_t), close(normed), close(rim), *away(weights))


def sent_kernel(sent_ref, hid, down, send_l, send_r):
    send_l[...] = dot_nt(two_quarters(hid, sent_ref, 0), down[STRIP:HALF, :]).astype(BF16)
    send_r[...] = dot_nt(two_quarters(hid, sent_ref, 1), down[HALF + STRIP : D, :]).astype(BF16)


def run_sent(sent, hidden, down):
    return pl.pallas_call(
        sent_kernel,
        out_shape=(close_out((2 * QUARTER, STRIP), BF16),) * 2,
        in_specs=[SMEM, VMEM, VMEM],
        out_specs=(VMEM,) * 2,
        compiler_params=limit(8),
        name="shrink_sent",
    )(sent, close(hidden), close(down))


def held_kernel(held_ref, hid, down, own, pass_1, pass_2):
    for half in range(2):
        both = dot_nt(two_quarters(hid, held_ref, half), down[half * HALF : (half + 1) * HALF, :])
        own[:, half * HALF : (half + 1) * HALF] = both[0:QUARTER, :]
        pass_1[:, half * STRIP : (half + 1) * STRIP] = both[QUARTER:, 0:STRIP]
        pass_2[:, half * STRIP : (half + 1) * STRIP] = both[QUARTER:, STRIP:HALF]


def run_held(held, hidden, down):
    return pl.pallas_call(
        held_kernel,
        out_shape=(
            close_out((QUARTER, D), F32),
            close_out((QUARTER, HALF), F32),
            close_out((QUARTER, HALF), F32),
        ),
        in_specs=[SMEM, VMEM, VMEM],
        out_specs=(VMEM,) * 3,
        compiler_params=limit(8),
        name="shrink_held",
    )(held, close(hidden), close(down))


def add_kernel(passed, once_l, once_r, out_l, out_r):
    out_l[...] = (passed[:, 0:STRIP] + once_l[QUARTER:, :].astype(F32)).astype(BF16)
    out_r[...] = (passed[:, STRIP:] + once_r[QUARTER:, :].astype(F32)).astype(BF16)


def run_add(passed, once_l, once_r):
    return pl.pallas_call(
        add_kernel,
        out_shape=(close_out((QUARTER, STRIP), BF16),) * 2,
        in_specs=[VMEM] * 3,
        out_specs=(VMEM,) * 2,
        compiler_params=limit(8),
        name="round_sum",
    )(close(passed), close(once_l), close(once_r))


def last_norm_kernel(
    place_ref, own, l_1, r_1, l_2, r_2, ll_1, rr_1, ll_2, rr_2, res_ref, scale_ref, out_ref
):
    for i in range(2):
        rows = slice(i * 64, (i + 1) * 64)
        kept = pl.ds(pl.multiple_of(place_ref[0] * QUARTER + i * 64, 64), 64)
        parts = []
        for k, (once, twice) in enumerate(((l_1, ll_1), (l_2, ll_2), (r_1, rr_1), (r_2, rr_2))):
            cols = slice(k * STRIP, (k + 1) * STRIP)
            part = own[rows, cols] + once[rows, :].astype(F32) + twice[rows, :].astype(F32)
            parts.append(part + ALPHA * res_ref[kept, cols].astype(F32))
        values = jnp.concatenate(parts, axis=1)
        centred = values - jnp.sum(values, axis=-1, keepdims=True) * (1.0 / D)
        spread = jnp.sum(centred * centred, axis=-1, keepdims=True) * (1.0 / D)
        out_ref[rows, :] = (centred * lax.rsqrt(spread + EPSILON) * scale_ref[...]).astype(BF16)


def run_last_norm(place, own, onces, twices, rows, scale):
    kept = [close(part) for part in (own, *onces, *twices, rows)]
    return pl.pallas_call(
        last_norm_kernel,
        out_shape=jax.ShapeDtypeStruct((QUARTER, D), BF16),
        in_specs=[SMEM] + [VMEM] * 11,
        out_specs=VMEM,
        compiler_params=limit(8),
        name="last_norm",
    )(place, *kept, *away(scale))


NEAR = [(0, 1), (1, 0), (2, 3), (3, 2)]
FAR = [(0, 3), (3, 0), (1, 2), (2, 1)]


def with_near(part):
    return lax.ppermute(part, "tp", NEAR)


def with_far(part):
    return lax.ppermute(part, "tp", FAR)


def forwarded(far_part, near_part):
    part = jnp.where(lax.axis_index("sp_2") == 0, far_part, near_part)
    pairs = [(i, j) for i, j in NEAR] + [(4 + i, 4 + j) for i, j in FAR]
    return lax.ppermute(part, ("sp_2", "tp"), pairs)


def with_core(part):
    return lax.ppermute(part, "sp_2", [(0, 1), (1, 0)])


def next_positions(shard):
    count = lax.axis_size(SP)
    return lax.ppermute(shard, SP, [(i, i + 1) for i in range(count - 1)])


def shards(
    incoming_residual_stream,
    result_valve,
    channel_feed_matrix,
    memory_feed_matrix,
    memory_query_matrix,
    unsoftened_deltas,
    delta_offset,
    channel_fading_speed,
    extra_log_fading,
    bypass_factor,
    channel_feed_kernel,
    memory_feed_kernel,
    memory_query_kernel,
    cluster_scaling_vector,
    mixer_result_matrix,
    initial_scaling_vector,
    valve_matrix,
    widen_matrix,
    shrink_matrix,
    valve_filter_kernel,
    widen_filter_kernel,
    latter_scaling_vector,
):
    own = lax.axis_index("tp").astype(jnp.int32)
    core = lax.axis_index("sp_2").astype(jnp.int32)
    near = own ^ 1
    far = 3 - own
    across = own ^ 2
    place = jnp.stack([own, near, far, across, core])
    sent = jnp.stack([jnp.stack([near, across]), jnp.stack([far, across])])
    held = jnp.stack([jnp.stack([own, far]), jnp.stack([own, near])])

    weights = lax.all_gather(
        jnp.concatenate([valve_matrix, widen_matrix, shrink_matrix.T], axis=1), SP, tiled=True
    )

    rim = run_rim(channel_feed_matrix, memory_feed_matrix, memory_query_matrix)
    _, projection, residual = lax.optimization_barrier(
        (rim, mixer_result_matrix, incoming_residual_stream)
    )
    rim = next_positions(rim)
    drives = (
        unsoftened_deltas.T,
        extra_log_fading.T,
        delta_offset.reshape(1, NH),
        channel_fading_speed.reshape(1, NH),
    )
    x_act, b_act, states, message = run_state(
        channel_feed_matrix,
        memory_feed_matrix,
        rim,
        channel_feed_kernel,
        memory_feed_kernel,
        *drives,
    )
    received = lax.all_to_all(message, SP, 0, 0, tiled=True)

    w_half = lax.dynamic_slice(projection, (0, core * HALF), (CH, HALF))
    w_near = with_near(w_half)
    w_far = with_far(w_half)
    res_near = with_near(residual)
    res_far = with_far(residual)

    y_local, c_act, grow = run_local(
        x_act,
        b_act,
        states,
        memory_query_matrix,
        rim,
        memory_query_kernel,
        *drives,
        bypass_factor.reshape(1, NH),
    )
    prefix = run_prefix(received)
    entering = lax.all_to_all(prefix, SP, 0, 0, tiled=True)
    _, late_near, late_far = lax.optimization_barrier((y_local, w_near, w_far))
    w_across = forwarded(late_far, late_near)
    _, late_near, late_far = lax.optimization_barrier((prefix, res_near, res_far))
    res_across = forwarded(late_far, late_near)
    y_l, y_r = run_gate(
        y_local, c_act, grow, entering, result_valve, cluster_scaling_vector.reshape(1, CH)
    )
    swap = lax.optimization_barrier((prefix, w_near, w_far))[1:]
    w_other = (
        with_core(swap[0]),
        with_core(swap[1]),
        with_core(lax.optimization_barrier((y_l, w_across))[1]),
    )
    far_l = with_far(y_l)
    near_r = with_near(y_r)
    near_l = with_near(y_l)
    far_r = with_far(y_r)
    across_l = with_near(far_l)
    across_r = with_far(near_r)
    normed, tail = run_project(
        place,
        initial_scaling_vector.reshape(1, D),
        (mixer_result_matrix, w_near, w_far, w_across, *w_other),
        (y_l, y_r, near_l, near_r, far_l, far_r, across_l, across_r),
        (residual, res_near, res_far, res_across),
    )
    hidden, down, send_l1, send_r1 = run_widen(
        sent, normed, next_positions(tail), weights, valve_filter_kernel, widen_filter_kernel
    )
    l_1 = with_near(send_l1)
    r_1 = with_far(send_r1)
    send_l2, send_r2 = run_sent(sent, hidden, down)
    l_2 = with_near(send_l2)
    r_2 = with_far(send_r2)
    kept, pass_1, pass_2 = run_held(held, hidden, down)
    on_l1, on_r1 = run_add(pass_1, l_1, r_1)
    ll_1 = with_far(on_l1)
    rr_1 = with_near(on_r1)
    on_l2, on_r2 = run_add(pass_2, l_2, r_2)
    ll_2 = with_far(on_l2)
    rr_2 = with_near(on_r2)
    return run_last_norm(
        place,
        kept,
        (l_1, r_1, l_2, r_2),
        (ll_1, rr_1, ll_2, rr_2),
        normed,
        latter_scaling_vector.reshape(1, D),
    )


def solution(mesh):
    split = Mesh(mesh.devices.reshape(8, 4, 2, mesh.shape["tp"]), ("sp_0", "sp_1", "sp_2", "tp"))
    in_specs = (
        P(SP_TP, None),
        P(SP, "tp"),
        P(SP, "tp"),
        P(SP, "tp"),
        P(SP, "tp"),
        P(SP, "tp"),
        P("tp"),
        P("tp"),
        P(SP, "tp"),
        P("tp"),
        P(None, "tp"),
        P(None, "tp"),
        P(None, "tp"),
        P("tp"),
        P("tp", None),
        P(),
        P(SP, "tp"),
        P(SP, "tp"),
        P("tp", SP),
        P(None, "tp"),
        P(None, "tp"),
        P(),
    )
    out_specs = P(SP_TP, None)

    return jax.shard_map(
        shards, mesh=split, in_specs=in_specs, out_specs=out_specs, check_vma=False
    )
```

```python
import jax
import jax.numpy as jnp
from jax import lax
from jax.experimental import pallas as pl
from jax.experimental.pallas import tpu as pltpu
from jax.sharding import Mesh
from jax.sharding import PartitionSpec as P

HEAD_DIM = 64
STATE = 128
CONV = 4
FCONV = 3
BLOCK = 128
SP = ("sp_0", "sp_1", "sp_2")
SP_TP = ("sp_0", "sp_1", "sp_2", "tp")

EPSILON = 1e-05
ALPHA = 2.0**0.25
F32 = jnp.float32
BF16 = jnp.bfloat16
NEG = -1e30

ROWS = 512
CH = 512
NH = 8
QUARTER = 128
HALFCH = 256
D = 2048
HALF = 1024
FFL = 1408

VMEM = pl.BlockSpec(memory_space=pltpu.VMEM)
SMEM = pl.BlockSpec(memory_space=pltpu.SMEM)
ANY = pl.BlockSpec(memory_space=pl.ANY)
HIGHEST = lax.Precision.HIGHEST
MIB = 1024 * 1024


def limit(mib):
    return pltpu.CompilerParams(vmem_limit_bytes=mib * MIB)


def close(value):
    return pltpu.with_memory_space_constraint(value, pltpu.VMEM)


def close_out(shape, kind):
    return pltpu.VMEM(shape, kind)


def away(*values):
    return tuple(pltpu.with_memory_space_constraint(value, pltpu.HBM) for value in values)


def away_out(shape, kind):
    return pltpu.HBM(shape, kind)


def dot(a, b):
    return jnp.dot(a, b, preferred_element_type=F32)


def dot_nt(a, b, precision=None):
    return lax.dot_general(
        a, b, (((1,), (1,)), ((), ())), precision=precision, preferred_element_type=F32
    )


def silu(v):
    return v / (1.0 + jnp.exp(-v))


def lane_pairs(column_of, rows):
    low = lax.broadcasted_iota(jnp.int32, (rows, 128), 1) < HEAD_DIM
    slabs = []
    for q in range(NH // 2):
        first = jnp.broadcast_to(column_of[:, 2 * q : 2 * q + 1], (rows, 128))
        second = jnp.broadcast_to(column_of[:, 2 * q + 1 : 2 * q + 2], (rows, 128))
        slabs.append(jnp.where(low, first, second))
    return slabs


def eye(n):
    line = lax.broadcasted_iota(jnp.int32, (n, n), 0)
    lane = lax.broadcasted_iota(jnp.int32, (n, n), 1)
    return jnp.where(line == lane, 1.0, 0.0).astype(F32)


def columns(rows):
    return dot_nt(eye(BLOCK), rows, precision=HIGHEST)


def down_column(ref):
    return jnp.sum(eye(NH) * ref[...], axis=1, keepdims=True)


def decays(delta, extra, offset, speed):
    step_in = delta + offset
    step = jnp.maximum(step_in, 0.0) + jnp.log1p(jnp.exp(-jnp.abs(step_in)))
    return step, extra - speed * step


def running_sum(fading):
    line = lax.broadcasted_iota(jnp.int32, (BLOCK, BLOCK), 0)
    lane = lax.broadcasted_iota(jnp.int32, (BLOCK, BLOCK), 1)
    upper = jnp.where(line <= lane, 1.0, 0.0).astype(F32)
    return jnp.dot(fading, upper, precision=HIGHEST, preferred_element_type=F32)


def conv_at(pad, taps, start):
    total = None
    for k in range(CONV):
        term = taps[k : k + 1, :].astype(F32) * pad[pl.ds(start + 8 - CONV + 1 + k, BLOCK), :]
        total = term if total is None else total + term
    return silu(total)


def conv_next(pad, taps, block):
    pad[8 : 8 + BLOCK, :] = block.astype(F32)
    total = None
    for k in range(CONV):
        term = taps[k : k + 1, :].astype(F32) * pad[pl.ds(8 - CONV + 1 + k, BLOCK), :]
        total = term if total is None else total + term
    pad[0:8, :] = pad[BLOCK : BLOCK + 8, :]
    return silu(total)


def pack_kernel(gate_ref, up_ref, down_ref, out_ref, sems):
    copies = [
        pltpu.make_async_copy(part, out_ref.at[:, k * FFL : (k + 1) * FFL], sems.at[k])
        for k, part in enumerate((gate_ref, up_ref, down_ref))
    ]
    for copy in copies:
        copy.start()
    for copy in copies:
        copy.wait()


def run_pack(gate, up, down):
    return pl.pallas_call(
        pack_kernel,
        out_shape=away_out((gate.shape[0], 3 * FFL), BF16),
        in_specs=[ANY] * 3,
        out_specs=ANY,
        scratch_shapes=[pltpu.SemaphoreType.DMA((3,))],
        name="pack",
    )(*away(gate, up, down))


def rim_kernel(x_ref, b_ref, c_ref, out_ref):
    out_ref[:, 0:CH] = x_ref[...]
    out_ref[:, CH : CH + STATE] = b_ref[...]
    out_ref[:, CH + STATE : CH + 2 * STATE] = c_ref[...]


def run_rim(x, b, c):
    last = lambda width: pl.BlockSpec((8, width), lambda i: (ROWS // 8 - 1, 0))
    return pl.pallas_call(
        rim_kernel,
        grid=(1,),
        out_shape=close_out((8, CH + 2 * STATE), BF16),
        in_specs=[last(CH), last(STATE), last(STATE)],
        out_specs=pl.BlockSpec((8, CH + 2 * STATE), lambda i: (0, 0)),
        name="rim",
    )(*away(x, b, c))


def state_kernel(
    x_ref, b_ref, rim_ref, xt_ref, bt_ref, delta_ref, extra_ref, offset_ref, speed_ref,
    x_out, b_out, state_out, msg_ref,
    xpad, bpad,
):
    xpad[0:8, :] = rim_ref[:, 0:CH].astype(F32)
    bpad[0:8, :] = rim_ref[:, CH : CH + STATE].astype(F32)
    xpad[8 : 8 + ROWS, :] = x_ref[...].astype(F32)
    bpad[8 : 8 + ROWS, :] = b_ref[...].astype(F32)
    step, fading = decays(
        delta_ref[...], extra_ref[...], down_column(offset_ref), down_column(speed_ref)
    )
    state = [jnp.zeros((STATE, 128), F32) for _ in range(NH // 2)]
    base = jnp.zeros((NH, 1), F32)
    for i in range(ROWS // BLOCK):
        start = i * BLOCK
        rows = pl.ds(start, BLOCK)
        here = slice(start, start + BLOCK)
        cum = running_sum(fading[:, here])
        last = cum[:, BLOCK - 1 : BLOCK]
        to_end = lane_pairs(columns(step[:, here] * jnp.exp(last - cum)), BLOCK)
        kept = lane_pairs(columns(jnp.broadcast_to(jnp.exp(last), (NH, BLOCK)))[0:1, :], 1)
        x_act = conv_at(xpad, xt_ref, start).astype(BF16)
        b_act = conv_at(bpad, bt_ref, start).astype(BF16)
        x_out[rows, :] = x_act
        b_out[rows, :] = b_act
        b_turned = b_act.astype(F32).T.astype(BF16)
        for q in range(NH // 2):
            cols = slice(q * 128, (q + 1) * 128)
            fresh = dot(b_turned, (x_act[:, cols].astype(F32) * to_end[q]).astype(BF16))
            state[q] = fresh if i == 0 else state[q] * kept[q] + fresh
            if i < ROWS // BLOCK - 1:
                state_out[i, :, cols] = state[q].astype(BF16)
        base = base + last
    totals = lane_pairs(columns(jnp.broadcast_to(base, (NH, BLOCK)))[0:1, :], 1)
    for q in range(NH // 2):
        block = slice(q * 16, (q + 1) * 16)
        msg_ref[block, 0:8, :] = state[q].reshape(16, 8, 128).astype(BF16)
        left = totals[q]
        parts = []
        for _ in range(3):
            part = left.astype(BF16)
            parts.append(part.astype(F32))
            left = left - part.astype(F32)
        line = lax.broadcasted_iota(jnp.int32, (8, 128), 0)
        packed = jnp.where(line == 0, parts[0], jnp.where(line == 1, parts[1], parts[2]))
        packed = jnp.where(line < 3, packed, 0.0).astype(BF16)
        msg_ref[block, 8:16, :] = jnp.broadcast_to(packed[None], (16, 8, 128))


def run_state(x, b, rim, xt, bt, delta, extra, offset, speed):
    return pl.pallas_call(
        state_kernel,
        out_shape=(
            away_out((ROWS, CH), BF16),
            away_out((ROWS, STATE), BF16),
            away_out((ROWS // BLOCK - 1, STATE, CH), BF16),
            close_out((64, 16, 128), BF16),
        ),
        compiler_params=limit(24),
        in_specs=[VMEM] * 9,
        out_specs=(VMEM,) * 4,
        scratch_shapes=[
            pltpu.VMEM((ROWS + 8, CH), F32),
            pltpu.VMEM((ROWS + 8, STATE), F32),
        ],
        name="local_state",
    )(*away(x, b), close(rim), *away(xt, bt, delta, extra, offset, speed))


def local_kernel(
    x_ref, b_ref, state_ref, c_ref, rim_ref, ct_ref, delta_ref, extra_ref, offset_ref, speed_ref,
    bypass_ref,
    y_ref, cact_ref, grow_ref,
    cpad,
):
    cpad[0:8, :] = rim_ref[:, CH + STATE : CH + 2 * STATE].astype(F32)
    offset = down_column(offset_ref)
    speed = down_column(speed_ref)
    bypass = lane_pairs(bypass_ref[...], 1)
    row = lax.broadcasted_iota(jnp.int32, (BLOCK, BLOCK), 0)
    col = lax.broadcasted_iota(jnp.int32, (BLOCK, BLOCK), 1)
    causal = row >= col
    low = col < HEAD_DIM

    def block_step(i, base):
        rows = pl.ds(pl.multiple_of(i * BLOCK, BLOCK), BLOCK)
        step, fading = decays(delta_ref[:, rows], extra_ref[:, rows], offset, speed)
        cum = running_sum(fading)
        turned = columns(jnp.concatenate([cum, jnp.exp(cum), jnp.exp(base + cum)], axis=0))
        grow_ref[rows, :] = turned[:, 2 * NH : 3 * NH]
        grown = lane_pairs(turned[:, NH : 2 * NH], BLOCK)
        c_act = conv_next(cpad, ct_ref, c_ref[rows, :]).astype(BF16)
        cact_ref[rows, :] = c_act
        affinity = dot_nt(c_act, b_ref[rows, :])
        for q in range(NH // 2):
            cols = slice(q * 128, (q + 1) * 128)
            x_here = x_ref[rows, cols]
            within = []
            for h in (2 * q, 2 * q + 1):
                between = turned[:, h : h + 1] - cum[h : h + 1, :]
                lag = jnp.exp(jnp.where(causal, between, NEG)) * step[h : h + 1, :]
                within.append(dot((affinity * lag).astype(BF16), x_here))
            total = jnp.where(low, within[0], within[1]) + bypass[q] * x_here.astype(F32)
            carried = dot(c_act, state_ref[jnp.maximum(i - 1, 0), :, cols]) * grown[q]
            y_ref[rows, cols] = total + jnp.where(i > 0, carried, 0.0)
        return base + cum[:, BLOCK - 1 : BLOCK]

    lax.fori_loop(0, ROWS // BLOCK, block_step, jnp.zeros((NH, 1), F32))


def run_local(x, b, states, c, rim, ct, delta, extra, offset, speed, bypass):
    return pl.pallas_call(
        local_kernel,
        out_shape=(
            away_out((ROWS, CH), F32),
            away_out((ROWS, STATE), BF16),
            away_out((ROWS, NH), F32),
        ),
        compiler_params=limit(24),
        in_specs=[VMEM] * 11,
        out_specs=(VMEM,) * 3,
        scratch_shapes=[pltpu.VMEM((BLOCK + 8, STATE), F32)],
        name="local_mixer",
    )(*away(x, b, states, c), close(rim), *away(ct, delta, extra, offset, speed, bypass))


def prefix_kernel(in_ref, out_ref):
    entering = jnp.zeros((8, 128), F32)
    for j in range(64):
        out_ref[j] = entering.astype(BF16)
        piece = in_ref[j].astype(F32)
        total = piece[8:9, :] + piece[9:10, :] + piece[10:11, :]
        entering = entering * jnp.exp(total) + piece[0:8, :]


def run_prefix(received):
    return pl.pallas_call(
        prefix_kernel,
        out_shape=close_out((64, 8, 128), BF16),
        compiler_params=limit(8),
        in_specs=[VMEM],
        out_specs=VMEM,
        name="state_prefix",
    )(close(received))


def gate_kernel(y_ref, cact_ref, grow_ref, in_ref, valve_ref, scale_ref, out_l, out_r):
    for i in range(ROWS // BLOCK):
        rows = pl.ds(i * BLOCK, BLOCK)
        grown = lane_pairs(grow_ref[rows, :], BLOCK)
        c_act = cact_ref[rows, :]
        gated = []
        square = jnp.zeros((BLOCK, 1), F32)
        for q in range(NH // 2):
            cols = slice(q * 128, (q + 1) * 128)
            entering = in_ref[q * 16 : (q + 1) * 16].astype(F32).reshape(STATE, 128).astype(BF16)
            y = y_ref[rows, cols] + dot(c_act, entering) * grown[q]
            y = y * silu(valve_ref[rows, cols].astype(F32))
            gated.append(y)
            square = square + jnp.sum(y * y, axis=-1, keepdims=True)
        factor = lax.rsqrt(square * (1.0 / CH) + EPSILON)
        for q in range(NH // 2):
            cols = slice(q * 128, (q + 1) * 128)
            half = (out_l, out_r)[q // 2]
            half[rows, (q % 2) * 128 : (q % 2 + 1) * 128] = (
                gated[q] * factor * scale_ref[0:1, cols]
            ).astype(BF16)


def run_gate(y, cact, grow, entering, valve, scale):
    return pl.pallas_call(
        gate_kernel,
        out_shape=(
            away_out((ROWS, HALFCH), BF16),
            away_out((ROWS, HALFCH), BF16),
        ),
        compiler_params=limit(16),
        in_specs=[VMEM] * 6,
        out_specs=(VMEM,) * 2,
        name="gate_norm",
    )(*away(y, cact, grow), close(entering), *away(valve, scale))


RIM = 16
CHUNK = 512


def project_kernel(
    place_ref, scale_ref, near_l, far_r, across_l, across_r,
    own_l, own_r, near_r, far_l, own_w, near_w, far_w, across_w, near_x, far_x, across_x,
    own_res, near_res, far_res, across_res,
    out_ref, tail_ref,
    weight, early, res, total, w_sems, e_sems, r_sems,
):
    core = place_ref[4]
    columns_of = (
        pl.ds(pl.multiple_of(core * HALF, HALF), HALF),
        pl.ds(pl.multiple_of((1 - core) * HALF, HALF), HALF),
    )
    arrived = ((near_w, far_w, across_w), (near_x, far_x, across_x))
    copies = ([], [])
    for half in range(2):
        sources = (own_w.at[:, columns_of[half]], *arrived[half])
        for k, source in enumerate(sources):
            target = weight.at[half, k * CH : (k + 1) * CH, :]
            copies[half].append(pltpu.make_async_copy(source, target, w_sems.at[half, k]))
    res_copies = []
    for k, source in enumerate((own_res, near_res, far_res, across_res)):
        rows = pl.ds(pl.multiple_of(place_ref[k] * QUARTER, QUARTER), QUARTER)
        res_copies.append(pltpu.make_async_copy(source, res.at[rows, :], r_sems.at[k]))
    early_copies = [
        pltpu.make_async_copy(source, early.at[k], e_sems.at[k])
        for k, source in enumerate((own_l, own_r, near_r, far_l))
    ]
    acts = (early.at[0], early.at[1], near_l, early.at[2], early.at[3], far_r, across_l, across_r)
    for copy in early_copies + copies[0]:
        copy.start()
    for copy in early_copies + copies[0]:
        copy.wait()
    for copy in copies[1] + res_copies:
        copy.start()
    for half in range(2):
        if half == 1:
            for copy in copies[1]:
                copy.wait()
        for n in range(HALF // CHUNK):
            cols = slice(n * CHUNK, (n + 1) * CHUNK)
            part = None
            for k, act in enumerate(acts):
                term = dot(act[...], weight[half, k * HALFCH : (k + 1) * HALFCH, cols])
                part = term if part is None else part + term
            start = pl.multiple_of((core if half == 0 else 1 - core) * HALF + n * CHUNK, CHUNK)
            total[:, pl.ds(start, CHUNK)] = part
    for copy in res_copies:
        copy.wait()

    def norm(values):
        centred = values - jnp.sum(values, axis=-1, keepdims=True) * (1.0 / D)
        spread = jnp.sum(centred * centred, axis=-1, keepdims=True) * (1.0 / D)
        return (centred * lax.rsqrt(spread + EPSILON) * scale_ref[...]).astype(BF16)


    def norm_rows(i, carry):
        rows = pl.ds(pl.multiple_of(i * 64, 64), 64)
        out_ref[rows, :] = norm(total[rows, :] + ALPHA * res[rows, :].astype(F32))
        return carry

    lax.fori_loop(0, ROWS // 64, norm_rows, 0)
    tail_ref[...] = out_ref[ROWS - RIM : ROWS, :]


def run_project(place, scale, weights, acts, residuals):
    return pl.pallas_call(
        project_kernel,
        out_shape=(close_out((ROWS, D), BF16), close_out((RIM, D), BF16)),
        in_specs=[SMEM] + [VMEM] * 5 + [ANY] * 15,
        out_specs=(VMEM, VMEM),
        scratch_shapes=[
            pltpu.VMEM((2, D, HALF), BF16),
            pltpu.VMEM((4, ROWS, HALFCH), BF16),
            pltpu.VMEM((ROWS, D), BF16),
            pltpu.VMEM((ROWS, D), F32),
            pltpu.SemaphoreType.DMA((2, 4)),
            pltpu.SemaphoreType.DMA((4,)),
            pltpu.SemaphoreType.DMA((4,)),
        ],
        compiler_params=limit(30),
        name="project_norm",
    )(
        place,
        *away(scale),
        *[close(acts[k]) for k in (2, 5, 6, 7)],
        *away(*[acts[k] for k in (0, 1, 3, 4)], *weights, *residuals),
    )


TILES = FFL // 128
NARROW = 512


def down_copies(w_ref, down, sems):
    return [
        pltpu.make_async_copy(
            w_ref.at[n * NARROW : (n + 1) * NARROW, 2 * FFL : 3 * FFL],
            down.at[n * NARROW : (n + 1) * NARROW, :],
            sems.at[n],
        )
        for n in range(D // NARROW)
    ]


def two_quarters(hid, place_ref, half):
    def rows_of(k):
        return hid[pl.ds(pl.multiple_of(place_ref[half, k] * QUARTER, QUARTER), QUARTER), :]

    return jnp.concatenate([rows_of(0), rows_of(1)], axis=0)


AHEAD = 4
STRIP = 512


def widen_kernel(
    sent_ref, gate_t, up_t, normed, rim, w_ref,
    hid, down, send_l, send_r,
    wide, gate_pad, up_pad, wide_sems, down_sems,
):
    def wide_copies(j):
        at = j * 128
        if not isinstance(j, int):
            at = pl.multiple_of(at, 128)
        return (
            pltpu.make_async_copy(
                w_ref.at[:, pl.ds(at, 128)], wide.at[j, :, 0:128], wide_sems.at[j, 0]
            ),
            pltpu.make_async_copy(
                w_ref.at[:, pl.ds(FFL + at, 128)], wide.at[j, :, 128:256], wide_sems.at[j, 1]
            ),
        )

    downs = down_copies(w_ref, down, down_sems)
    for j in range(AHEAD):
        for copy in wide_copies(j):
            copy.start()

    def conv(pad, taps, at):
        total = None
        for k in range(FCONV):
            tap = taps[k : k + 1, pl.ds(at, 128)].astype(F32)
            term = tap * pad[pl.ds(RIM - FCONV + 1 + k, ROWS), :]
            total = term if total is None else total + term
        return total

    def finish(j):
        at = j * 128
        if not isinstance(j, int):
            at = pl.multiple_of(at, 128)
        hid[:, pl.ds(at, 128)] = (
            silu(conv(gate_pad, gate_t, at)) * conv(up_pad, up_t, at)
        ).astype(BF16)

    def tile(j, carry):
        for copy in wide_copies(j):
            copy.wait()

        @pl.when(j + AHEAD < TILES)
        def _():
            for copy in wide_copies(j + AHEAD):
                copy.start()

        @pl.when(j + AHEAD == TILES)
        def _():
            for copy in downs:
                copy.start()

        finish(jnp.maximum(j - 1, 0))
        rows = jnp.concatenate([rim[...], normed[...]], axis=0)
        both = dot(rows, wide[j]).astype(BF16).astype(F32)
        gate_pad[...] = both[:, 0:128]
        up_pad[...] = both[:, 128:256]
        return carry

    lax.fori_loop(0, TILES, tile, 0)
    finish(TILES - 1)
    for copy in downs:
        copy.wait()
    send_l[...] = dot_nt(two_quarters(hid, sent_ref, 0), down[0:STRIP, :]).astype(BF16)
    send_r[...] = dot_nt(two_quarters(hid, sent_ref, 1), down[HALF : HALF + STRIP, :]).astype(BF16)


def run_widen(sent, normed, rim, weights, gate_t, up_t):
    return pl.pallas_call(
        widen_kernel,
        out_shape=(
            close_out((ROWS, FFL), BF16),
            close_out((D, FFL), BF16),
            close_out((2 * QUARTER, STRIP), BF16),
            close_out((2 * QUARTER, STRIP), BF16),
        ),
        in_specs=[SMEM, VMEM, VMEM, VMEM, VMEM, ANY],
        out_specs=(VMEM,) * 4,
        scratch_shapes=[
            pltpu.VMEM((TILES, D, 256), BF16),
            pltpu.VMEM((ROWS + RIM, 128), F32),
            pltpu.VMEM((ROWS + RIM, 128), F32),
            pltpu.SemaphoreType.DMA((TILES, 2)),
            pltpu.SemaphoreType.DMA((D // NARROW,)),
        ],
        compiler_params=limit(24),
        name="widen",
    )(sent, *away(gate_t, up_t), close(normed), close(rim), *away(weights))


def sent_kernel(sent_ref, hid, down, send_l, send_r):
    send_l[...] = dot_nt(two_quarters(hid, sent_ref, 0), down[STRIP:HALF, :]).astype(BF16)
    send_r[...] = dot_nt(two_quarters(hid, sent_ref, 1), down[HALF + STRIP : D, :]).astype(BF16)


def run_sent(sent, hidden, down):
    return pl.pallas_call(
        sent_kernel,
        out_shape=(close_out((2 * QUARTER, STRIP), BF16),) * 2,
        in_specs=[SMEM, VMEM, VMEM],
        out_specs=(VMEM,) * 2,
        compiler_params=limit(8),
        name="shrink_sent",
    )(sent, close(hidden), close(down))


def held_kernel(held_ref, hid, down, own, pass_1, pass_2):
    for half in range(2):
        both = dot_nt(two_quarters(hid, held_ref, half), down[half * HALF : (half + 1) * HALF, :])
        own[:, half * HALF : (half + 1) * HALF] = both[0:QUARTER, :]
        pass_1[:, half * STRIP : (half + 1) * STRIP] = both[QUARTER:, 0:STRIP]
        pass_2[:, half * STRIP : (half + 1) * STRIP] = both[QUARTER:, STRIP:HALF]


def run_held(held, hidden, down):
    return pl.pallas_call(
        held_kernel,
        out_shape=(
            close_out((QUARTER, D), F32),
            close_out((QUARTER, HALF), F32),
            close_out((QUARTER, HALF), F32),
        ),
        in_specs=[SMEM, VMEM, VMEM],
        out_specs=(VMEM,) * 3,
        compiler_params=limit(8),
        name="shrink_held",
    )(held, close(hidden), close(down))


def add_kernel(passed, once_l, once_r, out_l, out_r):
    out_l[...] = (passed[:, 0:STRIP] + once_l[QUARTER:, :].astype(F32)).astype(BF16)
    out_r[...] = (passed[:, STRIP:] + once_r[QUARTER:, :].astype(F32)).astype(BF16)


def run_add(passed, once_l, once_r):
    return pl.pallas_call(
        add_kernel,
        out_shape=(close_out((QUARTER, STRIP), BF16),) * 2,
        in_specs=[VMEM] * 3,
        out_specs=(VMEM,) * 2,
        compiler_params=limit(8),
        name="round_sum",
    )(close(passed), close(once_l), close(once_r))


def last_norm_kernel(
    place_ref, own, l_1, r_1, l_2, r_2, ll_1, rr_1, ll_2, rr_2, res_ref, scale_ref, out_ref
):
    for i in range(2):
        rows = slice(i * 64, (i + 1) * 64)
        kept = pl.ds(pl.multiple_of(place_ref[0] * QUARTER + i * 64, 64), 64)
        parts = []
        for k, (once, twice) in enumerate(((l_1, ll_1), (l_2, ll_2), (r_1, rr_1), (r_2, rr_2))):
            cols = slice(k * STRIP, (k + 1) * STRIP)
            part = own[rows, cols] + once[rows, :].astype(F32) + twice[rows, :].astype(F32)
            parts.append(part + ALPHA * res_ref[kept, cols].astype(F32))
        values = jnp.concatenate(parts, axis=1)
        centred = values - jnp.sum(values, axis=-1, keepdims=True) * (1.0 / D)
        spread = jnp.sum(centred * centred, axis=-1, keepdims=True) * (1.0 / D)
        out_ref[rows, :] = (centred * lax.rsqrt(spread + EPSILON) * scale_ref[...]).astype(BF16)


def run_last_norm(place, own, onces, twices, rows, scale):
    kept = [close(part) for part in (own, *onces, *twices, rows)]
    return pl.pallas_call(
        last_norm_kernel,
        out_shape=jax.ShapeDtypeStruct((QUARTER, D), BF16),
        in_specs=[SMEM] + [VMEM] * 11,
        out_specs=VMEM,
        compiler_params=limit(8),
        name="last_norm",
    )(place, *kept, *away(scale))


NEAR = [(0, 1), (1, 0), (2, 3), (3, 2)]
FAR = [(0, 3), (3, 0), (1, 2), (2, 1)]


def with_near(part):
    return lax.ppermute(part, "tp", NEAR)


def with_far(part):
    return lax.ppermute(part, "tp", FAR)


def forwarded(far_part, near_part):
    part = jnp.where(lax.axis_index("sp_2") == 0, far_part, near_part)
    pairs = [(i, j) for i, j in NEAR] + [(4 + i, 4 + j) for i, j in FAR]
    return lax.ppermute(part, ("sp_2", "tp"), pairs)


def with_core(part):
    return lax.ppermute(part, "sp_2", [(0, 1), (1, 0)])


def next_positions(shard):
    count = lax.axis_size(SP)
    return lax.ppermute(shard, SP, [(i, i + 1) for i in range(count - 1)])


def shards(
    incoming_residual_stream,
    result_valve,
    channel_feed_matrix,
    memory_feed_matrix,
    memory_query_matrix,
    unsoftened_deltas,
    delta_offset,
    channel_fading_speed,
    extra_log_fading,
    bypass_factor,
    channel_feed_kernel,
    memory_feed_kernel,
    memory_query_kernel,
    cluster_scaling_vector,
    mixer_result_matrix,
    initial_scaling_vector,
    valve_matrix,
    widen_matrix,
    shrink_matrix,
    valve_filter_kernel,
    widen_filter_kernel,
    latter_scaling_vector,
):
    own = lax.axis_index("tp").astype(jnp.int32)
    core = lax.axis_index("sp_2").astype(jnp.int32)
    near = own ^ 1
    far = 3 - own
    across = own ^ 2
    place = jnp.stack([own, near, far, across, core])
    sent = jnp.stack([jnp.stack([near, across]), jnp.stack([far, across])])
    held = jnp.stack([jnp.stack([own, far]), jnp.stack([own, near])])

    weights = lax.all_gather(
        run_pack(valve_matrix, widen_matrix, shrink_matrix.T), SP, tiled=True
    )

    rim = run_rim(channel_feed_matrix, memory_feed_matrix, memory_query_matrix)
    _, projection, residual = lax.optimization_barrier(
        (rim, mixer_result_matrix, incoming_residual_stream)
    )
    rim = next_positions(rim)
    drives = (
        unsoftened_deltas.T,
        extra_log_fading.T,
        delta_offset.reshape(1, NH),
        channel_fading_speed.reshape(1, NH),
    )
    x_act, b_act, states, message = run_state(
        channel_feed_matrix,
        memory_feed_matrix,
        rim,
        channel_feed_kernel,
        memory_feed_kernel,
        *drives,
    )
    received = lax.all_to_all(message, SP, 0, 0, tiled=True)

    w_half = lax.dynamic_slice(projection, (0, core * HALF), (CH, HALF))
    w_near = with_near(w_half)
    w_far = with_far(w_half)
    res_near = with_near(residual)
    res_far = with_far(residual)

    y_local, c_act, grow = run_local(
        x_act,
        b_act,
        states,
        memory_query_matrix,
        rim,
        memory_query_kernel,
        *drives,
        bypass_factor.reshape(1, NH),
    )
    prefix = run_prefix(received)
    entering = lax.all_to_all(prefix, SP, 0, 0, tiled=True)
    _, late_near, late_far = lax.optimization_barrier((y_local, w_near, w_far))
    w_across = forwarded(late_far, late_near)
    _, late_near, late_far = lax.optimization_barrier((prefix, res_near, res_far))
    res_across = forwarded(late_far, late_near)
    y_l, y_r = run_gate(
        y_local, c_act, grow, entering, result_valve, cluster_scaling_vector.reshape(1, CH)
    )
    swap = lax.optimization_barrier((prefix, w_near, w_far))[1:]
    w_other = (
        with_core(swap[0]),
        with_core(swap[1]),
        with_core(lax.optimization_barrier((y_l, w_across))[1]),
    )
    far_l = with_far(y_l)
    near_r = with_near(y_r)
    near_l = with_near(y_l)
    far_r = with_far(y_r)
    across_l = with_near(far_l)
    across_r = with_far(near_r)
    normed, tail = run_project(
        place,
        initial_scaling_vector.reshape(1, D),
        (mixer_result_matrix, w_near, w_far, w_across, *w_other),
        (y_l, y_r, near_l, near_r, far_l, far_r, across_l, across_r),
        (residual, res_near, res_far, res_across),
    )
    hidden, down, send_l1, send_r1 = run_widen(
        sent, normed, next_positions(tail), weights, valve_filter_kernel, widen_filter_kernel
    )
    l_1 = with_near(send_l1)
    r_1 = with_far(send_r1)
    send_l2, send_r2 = run_sent(sent, hidden, down)
    l_2 = with_near(send_l2)
    r_2 = with_far(send_r2)
    kept, pass_1, pass_2 = run_held(held, hidden, down)
    on_l1, on_r1 = run_add(pass_1, l_1, r_1)
    ll_1 = with_far(on_l1)
    rr_1 = with_near(on_r1)
    on_l2, on_r2 = run_add(pass_2, l_2, r_2)
    ll_2 = with_far(on_l2)
    rr_2 = with_near(on_r2)
    return run_last_norm(
        place,
        kept,
        (l_1, r_1, l_2, r_2),
        (ll_1, rr_1, ll_2, rr_2),
        normed,
        latter_scaling_vector.reshape(1, D),
    )


def solution(mesh):
    split = Mesh(mesh.devices.reshape(8, 4, 2, mesh.shape["tp"]), ("sp_0", "sp_1", "sp_2", "tp"))
    in_specs = (
        P(SP_TP, None),
        P(SP, "tp"),
        P(SP, "tp"),
        P(SP, "tp"),
        P(SP, "tp"),
        P(SP, "tp"),
        P("tp"),
        P("tp"),
        P(SP, "tp"),
        P("tp"),
        P(None, "tp"),
        P(None, "tp"),
        P(None, "tp"),
        P("tp"),
        P("tp", None),
        P(),
        P(SP, "tp"),
        P(SP, "tp"),
        P("tp", SP),
        P(None, "tp"),
        P(None, "tp"),
        P(),
    )
    out_specs = P(SP_TP, None)

    return jax.shard_map(
        shards, mesh=split, in_specs=in_specs, out_specs=out_specs, check_vma=False
    )
```

```python
import jax
import jax.numpy as jnp
from jax import lax
from jax.experimental import pallas as pl
from jax.experimental.pallas import tpu as pltpu
from jax.sharding import Mesh
from jax.sharding import PartitionSpec as P

HEAD_DIM = 64
STATE = 128
CONV = 4
FCONV = 3
BLOCK = 128
SP = ("sp_0", "sp_1", "sp_2")
SP_TP = ("sp_0", "sp_1", "sp_2", "tp")

EPSILON = 1e-05
ALPHA = 2.0**0.25
F32 = jnp.float32
BF16 = jnp.bfloat16
NEG = -1e30

ROWS = 512
CH = 512
NH = 8
QUARTER = 128
HALFCH = 256
D = 2048
HALF = 1024
FFL = 1408

VMEM = pl.BlockSpec(memory_space=pltpu.VMEM)
SMEM = pl.BlockSpec(memory_space=pltpu.SMEM)
ANY = pl.BlockSpec(memory_space=pl.ANY)
HIGHEST = lax.Precision.HIGHEST
MIB = 1024 * 1024


def limit(mib):
    return pltpu.CompilerParams(vmem_limit_bytes=mib * MIB)


def close(value):
    return pltpu.with_memory_space_constraint(value, pltpu.VMEM)


def close_out(shape, kind):
    return pltpu.VMEM(shape, kind)


def away(*values):
    return tuple(pltpu.with_memory_space_constraint(value, pltpu.HBM) for value in values)


def away_out(shape, kind):
    return pltpu.HBM(shape, kind)


def dot(a, b):
    return jnp.dot(a, b, preferred_element_type=F32)


def dot_nt(a, b, precision=None):
    return lax.dot_general(
        a, b, (((1,), (1,)), ((), ())), precision=precision, preferred_element_type=F32
    )


def silu(v):
    return v / (1.0 + jnp.exp(-v))


def lane_pairs(column_of, rows):
    low = lax.broadcasted_iota(jnp.int32, (rows, 128), 1) < HEAD_DIM
    slabs = []
    for q in range(NH // 2):
        first = jnp.broadcast_to(column_of[:, 2 * q : 2 * q + 1], (rows, 128))
        second = jnp.broadcast_to(column_of[:, 2 * q + 1 : 2 * q + 2], (rows, 128))
        slabs.append(jnp.where(low, first, second))
    return slabs


def eye(n):
    line = lax.broadcasted_iota(jnp.int32, (n, n), 0)
    lane = lax.broadcasted_iota(jnp.int32, (n, n), 1)
    return jnp.where(line == lane, 1.0, 0.0).astype(F32)


def columns(rows):
    return dot_nt(eye(BLOCK), rows, precision=HIGHEST)


def down_column(ref):
    return jnp.sum(eye(NH) * ref[...], axis=1, keepdims=True)


def decays(delta, extra, offset, speed):
    step_in = delta + offset
    step = jnp.maximum(step_in, 0.0) + jnp.log1p(jnp.exp(-jnp.abs(step_in)))
    return step, extra - speed * step


def running_sum(fading):
    line = lax.broadcasted_iota(jnp.int32, (BLOCK, BLOCK), 0)
    lane = lax.broadcasted_iota(jnp.int32, (BLOCK, BLOCK), 1)
    upper = jnp.where(line <= lane, 1.0, 0.0).astype(F32)
    return jnp.dot(fading, upper, precision=HIGHEST, preferred_element_type=F32)


def conv_at(pad, taps, start):
    total = None
    for k in range(CONV):
        term = taps[k : k + 1, :].astype(F32) * pad[pl.ds(start + 8 - CONV + 1 + k, BLOCK), :]
        total = term if total is None else total + term
    return silu(total)


def conv_next(pad, taps, block):
    pad[8 : 8 + BLOCK, :] = block.astype(F32)
    total = None
    for k in range(CONV):
        term = taps[k : k + 1, :].astype(F32) * pad[pl.ds(8 - CONV + 1 + k, BLOCK), :]
        total = term if total is None else total + term
    pad[0:8, :] = pad[BLOCK : BLOCK + 8, :]
    return silu(total)


def rim_kernel(x_ref, b_ref, c_ref, out_ref):
    out_ref[:, 0:CH] = x_ref[...]
    out_ref[:, CH : CH + STATE] = b_ref[...]
    out_ref[:, CH + STATE : CH + 2 * STATE] = c_ref[...]


def run_rim(x, b, c):
    last = lambda width: pl.BlockSpec((8, width), lambda i: (ROWS // 8 - 1, 0))
    return pl.pallas_call(
        rim_kernel,
        grid=(1,),
        out_shape=close_out((8, CH + 2 * STATE), BF16),
        in_specs=[last(CH), last(STATE), last(STATE)],
        out_specs=pl.BlockSpec((8, CH + 2 * STATE), lambda i: (0, 0)),
        name="rim",
    )(*away(x, b, c))


def state_kernel(
    x_ref, b_ref, rim_ref, xt_ref, bt_ref, delta_ref, extra_ref, offset_ref, speed_ref,
    x_out, b_out, state_out, msg_ref,
    xpad, bpad,
):
    xpad[0:8, :] = rim_ref[:, 0:CH].astype(F32)
    bpad[0:8, :] = rim_ref[:, CH : CH + STATE].astype(F32)
    xpad[8 : 8 + ROWS, :] = x_ref[...].astype(F32)
    bpad[8 : 8 + ROWS, :] = b_ref[...].astype(F32)
    step, fading = decays(
        delta_ref[...], extra_ref[...], down_column(offset_ref), down_column(speed_ref)
    )
    state = [jnp.zeros((STATE, 128), F32) for _ in range(NH // 2)]
    base = jnp.zeros((NH, 1), F32)
    for i in range(ROWS // BLOCK):
        start = i * BLOCK
        rows = pl.ds(start, BLOCK)
        here = slice(start, start + BLOCK)
        cum = running_sum(fading[:, here])
        last = cum[:, BLOCK - 1 : BLOCK]
        to_end = lane_pairs(columns(step[:, here] * jnp.exp(last - cum)), BLOCK)
        kept = lane_pairs(columns(jnp.broadcast_to(jnp.exp(last), (NH, BLOCK)))[0:1, :], 1)
        x_act = conv_at(xpad, xt_ref, start).astype(BF16)
        b_act = conv_at(bpad, bt_ref, start).astype(BF16)
        x_out[rows, :] = x_act
        b_out[rows, :] = b_act
        b_turned = b_act.astype(F32).T.astype(BF16)
        for q in range(NH // 2):
            cols = slice(q * 128, (q + 1) * 128)
            fresh = dot(b_turned, (x_act[:, cols].astype(F32) * to_end[q]).astype(BF16))
            state[q] = fresh if i == 0 else state[q] * kept[q] + fresh
            if i < ROWS // BLOCK - 1:
                state_out[i, :, cols] = state[q].astype(BF16)
        base = base + last
    totals = lane_pairs(columns(jnp.broadcast_to(base, (NH, BLOCK)))[0:1, :], 1)
    for q in range(NH // 2):
        block = slice(q * 16, (q + 1) * 16)
        msg_ref[block, 0:8, :] = state[q].reshape(16, 8, 128).astype(BF16)
        left = totals[q]
        parts = []
        for _ in range(3):
            part = left.astype(BF16)
            parts.append(part.astype(F32))
            left = left - part.astype(F32)
        line = lax.broadcasted_iota(jnp.int32, (8, 128), 0)
        packed = jnp.where(line == 0, parts[0], jnp.where(line == 1, parts[1], parts[2]))
        packed = jnp.where(line < 3, packed, 0.0).astype(BF16)
        msg_ref[block, 8:16, :] = jnp.broadcast_to(packed[None], (16, 8, 128))


def run_state(x, b, rim, xt, bt, delta, extra, offset, speed):
    return pl.pallas_call(
        state_kernel,
        out_shape=(
            away_out((ROWS, CH), BF16),
            away_out((ROWS, STATE), BF16),
            away_out((ROWS // BLOCK - 1, STATE, CH), BF16),
            close_out((64, 16, 128), BF16),
        ),
        compiler_params=limit(24),
        in_specs=[VMEM] * 9,
        out_specs=(VMEM,) * 4,
        scratch_shapes=[
            pltpu.VMEM((ROWS + 8, CH), F32),
            pltpu.VMEM((ROWS + 8, STATE), F32),
        ],
        name="local_state",
    )(*away(x, b), close(rim), *away(xt, bt, delta, extra, offset, speed))


def local_kernel(
    x_ref, b_ref, state_ref, c_ref, rim_ref, ct_ref, delta_ref, extra_ref, offset_ref, speed_ref,
    bypass_ref,
    y_ref, cact_ref, grow_ref,
    cpad,
):
    cpad[0:8, :] = rim_ref[:, CH + STATE : CH + 2 * STATE].astype(F32)
    offset = down_column(offset_ref)
    speed = down_column(speed_ref)
    bypass = lane_pairs(bypass_ref[...], 1)
    row = lax.broadcasted_iota(jnp.int32, (BLOCK, BLOCK), 0)
    col = lax.broadcasted_iota(jnp.int32, (BLOCK, BLOCK), 1)
    causal = row >= col
    low = col < HEAD_DIM

    def block_step(i, base):
        rows = pl.ds(pl.multiple_of(i * BLOCK, BLOCK), BLOCK)
        step, fading = decays(delta_ref[:, rows], extra_ref[:, rows], offset, speed)
        cum = running_sum(fading)
        turned = columns(jnp.concatenate([cum, jnp.exp(cum), jnp.exp(base + cum)], axis=0))
        grow_ref[rows, :] = turned[:, 2 * NH : 3 * NH]
        grown = lane_pairs(turned[:, NH : 2 * NH], BLOCK)
        c_act = conv_next(cpad, ct_ref, c_ref[rows, :]).astype(BF16)
        cact_ref[rows, :] = c_act
        affinity = dot_nt(c_act, b_ref[rows, :])
        for q in range(NH // 2):
            cols = slice(q * 128, (q + 1) * 128)
            x_here = x_ref[rows, cols]
            within = []
            for h in (2 * q, 2 * q + 1):
                between = turned[:, h : h + 1] - cum[h : h + 1, :]
                lag = jnp.exp(jnp.where(causal, between, NEG)) * step[h : h + 1, :]
                within.append(dot((affinity * lag).astype(BF16), x_here))
            total = jnp.where(low, within[0], within[1]) + bypass[q] * x_here.astype(F32)
            carried = dot(c_act, state_ref[jnp.maximum(i - 1, 0), :, cols]) * grown[q]
            y_ref[rows, cols] = total + jnp.where(i > 0, carried, 0.0)
        return base + cum[:, BLOCK - 1 : BLOCK]

    lax.fori_loop(0, ROWS // BLOCK, block_step, jnp.zeros((NH, 1), F32))


def run_local(x, b, states, c, rim, ct, delta, extra, offset, speed, bypass):
    return pl.pallas_call(
        local_kernel,
        out_shape=(
            away_out((ROWS, CH), F32),
            away_out((ROWS, STATE), BF16),
            away_out((ROWS, NH), F32),
        ),
        compiler_params=limit(24),
        in_specs=[VMEM] * 11,
        out_specs=(VMEM,) * 3,
        scratch_shapes=[pltpu.VMEM((BLOCK + 8, STATE), F32)],
        name="local_mixer",
    )(*away(x, b, states, c), close(rim), *away(ct, delta, extra, offset, speed, bypass))


def prefix_kernel(in_ref, out_ref):
    entering = jnp.zeros((8, 128), F32)
    for j in range(64):
        out_ref[j] = entering.astype(BF16)
        piece = in_ref[j].astype(F32)
        total = piece[8:9, :] + piece[9:10, :] + piece[10:11, :]
        entering = entering * jnp.exp(total) + piece[0:8, :]


def run_prefix(received):
    return pl.pallas_call(
        prefix_kernel,
        out_shape=close_out((64, 8, 128), BF16),
        compiler_params=limit(8),
        in_specs=[VMEM],
        out_specs=VMEM,
        name="state_prefix",
    )(close(received))


def gate_kernel(y_ref, cact_ref, grow_ref, in_ref, valve_ref, scale_ref, out_l, out_r):
    for i in range(ROWS // BLOCK):
        rows = pl.ds(i * BLOCK, BLOCK)
        grown = lane_pairs(grow_ref[rows, :], BLOCK)
        c_act = cact_ref[rows, :]
        gated = []
        square = jnp.zeros((BLOCK, 1), F32)
        for q in range(NH // 2):
            cols = slice(q * 128, (q + 1) * 128)
            entering = in_ref[q * 16 : (q + 1) * 16].astype(F32).reshape(STATE, 128).astype(BF16)
            y = y_ref[rows, cols] + dot(c_act, entering) * grown[q]
            y = y * silu(valve_ref[rows, cols].astype(F32))
            gated.append(y)
            square = square + jnp.sum(y * y, axis=-1, keepdims=True)
        factor = lax.rsqrt(square * (1.0 / CH) + EPSILON)
        for q in range(NH // 2):
            cols = slice(q * 128, (q + 1) * 128)
            half = (out_l, out_r)[q // 2]
            half[rows, (q % 2) * 128 : (q % 2 + 1) * 128] = (
                gated[q] * factor * scale_ref[0:1, cols]
            ).astype(BF16)


def run_gate(y, cact, grow, entering, valve, scale):
    return pl.pallas_call(
        gate_kernel,
        out_shape=(
            away_out((ROWS, HALFCH), BF16),
            away_out((ROWS, HALFCH), BF16),
        ),
        compiler_params=limit(16),
        in_specs=[VMEM] * 6,
        out_specs=(VMEM,) * 2,
        name="gate_norm",
    )(*away(y, cact, grow), close(entering), *away(valve, scale))


RIM = 16
CHUNK = 512


def project_kernel(
    place_ref, scale_ref, near_l, far_r, across_l, across_r,
    own_l, own_r, near_r, far_l, own_w, near_w, far_w, across_w, near_x, far_x, across_x,
    own_res, near_res, far_res, across_res,
    out_ref, tail_ref,
    weight, early, res, total, w_sems, e_sems, r_sems,
):
    core = place_ref[4]
    columns_of = (
        pl.ds(pl.multiple_of(core * HALF, HALF), HALF),
        pl.ds(pl.multiple_of((1 - core) * HALF, HALF), HALF),
    )
    arrived = ((near_w, far_w, across_w), (near_x, far_x, across_x))
    copies = ([], [])
    for half in range(2):
        sources = (own_w.at[:, columns_of[half]], *arrived[half])
        for k, source in enumerate(sources):
            target = weight.at[half, k * CH : (k + 1) * CH, :]
            copies[half].append(pltpu.make_async_copy(source, target, w_sems.at[half, k]))
    res_copies = []
    for k, source in enumerate((own_res, near_res, far_res, across_res)):
        rows = pl.ds(pl.multiple_of(place_ref[k] * QUARTER, QUARTER), QUARTER)
        res_copies.append(pltpu.make_async_copy(source, res.at[rows, :], r_sems.at[k]))
    early_copies = [
        pltpu.make_async_copy(source, early.at[k], e_sems.at[k])
        for k, source in enumerate((own_l, own_r, near_r, far_l))
    ]
    acts = (early.at[0], early.at[1], near_l, early.at[2], early.at[3], far_r, across_l, across_r)
    for copy in early_copies + copies[0]:
        copy.start()
    for copy in early_copies + copies[0]:
        copy.wait()
    for copy in copies[1] + res_copies:
        copy.start()
    for half in range(2):
        if half == 1:
            for copy in copies[1]:
                copy.wait()
        for n in range(HALF // CHUNK):
            cols = slice(n * CHUNK, (n + 1) * CHUNK)
            part = None
            for k, act in enumerate(acts):
                term = dot(act[...], weight[half, k * HALFCH : (k + 1) * HALFCH, cols])
                part = term if part is None else part + term
            start = pl.multiple_of((core if half == 0 else 1 - core) * HALF + n * CHUNK, CHUNK)
            total[:, pl.ds(start, CHUNK)] = part
    for copy in res_copies:
        copy.wait()

    def norm(values):
        centred = values - jnp.sum(values, axis=-1, keepdims=True) * (1.0 / D)
        spread = jnp.sum(centred * centred, axis=-1, keepdims=True) * (1.0 / D)
        return (centred * lax.rsqrt(spread + EPSILON) * scale_ref[...]).astype(BF16)


    def norm_rows(i, carry):
        rows = pl.ds(pl.multiple_of(i * 64, 64), 64)
        out_ref[rows, :] = norm(total[rows, :] + ALPHA * res[rows, :].astype(F32))
        return carry

    lax.fori_loop(0, ROWS // 64, norm_rows, 0)
    tail_ref[...] = out_ref[ROWS - RIM : ROWS, :]


def run_project(place, scale, weights, acts, residuals):
    return pl.pallas_call(
        project_kernel,
        out_shape=(close_out((ROWS, D), BF16), close_out((RIM, D), BF16)),
        in_specs=[SMEM] + [VMEM] * 5 + [ANY] * 15,
        out_specs=(VMEM, VMEM),
        scratch_shapes=[
            pltpu.VMEM((2, D, HALF), BF16),
            pltpu.VMEM((4, ROWS, HALFCH), BF16),
            pltpu.VMEM((ROWS, D), BF16),
            pltpu.VMEM((ROWS, D), F32),
            pltpu.SemaphoreType.DMA((2, 4)),
            pltpu.SemaphoreType.DMA((4,)),
            pltpu.SemaphoreType.DMA((4,)),
        ],
        compiler_params=limit(30),
        name="project_norm",
    )(
        place,
        *away(scale),
        *[close(acts[k]) for k in (2, 5, 6, 7)],
        *away(*[acts[k] for k in (0, 1, 3, 4)], *weights, *residuals),
    )


TILES = FFL // 128
NARROW = 512


def down_copies(w_ref, down, sems):
    return [
        pltpu.make_async_copy(
            w_ref.at[n * NARROW : (n + 1) * NARROW, 2 * FFL : 3 * FFL],
            down.at[n * NARROW : (n + 1) * NARROW, :],
            sems.at[n],
        )
        for n in range(D // NARROW)
    ]


def two_quarters(hid, place_ref, half):
    def rows_of(k):
        return hid[pl.ds(pl.multiple_of(place_ref[half, k] * QUARTER, QUARTER), QUARTER), :]

    return jnp.concatenate([rows_of(0), rows_of(1)], axis=0)


AHEAD = 4
STRIP = 512


def widen_kernel(
    sent_ref, gate_t, up_t, normed, rim, w_ref,
    hid, down, send_l, send_r,
    wide, gate_pad, up_pad, wide_sems, down_sems,
):
    def wide_copies(j):
        at = j * 128
        if not isinstance(j, int):
            at = pl.multiple_of(at, 128)
        return (
            pltpu.make_async_copy(
                w_ref.at[:, pl.ds(at, 128)], wide.at[j, :, 0:128], wide_sems.at[j, 0]
            ),
            pltpu.make_async_copy(
                w_ref.at[:, pl.ds(FFL + at, 128)], wide.at[j, :, 128:256], wide_sems.at[j, 1]
            ),
        )

    downs = down_copies(w_ref, down, down_sems)
    for j in range(AHEAD):
        for copy in wide_copies(j):
            copy.start()

    def conv(pad, taps, at):
        total = None
        for k in range(FCONV):
            tap = taps[k : k + 1, pl.ds(at, 128)].astype(F32)
            term = tap * pad[pl.ds(RIM - FCONV + 1 + k, ROWS), :]
            total = term if total is None else total + term
        return total

    def finish(j):
        at = j * 128
        if not isinstance(j, int):
            at = pl.multiple_of(at, 128)
        hid[:, pl.ds(at, 128)] = (
            silu(conv(gate_pad, gate_t, at)) * conv(up_pad, up_t, at)
        ).astype(BF16)

    def tile(j, carry):
        for copy in wide_copies(j):
            copy.wait()

        @pl.when(j + AHEAD < TILES)
        def _():
            for copy in wide_copies(j + AHEAD):
                copy.start()

        @pl.when(j + AHEAD == TILES)
        def _():
            for copy in downs:
                copy.start()

        finish(jnp.maximum(j - 1, 0))
        rows = jnp.concatenate([rim[...], normed[...]], axis=0)
        both = dot(rows, wide[j]).astype(BF16).astype(F32)
        gate_pad[...] = both[:, 0:128]
        up_pad[...] = both[:, 128:256]
        return carry

    lax.fori_loop(0, TILES, tile, 0)
    finish(TILES - 1)
    for copy in downs:
        copy.wait()
    send_l[...] = dot_nt(two_quarters(hid, sent_ref, 0), down[0:STRIP, :]).astype(BF16)
    send_r[...] = dot_nt(two_quarters(hid, sent_ref, 1), down[HALF : HALF + STRIP, :]).astype(BF16)


def run_widen(sent, normed, rim, weights, gate_t, up_t):
    return pl.pallas_call(
        widen_kernel,
        out_shape=(
            close_out((ROWS, FFL), BF16),
            close_out((D, FFL), BF16),
            close_out((2 * QUARTER, STRIP), BF16),
            close_out((2 * QUARTER, STRIP), BF16),
        ),
        in_specs=[SMEM, VMEM, VMEM, VMEM, VMEM, ANY],
        out_specs=(VMEM,) * 4,
        scratch_shapes=[
            pltpu.VMEM((TILES, D, 256), BF16),
            pltpu.VMEM((ROWS + RIM, 128), F32),
            pltpu.VMEM((ROWS + RIM, 128), F32),
            pltpu.SemaphoreType.DMA((TILES, 2)),
            pltpu.SemaphoreType.DMA((D // NARROW,)),
        ],
        compiler_params=limit(24),
        name="widen",
    )(sent, *away(gate_t, up_t), close(normed), close(rim), *away(weights))


def sent_kernel(sent_ref, hid, down, send_l, send_r):
    send_l[...] = dot_nt(two_quarters(hid, sent_ref, 0), down[STRIP:HALF, :]).astype(BF16)
    send_r[...] = dot_nt(two_quarters(hid, sent_ref, 1), down[HALF + STRIP : D, :]).astype(BF16)


def run_sent(sent, hidden, down):
    return pl.pallas_call(
        sent_kernel,
        out_shape=(close_out((2 * QUARTER, STRIP), BF16),) * 2,
        in_specs=[SMEM, VMEM, VMEM],
        out_specs=(VMEM,) * 2,
        compiler_params=limit(8),
        name="shrink_sent",
    )(sent, close(hidden), close(down))


def held_kernel(held_ref, hid, down, own, pass_1, pass_2):
    for half in range(2):
        both = dot_nt(two_quarters(hid, held_ref, half), down[half * HALF : (half + 1) * HALF, :])
        own[:, half * HALF : (half + 1) * HALF] = both[0:QUARTER, :]
        pass_1[:, half * STRIP : (half + 1) * STRIP] = both[QUARTER:, 0:STRIP]
        pass_2[:, half * STRIP : (half + 1) * STRIP] = both[QUARTER:, STRIP:HALF]


def run_held(held, hidden, down):
    return pl.pallas_call(
        held_kernel,
        out_shape=(
            close_out((QUARTER, D), F32),
            close_out((QUARTER, HALF), F32),
            close_out((QUARTER, HALF), F32),
        ),
        in_specs=[SMEM, VMEM, VMEM],
        out_specs=(VMEM,) * 3,
        compiler_params=limit(8),
        name="shrink_held",
    )(held, close(hidden), close(down))


def add_kernel(passed, once_l, once_r, out_l, out_r):
    out_l[...] = (passed[:, 0:STRIP] + once_l[QUARTER:, :].astype(F32)).astype(BF16)
    out_r[...] = (passed[:, STRIP:] + once_r[QUARTER:, :].astype(F32)).astype(BF16)


def run_add(passed, once_l, once_r):
    return pl.pallas_call(
        add_kernel,
        out_shape=(close_out((QUARTER, STRIP), BF16),) * 2,
        in_specs=[VMEM] * 3,
        out_specs=(VMEM,) * 2,
        compiler_params=limit(8),
        name="round_sum",
    )(close(passed), close(once_l), close(once_r))


def last_norm_kernel(
    place_ref, own, l_1, r_1, l_2, r_2, ll_1, rr_1, ll_2, rr_2, res_ref, scale_ref, out_ref
):
    for i in range(2):
        rows = slice(i * 64, (i + 1) * 64)
        kept = pl.ds(pl.multiple_of(place_ref[0] * QUARTER + i * 64, 64), 64)
        parts = []
        for k, (once, twice) in enumerate(((l_1, ll_1), (l_2, ll_2), (r_1, rr_1), (r_2, rr_2))):
            cols = slice(k * STRIP, (k + 1) * STRIP)
            part = own[rows, cols] + once[rows, :].astype(F32) + twice[rows, :].astype(F32)
            parts.append(part + ALPHA * res_ref[kept, cols].astype(F32))
        values = jnp.concatenate(parts, axis=1)
        centred = values - jnp.sum(values, axis=-1, keepdims=True) * (1.0 / D)
        spread = jnp.sum(centred * centred, axis=-1, keepdims=True) * (1.0 / D)
        out_ref[rows, :] = (centred * lax.rsqrt(spread + EPSILON) * scale_ref[...]).astype(BF16)


def run_last_norm(place, own, onces, twices, rows, scale):
    kept = [close(part) for part in (own, *onces, *twices, rows)]
    return pl.pallas_call(
        last_norm_kernel,
        out_shape=jax.ShapeDtypeStruct((QUARTER, D), BF16),
        in_specs=[SMEM] + [VMEM] * 11,
        out_specs=VMEM,
        compiler_params=limit(8),
        name="last_norm",
    )(place, *kept, *away(scale))


NEAR = [(0, 1), (1, 0), (2, 3), (3, 2)]
FAR = [(0, 3), (3, 0), (1, 2), (2, 1)]


def with_near(part):
    return lax.ppermute(part, "tp", NEAR)


def with_far(part):
    return lax.ppermute(part, "tp", FAR)


def forwarded(far_part, near_part):
    part = jnp.where(lax.axis_index("sp_2") == 0, far_part, near_part)
    pairs = [(i, j) for i, j in NEAR] + [(4 + i, 4 + j) for i, j in FAR]
    return lax.ppermute(part, ("sp_2", "tp"), pairs)


def with_core(part):
    return lax.ppermute(part, "sp_2", [(0, 1), (1, 0)])


def next_positions(shard):
    count = lax.axis_size(SP)
    return lax.ppermute(shard, SP, [(i, i + 1) for i in range(count - 1)])


def shards(
    incoming_residual_stream,
    result_valve,
    channel_feed_matrix,
    memory_feed_matrix,
    memory_query_matrix,
    unsoftened_deltas,
    delta_offset,
    channel_fading_speed,
    extra_log_fading,
    bypass_factor,
    channel_feed_kernel,
    memory_feed_kernel,
    memory_query_kernel,
    cluster_scaling_vector,
    mixer_result_matrix,
    initial_scaling_vector,
    valve_matrix,
    widen_matrix,
    shrink_matrix,
    valve_filter_kernel,
    widen_filter_kernel,
    latter_scaling_vector,
):
    own = lax.axis_index("tp").astype(jnp.int32)
    core = lax.axis_index("sp_2").astype(jnp.int32)
    near = own ^ 1
    far = 3 - own
    across = own ^ 2
    place = jnp.stack([own, near, far, across, core])
    sent = jnp.stack([jnp.stack([near, across]), jnp.stack([far, across])])
    held = jnp.stack([jnp.stack([own, far]), jnp.stack([own, near])])

    weights = lax.all_gather(
        jnp.concatenate([valve_matrix, widen_matrix, shrink_matrix.T], axis=1), SP, tiled=True
    )

    rim = run_rim(channel_feed_matrix, memory_feed_matrix, memory_query_matrix)
    _, projection, residual = lax.optimization_barrier(
        (rim, mixer_result_matrix, incoming_residual_stream)
    )
    rim = next_positions(rim)
    drives = (
        unsoftened_deltas.T,
        extra_log_fading.T,
        delta_offset.reshape(1, NH),
        channel_fading_speed.reshape(1, NH),
    )
    x_act, b_act, states, message = run_state(
        channel_feed_matrix,
        memory_feed_matrix,
        rim,
        channel_feed_kernel,
        memory_feed_kernel,
        *drives,
    )
    received = lax.all_to_all(message, SP, 0, 0, tiled=True)

    w_half = lax.dynamic_slice(projection, (0, core * HALF), (CH, HALF))
    w_near = with_near(w_half)
    w_far = with_far(w_half)
    res_near = with_near(residual)
    res_far = with_far(residual)

    y_local, c_act, grow = run_local(
        x_act,
        b_act,
        states,
        memory_query_matrix,
        rim,
        memory_query_kernel,
        *drives,
        bypass_factor.reshape(1, NH),
    )
    prefix = run_prefix(received)
    entering = lax.all_to_all(prefix, SP, 0, 0, tiled=True)
    _, late_near, late_far = lax.optimization_barrier((y_local, w_near, w_far))
    w_across = forwarded(late_far, late_near)
    _, late_near, late_far = lax.optimization_barrier((prefix, res_near, res_far))
    res_across = forwarded(late_far, late_near)
    y_l, y_r = run_gate(
        y_local, c_act, grow, entering, result_valve, cluster_scaling_vector.reshape(1, CH)
    )
    swap = lax.optimization_barrier((prefix, w_near, w_far))[1:]
    w_other = (
        with_core(swap[0]),
        with_core(swap[1]),
        with_core(lax.optimization_barrier((y_l, w_across))[1]),
    )
    far_l = with_far(y_l)
    near_r = with_near(y_r)
    near_l = with_near(y_l)
    far_r = with_far(y_r)
    across_l = with_near(far_l)
    across_r = with_far(near_r)
    normed, tail = run_project(
        place,
        initial_scaling_vector.reshape(1, D),
        (mixer_result_matrix, w_near, w_far, w_across, *w_other),
        (y_l, y_r, near_l, near_r, far_l, far_r, across_l, across_r),
        (residual, res_near, res_far, res_across),
    )
    hidden, down, send_l1, send_r1 = run_widen(
        sent, normed, next_positions(tail), weights, valve_filter_kernel, widen_filter_kernel
    )
    l_1 = with_near(send_l1)
    r_1 = with_far(send_r1)
    send_l2, send_r2 = run_sent(sent, hidden, down)
    l_2 = with_near(send_l2)
    r_2 = with_far(send_r2)
    kept, pass_1, pass_2 = run_held(held, hidden, down)
    on_l1, on_r1 = run_add(pass_1, l_1, r_1)
    ll_1 = with_far(on_l1)
    rr_1 = with_near(on_r1)
    on_l2, on_r2 = run_add(pass_2, l_2, r_2)
    ll_2 = with_far(on_l2)
    rr_2 = with_near(on_r2)
    return run_last_norm(
        place,
        kept,
        (l_1, r_1, l_2, r_2),
        (ll_1, rr_1, ll_2, rr_2),
        normed,
        latter_scaling_vector.reshape(1, D),
    )


def solution(mesh):
    split = Mesh(mesh.devices.reshape(8, 4, 2, mesh.shape["tp"]), ("sp_0", "sp_1", "sp_2", "tp"))
    in_specs = (
        P(SP_TP, None),
        P(SP, "tp"),
        P(SP, "tp"),
        P(SP, "tp"),
        P(SP, "tp"),
        P(SP, "tp"),
        P("tp"),
        P("tp"),
        P(SP, "tp"),
        P("tp"),
        P(None, "tp"),
        P(None, "tp"),
        P(None, "tp"),
        P("tp"),
        P("tp", None),
        P(),
        P(SP, "tp"),
        P(SP, "tp"),
        P("tp", SP),
        P(None, "tp"),
        P(None, "tp"),
        P(),
    )
    out_specs = P(SP_TP, None)

    return jax.shard_map(
        shards, mesh=split, in_specs=in_specs, out_specs=out_specs, check_vma=False
    )
```

```python
import jax
import jax.numpy as jnp
from jax import lax
from jax.experimental import pallas as pl
from jax.experimental.pallas import tpu as pltpu
from jax.sharding import Mesh
from jax.sharding import PartitionSpec as P

HEAD_DIM = 64
STATE = 128
CONV = 4
FCONV = 3
BLOCK = 128
SP = ("sp_0", "sp_1", "sp_2")
SP_TP = ("sp_0", "sp_1", "sp_2", "tp")

EPSILON = 1e-05
ALPHA = 2.0**0.25
F32 = jnp.float32
BF16 = jnp.bfloat16
NEG = -1e30

ROWS = 512
CH = 512
NH = 8
QUARTER = 128
HALFCH = 256
D = 2048
HALF = 1024
FFL = 1408

VMEM = pl.BlockSpec(memory_space=pltpu.VMEM)
SMEM = pl.BlockSpec(memory_space=pltpu.SMEM)
ANY = pl.BlockSpec(memory_space=pl.ANY)
HIGHEST = lax.Precision.HIGHEST
MIB = 1024 * 1024


def limit(mib):
    return pltpu.CompilerParams(vmem_limit_bytes=mib * MIB)


def close(value):
    return pltpu.with_memory_space_constraint(value, pltpu.VMEM)


def close_out(shape, kind):
    return pltpu.VMEM(shape, kind)


def away(*values):
    return tuple(pltpu.with_memory_space_constraint(value, pltpu.HBM) for value in values)


def away_out(shape, kind):
    return pltpu.HBM(shape, kind)


def dot(a, b):
    return jnp.dot(a, b, preferred_element_type=F32)


def dot_nt(a, b, precision=None):
    return lax.dot_general(
        a, b, (((1,), (1,)), ((), ())), precision=precision, preferred_element_type=F32
    )


def silu(v):
    return v / (1.0 + jnp.exp(-v))


def lane_pairs(column_of, rows):
    low = lax.broadcasted_iota(jnp.int32, (rows, 128), 1) < HEAD_DIM
    slabs = []
    for q in range(NH // 2):
        first = jnp.broadcast_to(column_of[:, 2 * q : 2 * q + 1], (rows, 128))
        second = jnp.broadcast_to(column_of[:, 2 * q + 1 : 2 * q + 2], (rows, 128))
        slabs.append(jnp.where(low, first, second))
    return slabs


def eye(n):
    line = lax.broadcasted_iota(jnp.int32, (n, n), 0)
    lane = lax.broadcasted_iota(jnp.int32, (n, n), 1)
    return jnp.where(line == lane, 1.0, 0.0).astype(F32)


def columns(rows):
    return dot_nt(eye(BLOCK), rows, precision=HIGHEST)


def down_column(ref):
    return jnp.sum(eye(NH) * ref[...], axis=1, keepdims=True)


def decays(delta, extra, offset, speed):
    step_in = delta + offset
    step = jnp.maximum(step_in, 0.0) + jnp.log1p(jnp.exp(-jnp.abs(step_in)))
    return step, extra - speed * step


def running_sum(fading):
    line = lax.broadcasted_iota(jnp.int32, (BLOCK, BLOCK), 0)
    lane = lax.broadcasted_iota(jnp.int32, (BLOCK, BLOCK), 1)
    upper = jnp.where(line <= lane, 1.0, 0.0).astype(F32)
    return jnp.dot(fading, upper, precision=HIGHEST, preferred_element_type=F32)


def conv_at(pad, taps, start):
    total = None
    for k in range(CONV):
        term = taps[k : k + 1, :].astype(F32) * pad[pl.ds(start + 8 - CONV + 1 + k, BLOCK), :]
        total = term if total is None else total + term
    return silu(total)


def conv_next(pad, taps, block):
    pad[8 : 8 + BLOCK, :] = block.astype(F32)
    total = None
    for k in range(CONV):
        term = taps[k : k + 1, :].astype(F32) * pad[pl.ds(8 - CONV + 1 + k, BLOCK), :]
        total = term if total is None else total + term
    pad[0:8, :] = pad[BLOCK : BLOCK + 8, :]
    return silu(total)


def rim_kernel(x_ref, b_ref, c_ref, out_ref):
    out_ref[:, 0:CH] = x_ref[...]
    out_ref[:, CH : CH + STATE] = b_ref[...]
    out_ref[:, CH + STATE : CH + 2 * STATE] = c_ref[...]


def run_rim(x, b, c):
    last = lambda width: pl.BlockSpec((8, width), lambda i: (ROWS // 8 - 1, 0))
    return pl.pallas_call(
        rim_kernel,
        grid=(1,),
        out_shape=close_out((8, CH + 2 * STATE), BF16),
        in_specs=[last(CH), last(STATE), last(STATE)],
        out_specs=pl.BlockSpec((8, CH + 2 * STATE), lambda i: (0, 0)),
        name="rim",
    )(*away(x, b, c))


def state_kernel(
    x_ref, b_ref, rim_ref, xt_ref, bt_ref, delta_ref, extra_ref, offset_ref, speed_ref,
    x_out, b_out, state_out, msg_ref,
    xpad, bpad,
):
    xpad[0:8, :] = rim_ref[:, 0:CH].astype(F32)
    bpad[0:8, :] = rim_ref[:, CH : CH + STATE].astype(F32)
    xpad[8 : 8 + ROWS, :] = x_ref[...].astype(F32)
    bpad[8 : 8 + ROWS, :] = b_ref[...].astype(F32)
    step, fading = decays(
        delta_ref[...], extra_ref[...], down_column(offset_ref), down_column(speed_ref)
    )
    state = [jnp.zeros((STATE, 128), F32) for _ in range(NH // 2)]
    base = jnp.zeros((NH, 1), F32)
    for i in range(ROWS // BLOCK):
        start = i * BLOCK
        rows = pl.ds(start, BLOCK)
        here = slice(start, start + BLOCK)
        cum = running_sum(fading[:, here])
        last = cum[:, BLOCK - 1 : BLOCK]
        to_end = lane_pairs(columns(step[:, here] * jnp.exp(last - cum)), BLOCK)
        kept = lane_pairs(columns(jnp.broadcast_to(jnp.exp(last), (NH, BLOCK)))[0:1, :], 1)
        x_act = conv_at(xpad, xt_ref, start).astype(BF16)
        b_act = conv_at(bpad, bt_ref, start).astype(BF16)
        x_out[rows, :] = x_act
        b_out[rows, :] = b_act
        b_turned = b_act.astype(F32).T.astype(BF16)
        for q in range(NH // 2):
            cols = slice(q * 128, (q + 1) * 128)
            fresh = dot(b_turned, (x_act[:, cols].astype(F32) * to_end[q]).astype(BF16))
            state[q] = fresh if i == 0 else state[q] * kept[q] + fresh
            if i < ROWS // BLOCK - 1:
                state_out[i, :, cols] = state[q].astype(BF16)
        base = base + last
    totals = lane_pairs(columns(jnp.broadcast_to(base, (NH, BLOCK)))[0:1, :], 1)
    for q in range(NH // 2):
        block = slice(q * 16, (q + 1) * 16)
        msg_ref[block, 0:8, :] = state[q].reshape(16, 8, 128).astype(BF16)
        left = totals[q]
        parts = []
        for _ in range(3):
            part = left.astype(BF16)
            parts.append(part.astype(F32))
            left = left - part.astype(F32)
        line = lax.broadcasted_iota(jnp.int32, (8, 128), 0)
        packed = jnp.where(line == 0, parts[0], jnp.where(line == 1, parts[1], parts[2]))
        packed = jnp.where(line < 3, packed, 0.0).astype(BF16)
        msg_ref[block, 8:16, :] = jnp.broadcast_to(packed[None], (16, 8, 128))


def run_state(x, b, rim, xt, bt, delta, extra, offset, speed):
    return pl.pallas_call(
        state_kernel,
        out_shape=(
            away_out((ROWS, CH), BF16),
            away_out((ROWS, STATE), BF16),
            away_out((ROWS // BLOCK - 1, STATE, CH), BF16),
            close_out((64, 16, 128), BF16),
        ),
        compiler_params=limit(24),
        in_specs=[VMEM] * 9,
        out_specs=(VMEM,) * 4,
        scratch_shapes=[
            pltpu.VMEM((ROWS + 8, CH), F32),
            pltpu.VMEM((ROWS + 8, STATE), F32),
        ],
        name="local_state",
    )(*away(x, b), close(rim), *away(xt, bt, delta, extra, offset, speed))


def local_kernel(
    x_ref, b_ref, state_ref, c_ref, rim_ref, ct_ref, delta_ref, extra_ref, offset_ref, speed_ref,
    bypass_ref,
    y_ref, cact_ref, grow_ref,
    cpad,
):
    cpad[0:8, :] = rim_ref[:, CH + STATE : CH + 2 * STATE].astype(F32)
    offset = down_column(offset_ref)
    speed = down_column(speed_ref)
    bypass = lane_pairs(bypass_ref[...], 1)
    row = lax.broadcasted_iota(jnp.int32, (BLOCK, BLOCK), 0)
    col = lax.broadcasted_iota(jnp.int32, (BLOCK, BLOCK), 1)
    causal = row >= col
    low = col < HEAD_DIM

    def block_step(i, base):
        rows = pl.ds(pl.multiple_of(i * BLOCK, BLOCK), BLOCK)
        step, fading = decays(delta_ref[:, rows], extra_ref[:, rows], offset, speed)
        cum = running_sum(fading)
        turned = columns(jnp.concatenate([cum, jnp.exp(cum), jnp.exp(base + cum)], axis=0))
        grow_ref[rows, :] = turned[:, 2 * NH : 3 * NH]
        grown = lane_pairs(turned[:, NH : 2 * NH], BLOCK)
        c_act = conv_next(cpad, ct_ref, c_ref[rows, :]).astype(BF16)
        cact_ref[rows, :] = c_act
        affinity = dot_nt(c_act, b_ref[rows, :])
        for q in range(NH // 2):
            cols = slice(q * 128, (q + 1) * 128)
            x_here = x_ref[rows, cols]
            within = []
            for h in (2 * q, 2 * q + 1):
                between = turned[:, h : h + 1] - cum[h : h + 1, :]
                lag = jnp.exp(jnp.where(causal, between, NEG)) * step[h : h + 1, :]
                within.append(dot((affinity * lag).astype(BF16), x_here))
            total = jnp.where(low, within[0], within[1]) + bypass[q] * x_here.astype(F32)
            carried = dot(c_act, state_ref[jnp.maximum(i - 1, 0), :, cols]) * grown[q]
            y_ref[rows, cols] = total + jnp.where(i > 0, carried, 0.0)
        return base + cum[:, BLOCK - 1 : BLOCK]

    lax.fori_loop(0, ROWS // BLOCK, block_step, jnp.zeros((NH, 1), F32))


def run_local(x, b, states, c, rim, ct, delta, extra, offset, speed, bypass):
    return pl.pallas_call(
        local_kernel,
        out_shape=(
            away_out((ROWS, CH), F32),
            away_out((ROWS, STATE), BF16),
            away_out((ROWS, NH), F32),
        ),
        compiler_params=limit(24),
        in_specs=[VMEM] * 11,
        out_specs=(VMEM,) * 3,
        scratch_shapes=[pltpu.VMEM((BLOCK + 8, STATE), F32)],
        name="local_mixer",
    )(*away(x, b, states, c), close(rim), *away(ct, delta, extra, offset, speed, bypass))


def prefix_kernel(in_ref, out_ref):
    entering = jnp.zeros((8, 128), F32)
    for j in range(64):
        out_ref[j] = entering.astype(BF16)
        piece = in_ref[j].astype(F32)
        total = piece[8:9, :] + piece[9:10, :] + piece[10:11, :]
        entering = entering * jnp.exp(total) + piece[0:8, :]


def run_prefix(received):
    return pl.pallas_call(
        prefix_kernel,
        out_shape=close_out((64, 8, 128), BF16),
        compiler_params=limit(8),
        in_specs=[VMEM],
        out_specs=VMEM,
        name="state_prefix",
    )(close(received))


def gate_kernel(y_ref, cact_ref, grow_ref, in_ref, valve_ref, scale_ref, out_l, out_r):
    for i in range(ROWS // BLOCK):
        rows = pl.ds(i * BLOCK, BLOCK)
        grown = lane_pairs(grow_ref[rows, :], BLOCK)
        c_act = cact_ref[rows, :]
        gated = []
        square = jnp.zeros((BLOCK, 1), F32)
        for q in range(NH // 2):
            cols = slice(q * 128, (q + 1) * 128)
            entering = in_ref[q * 16 : (q + 1) * 16].astype(F32).reshape(STATE, 128).astype(BF16)
            y = y_ref[rows, cols] + dot(c_act, entering) * grown[q]
            y = y * silu(valve_ref[rows, cols].astype(F32))
            gated.append(y)
            square = square + jnp.sum(y * y, axis=-1, keepdims=True)
        factor = lax.rsqrt(square * (1.0 / CH) + EPSILON)
        for q in range(NH // 2):
            cols = slice(q * 128, (q + 1) * 128)
            half = (out_l, out_r)[q // 2]
            half[rows, (q % 2) * 128 : (q % 2 + 1) * 128] = (
                gated[q] * factor * scale_ref[0:1, cols]
            ).astype(BF16)


def run_gate(y, cact, grow, entering, valve, scale):
    return pl.pallas_call(
        gate_kernel,
        out_shape=(
            away_out((ROWS, HALFCH), BF16),
            away_out((ROWS, HALFCH), BF16),
        ),
        compiler_params=limit(16),
        in_specs=[VMEM] * 6,
        out_specs=(VMEM,) * 2,
        name="gate_norm",
    )(*away(y, cact, grow), close(entering), *away(valve, scale))


RIM = 16
CHUNK = 512


def project_kernel(
    place_ref, scale_ref, near_l, far_r, across_l, across_r,
    own_l, own_r, near_r, far_l, own_w, near_w, far_w, across_w, near_x, far_x, across_x,
    own_res, near_res, far_res, across_res,
    out_ref, tail_ref,
    weight, early, res, total, w_sems, e_sems, r_sems,
):
    core = place_ref[4]
    columns_of = (
        pl.ds(pl.multiple_of(core * HALF, HALF), HALF),
        pl.ds(pl.multiple_of((1 - core) * HALF, HALF), HALF),
    )
    arrived = ((near_w, far_w, across_w), (near_x, far_x, across_x))
    copies = ([], [])
    for half in range(2):
        sources = (own_w.at[:, columns_of[half]], *arrived[half])
        for k, source in enumerate(sources):
            target = weight.at[half, k * CH : (k + 1) * CH, :]
            copies[half].append(pltpu.make_async_copy(source, target, w_sems.at[half, k]))
    res_copies = []
    for k, source in enumerate((own_res, near_res, far_res, across_res)):
        rows = pl.ds(pl.multiple_of(place_ref[k] * QUARTER, QUARTER), QUARTER)
        res_copies.append(pltpu.make_async_copy(source, res.at[rows, :], r_sems.at[k]))
    early_copies = [
        pltpu.make_async_copy(source, early.at[k], e_sems.at[k])
        for k, source in enumerate((own_l, own_r, near_r, far_l))
    ]
    acts = (early.at[0], early.at[1], near_l, early.at[2], early.at[3], far_r, across_l, across_r)
    for copy in early_copies + copies[0]:
        copy.start()
    for copy in early_copies + copies[0]:
        copy.wait()
    for copy in copies[1] + res_copies:
        copy.start()
    for half in range(2):
        if half == 1:
            for copy in copies[1]:
                copy.wait()
        for n in range(HALF // CHUNK):
            cols = slice(n * CHUNK, (n + 1) * CHUNK)
            part = None
            for k, act in enumerate(acts):
                term = dot(act[...], weight[half, k * HALFCH : (k + 1) * HALFCH, cols])
                part = term if part is None else part + term
            start = pl.multiple_of((core if half == 0 else 1 - core) * HALF + n * CHUNK, CHUNK)
            total[:, pl.ds(start, CHUNK)] = part
    for copy in res_copies:
        copy.wait()

    def norm(values):
        centred = values - jnp.sum(values, axis=-1, keepdims=True) * (1.0 / D)
        spread = jnp.sum(centred * centred, axis=-1, keepdims=True) * (1.0 / D)
        return (centred * lax.rsqrt(spread + EPSILON) * scale_ref[...]).astype(BF16)


    def norm_rows(i, carry):
        rows = pl.ds(pl.multiple_of(i * 64, 64), 64)
        out_ref[rows, :] = norm(total[rows, :] + ALPHA * res[rows, :].astype(F32))
        return carry

    lax.fori_loop(0, ROWS // 64, norm_rows, 0)
    tail_ref[...] = out_ref[ROWS - RIM : ROWS, :]


def run_project(place, scale, weights, acts, residuals):
    return pl.pallas_call(
        project_kernel,
        out_shape=(close_out((ROWS, D), BF16), close_out((RIM, D), BF16)),
        in_specs=[SMEM] + [VMEM] * 5 + [ANY] * 15,
        out_specs=(VMEM, VMEM),
        scratch_shapes=[
            pltpu.VMEM((2, D, HALF), BF16),
            pltpu.VMEM((4, ROWS, HALFCH), BF16),
            pltpu.VMEM((ROWS, D), BF16),
            pltpu.VMEM((ROWS, D), F32),
            pltpu.SemaphoreType.DMA((2, 4)),
            pltpu.SemaphoreType.DMA((4,)),
            pltpu.SemaphoreType.DMA((4,)),
        ],
        compiler_params=limit(30),
        name="project_norm",
    )(
        place,
        *away(scale),
        *[close(acts[k]) for k in (2, 5, 6, 7)],
        *away(*[acts[k] for k in (0, 1, 3, 4)], *weights, *residuals),
    )


TILES = FFL // 128
NARROW = 512


def down_copies(w_ref, down, sems):
    return [
        pltpu.make_async_copy(
            w_ref.at[n * NARROW : (n + 1) * NARROW, 2 * FFL : 3 * FFL],
            down.at[n * NARROW : (n + 1) * NARROW, :],
            sems.at[n],
        )
        for n in range(D // NARROW)
    ]


def two_quarters(hid, place_ref, half):
    def rows_of(k):
        return hid[pl.ds(pl.multiple_of(place_ref[half, k] * QUARTER, QUARTER), QUARTER), :]

    return jnp.concatenate([rows_of(0), rows_of(1)], axis=0)


AHEAD = 4
FIRST = 2
STRIP = 512


def widen_kernel(
    sent_ref, gate_t, up_t, normed, rim, w_ref,
    hid, down, send_l, send_r,
    wide, gate_pad, up_pad, wide_sems, down_sems,
):
    def wide_copies(j):
        at = j * 128
        if not isinstance(j, int):
            at = pl.multiple_of(at, 128)
        return (
            pltpu.make_async_copy(
                w_ref.at[:, pl.ds(at, 128)], wide.at[j, :, 0:128], wide_sems.at[j, 0]
            ),
            pltpu.make_async_copy(
                w_ref.at[:, pl.ds(FFL + at, 128)], wide.at[j, :, 128:256], wide_sems.at[j, 1]
            ),
        )

    downs = down_copies(w_ref, down, down_sems)
    for j in range(FIRST):
        for copy in wide_copies(j):
            copy.start()

    def conv(pad, taps, at):
        total = None
        for k in range(FCONV):
            tap = taps[k : k + 1, pl.ds(at, 128)].astype(F32)
            term = tap * pad[pl.ds(RIM - FCONV + 1 + k, ROWS), :]
            total = term if total is None else total + term
        return total

    def finish(j):
        at = j * 128
        if not isinstance(j, int):
            at = pl.multiple_of(at, 128)
        hid[:, pl.ds(at, 128)] = (
            silu(conv(gate_pad, gate_t, at)) * conv(up_pad, up_t, at)
        ).astype(BF16)

    def tile(j, carry):
        for copy in wide_copies(j):
            copy.wait()

        @pl.when(j == 0)
        def _():
            for later in range(FIRST, AHEAD):
                for copy in wide_copies(later):
                    copy.start()

        @pl.when(j + AHEAD < TILES)
        def _():
            for copy in wide_copies(j + AHEAD):
                copy.start()

        @pl.when(j + AHEAD == TILES)
        def _():
            for copy in downs:
                copy.start()

        finish(jnp.maximum(j - 1, 0))
        rows = jnp.concatenate([rim[...], normed[...]], axis=0)
        both = dot(rows, wide[j]).astype(BF16).astype(F32)
        gate_pad[...] = both[:, 0:128]
        up_pad[...] = both[:, 128:256]
        return carry

    lax.fori_loop(0, TILES, tile, 0)
    finish(TILES - 1)
    for copy in downs:
        copy.wait()
    send_l[...] = dot_nt(two_quarters(hid, sent_ref, 0), down[0:STRIP, :]).astype(BF16)
    send_r[...] = dot_nt(two_quarters(hid, sent_ref, 1), down[HALF : HALF + STRIP, :]).astype(BF16)


def run_widen(sent, normed, rim, weights, gate_t, up_t):
    return pl.pallas_call(
        widen_kernel,
        out_shape=(
            close_out((ROWS, FFL), BF16),
            close_out((D, FFL), BF16),
            close_out((2 * QUARTER, STRIP), BF16),
            close_out((2 * QUARTER, STRIP), BF16),
        ),
        in_specs=[SMEM, VMEM, VMEM, VMEM, VMEM, ANY],
        out_specs=(VMEM,) * 4,
        scratch_shapes=[
            pltpu.VMEM((TILES, D, 256), BF16),
            pltpu.VMEM((ROWS + RIM, 128), F32),
            pltpu.VMEM((ROWS + RIM, 128), F32),
            pltpu.SemaphoreType.DMA((TILES, 2)),
            pltpu.SemaphoreType.DMA((D // NARROW,)),
        ],
        compiler_params=limit(24),
        name="widen",
    )(sent, *away(gate_t, up_t), close(normed), close(rim), *away(weights))


def sent_kernel(sent_ref, hid, down, send_l, send_r):
    send_l[...] = dot_nt(two_quarters(hid, sent_ref, 0), down[STRIP:HALF, :]).astype(BF16)
    send_r[...] = dot_nt(two_quarters(hid, sent_ref, 1), down[HALF + STRIP : D, :]).astype(BF16)


def run_sent(sent, hidden, down):
    return pl.pallas_call(
        sent_kernel,
        out_shape=(close_out((2 * QUARTER, STRIP), BF16),) * 2,
        in_specs=[SMEM, VMEM, VMEM],
        out_specs=(VMEM,) * 2,
        compiler_params=limit(8),
        name="shrink_sent",
    )(sent, close(hidden), close(down))


def held_kernel(held_ref, hid, down, own, pass_1, pass_2):
    for half in range(2):
        both = dot_nt(two_quarters(hid, held_ref, half), down[half * HALF : (half + 1) * HALF, :])
        own[:, half * HALF : (half + 1) * HALF] = both[0:QUARTER, :]
        pass_1[:, half * STRIP : (half + 1) * STRIP] = both[QUARTER:, 0:STRIP]
        pass_2[:, half * STRIP : (half + 1) * STRIP] = both[QUARTER:, STRIP:HALF]


def run_held(held, hidden, down):
    return pl.pallas_call(
        held_kernel,
        out_shape=(
            close_out((QUARTER, D), F32),
            close_out((QUARTER, HALF), F32),
            close_out((QUARTER, HALF), F32),
        ),
        in_specs=[SMEM, VMEM, VMEM],
        out_specs=(VMEM,) * 3,
        compiler_params=limit(8),
        name="shrink_held",
    )(held, close(hidden), close(down))


def add_kernel(passed, once_l, once_r, out_l, out_r):
    out_l[...] = (passed[:, 0:STRIP] + once_l[QUARTER:, :].astype(F32)).astype(BF16)
    out_r[...] = (passed[:, STRIP:] + once_r[QUARTER:, :].astype(F32)).astype(BF16)


def run_add(passed, once_l, once_r):
    return pl.pallas_call(
        add_kernel,
        out_shape=(close_out((QUARTER, STRIP), BF16),) * 2,
        in_specs=[VMEM] * 3,
        out_specs=(VMEM,) * 2,
        compiler_params=limit(8),
        name="round_sum",
    )(close(passed), close(once_l), close(once_r))


def last_norm_kernel(
    place_ref, own, l_1, r_1, l_2, r_2, ll_1, rr_1, ll_2, rr_2, res_ref, scale_ref, out_ref
):
    for i in range(2):
        rows = slice(i * 64, (i + 1) * 64)
        kept = pl.ds(pl.multiple_of(place_ref[0] * QUARTER + i * 64, 64), 64)
        parts = []
        for k, (once, twice) in enumerate(((l_1, ll_1), (l_2, ll_2), (r_1, rr_1), (r_2, rr_2))):
            cols = slice(k * STRIP, (k + 1) * STRIP)
            part = own[rows, cols] + once[rows, :].astype(F32) + twice[rows, :].astype(F32)
            parts.append(part + ALPHA * res_ref[kept, cols].astype(F32))
        values = jnp.concatenate(parts, axis=1)
        centred = values - jnp.sum(values, axis=-1, keepdims=True) * (1.0 / D)
        spread = jnp.sum(centred * centred, axis=-1, keepdims=True) * (1.0 / D)
        out_ref[rows, :] = (centred * lax.rsqrt(spread + EPSILON) * scale_ref[...]).astype(BF16)


def run_last_norm(place, own, onces, twices, rows, scale):
    kept = [close(part) for part in (own, *onces, *twices, rows)]
    return pl.pallas_call(
        last_norm_kernel,
        out_shape=jax.ShapeDtypeStruct((QUARTER, D), BF16),
        in_specs=[SMEM] + [VMEM] * 11,
        out_specs=VMEM,
        compiler_params=limit(8),
        name="last_norm",
    )(place, *kept, *away(scale))


NEAR = [(0, 1), (1, 0), (2, 3), (3, 2)]
FAR = [(0, 3), (3, 0), (1, 2), (2, 1)]


def with_near(part):
    return lax.ppermute(part, "tp", NEAR)


def with_far(part):
    return lax.ppermute(part, "tp", FAR)


def forwarded(far_part, near_part):
    part = jnp.where(lax.axis_index("sp_2") == 0, far_part, near_part)
    pairs = [(i, j) for i, j in NEAR] + [(4 + i, 4 + j) for i, j in FAR]
    return lax.ppermute(part, ("sp_2", "tp"), pairs)


def with_core(part):
    return lax.ppermute(part, "sp_2", [(0, 1), (1, 0)])


def next_positions(shard):
    count = lax.axis_size(SP)
    return lax.ppermute(shard, SP, [(i, i + 1) for i in range(count - 1)])


def shards(
    incoming_residual_stream,
    result_valve,
    channel_feed_matrix,
    memory_feed_matrix,
    memory_query_matrix,
    unsoftened_deltas,
    delta_offset,
    channel_fading_speed,
    extra_log_fading,
    bypass_factor,
    channel_feed_kernel,
    memory_feed_kernel,
    memory_query_kernel,
    cluster_scaling_vector,
    mixer_result_matrix,
    initial_scaling_vector,
    valve_matrix,
    widen_matrix,
    shrink_matrix,
    valve_filter_kernel,
    widen_filter_kernel,
    latter_scaling_vector,
):
    own = lax.axis_index("tp").astype(jnp.int32)
    core = lax.axis_index("sp_2").astype(jnp.int32)
    near = own ^ 1
    far = 3 - own
    across = own ^ 2
    place = jnp.stack([own, near, far, across, core])
    sent = jnp.stack([jnp.stack([near, across]), jnp.stack([far, across])])
    held = jnp.stack([jnp.stack([own, far]), jnp.stack([own, near])])

    weights = lax.all_gather(
        jnp.concatenate([valve_matrix, widen_matrix, shrink_matrix.T], axis=1), SP, tiled=True
    )

    rim = run_rim(channel_feed_matrix, memory_feed_matrix, memory_query_matrix)
    _, projection, residual = lax.optimization_barrier(
        (rim, mixer_result_matrix, incoming_residual_stream)
    )
    rim = next_positions(rim)
    drives = (
        unsoftened_deltas.T,
        extra_log_fading.T,
        delta_offset.reshape(1, NH),
        channel_fading_speed.reshape(1, NH),
    )
    x_act, b_act, states, message = run_state(
        channel_feed_matrix,
        memory_feed_matrix,
        rim,
        channel_feed_kernel,
        memory_feed_kernel,
        *drives,
    )
    received = lax.all_to_all(message, SP, 0, 0, tiled=True)

    w_half = lax.dynamic_slice(projection, (0, core * HALF), (CH, HALF))
    w_near = with_near(w_half)
    w_far = with_far(w_half)
    res_near = with_near(residual)
    res_far = with_far(residual)

    y_local, c_act, grow = run_local(
        x_act,
        b_act,
        states,
        memory_query_matrix,
        rim,
        memory_query_kernel,
        *drives,
        bypass_factor.reshape(1, NH),
    )
    prefix = run_prefix(received)
    entering = lax.all_to_all(prefix, SP, 0, 0, tiled=True)
    _, late_near, late_far = lax.optimization_barrier((y_local, w_near, w_far))
    w_across = forwarded(late_far, late_near)
    _, late_near, late_far = lax.optimization_barrier((prefix, res_near, res_far))
    res_across = forwarded(late_far, late_near)
    y_l, y_r = run_gate(
        y_local, c_act, grow, entering, result_valve, cluster_scaling_vector.reshape(1, CH)
    )
    swap = lax.optimization_barrier((prefix, w_near, w_far))[1:]
    w_other = (
        with_core(swap[0]),
        with_core(swap[1]),
        with_core(lax.optimization_barrier((y_l, w_across))[1]),
    )
    far_l = with_far(y_l)
    near_r = with_near(y_r)
    near_l = with_near(y_l)
    far_r = with_far(y_r)
    across_l = with_near(far_l)
    across_r = with_far(near_r)
    normed, tail = run_project(
        place,
        initial_scaling_vector.reshape(1, D),
        (mixer_result_matrix, w_near, w_far, w_across, *w_other),
        (y_l, y_r, near_l, near_r, far_l, far_r, across_l, across_r),
        (residual, res_near, res_far, res_across),
    )
    hidden, down, send_l1, send_r1 = run_widen(
        sent, normed, next_positions(tail), weights, valve_filter_kernel, widen_filter_kernel
    )
    l_1 = with_near(send_l1)
    r_1 = with_far(send_r1)
    send_l2, send_r2 = run_sent(sent, hidden, down)
    l_2 = with_near(send_l2)
    r_2 = with_far(send_r2)
    kept, pass_1, pass_2 = run_held(held, hidden, down)
    on_l1, on_r1 = run_add(pass_1, l_1, r_1)
    ll_1 = with_far(on_l1)
    rr_1 = with_near(on_r1)
    on_l2, on_r2 = run_add(pass_2, l_2, r_2)
    ll_2 = with_far(on_l2)
    rr_2 = with_near(on_r2)
    return run_last_norm(
        place,
        kept,
        (l_1, r_1, l_2, r_2),
        (ll_1, rr_1, ll_2, rr_2),
        normed,
        latter_scaling_vector.reshape(1, D),
    )


def solution(mesh):
    split = Mesh(mesh.devices.reshape(8, 4, 2, mesh.shape["tp"]), ("sp_0", "sp_1", "sp_2", "tp"))
    in_specs = (
        P(SP_TP, None),
        P(SP, "tp"),
        P(SP, "tp"),
        P(SP, "tp"),
        P(SP, "tp"),
        P(SP, "tp"),
        P("tp"),
        P("tp"),
        P(SP, "tp"),
        P("tp"),
        P(None, "tp"),
        P(None, "tp"),
        P(None, "tp"),
        P("tp"),
        P("tp", None),
        P(),
        P(SP, "tp"),
        P(SP, "tp"),
        P("tp", SP),
        P(None, "tp"),
        P(None, "tp"),
        P(),
    )
    out_specs = P(SP_TP, None)

    return jax.shard_map(
        shards, mesh=split, in_specs=in_specs, out_specs=out_specs, check_vma=False
    )
```
